128 devices in a mesh: sp: 32 (over z, y, core), tp: 4 (over x).
Axes of the slice: x: 4, y: 4, z: 4, core: 2. Of those that a mesh axis runs over, the one named last changes fastest.
Arguments:
- tokens: bfloat16 [4096, 1024], P('sp', 'tp'), may hold values from -6 to 6
- norm_gain: float32 [1024], replicated, may hold values from 0.1 to 1.9
- attn_query: bfloat16 [1024, 512], P('sp', 'tp'), may hold values from -0.1875 to 0.1875
- attn_key: bfloat16 [1024, 256], P('sp', 'tp'), may hold values from -0.1875 to 0.1875
- attn_value: bfloat16 [1024, 256], P('sp', 'tp'), may hold values from -0.1875 to 0.1875
- sink_logit: float32 [8], P('tp'), may hold values from 2 to 7
- delta_query: bfloat16 [1024, 512], P('sp', 'tp'), may hold values from -0.1875 to 0.1875
- delta_key: bfloat16 [1024, 512], P('sp', 'tp'), may hold values from -0.1875 to 0.1875
- delta_value: bfloat16 [1024, 512], P('sp', 'tp'), may hold values from -0.1875 to 0.1875
- delta_gate: bfloat16 [1024, 512], P('sp', 'tp'), may hold values from -0.1875 to 0.1875
- beta_weight: bfloat16 [1024, 8, 2], P('sp', 'tp'), may hold values from -0.1875 to 0.1875
- decay_weight: bfloat16 [1024, 8, 2], P('sp', 'tp'), may hold values from -0.1875 to 0.1875
- beta_shift: float32 [2, 8], P(None, 'tp'), may hold values from -5 to -2
- decay_log: float32 [2, 8], P(None, 'tp'), may hold values from -2.5 to 1
- out_gain: float32 [64], replicated, may hold values from 0.1 to 1.9
- attn_out: bfloat16 [512, 1024], P('tp', 'sp'), may hold values from -1.5 to 1.5
- delta_out: bfloat16 [512, 1024], P('tp', 'sp'), may hold values from -0.25 to 0.25
Outputs:
- mixed: bfloat16 [4096, 1024], P(('sp', 'tp'))
The draws below stay inside these ranges and needn't reach their ends.
All inputs are finite; a program needn't handle non-finite values.
Results may differ from the reference program's by a relative error of at most 0.0045.
Values may be sent and summed in bfloat16 or wider, within the bound.
A program may use at most 64 MiB of HBM per device.

```python
import jax
import jax.numpy as jnp
from jax import lax

D = 1024
HEAD_DIM = 64
HEADS = 8
KV_HEADS = 4
DELTA_HEADS = 8
WINDOW = 64
TOK_DEV = 128
TOKENS = 4096
N_SP = 32


def shard_levels(stream_key, dims, split, low, largest):
    level, own = 1.0, jax.random.fold_in(stream_key, 6)
    for position, blocks in split:
        steps = jnp.exp(jax.random.uniform(jax.random.fold_in(own, position), (blocks,), jnp.float32, low / len(split), largest / len(split)))
        level = level * jnp.repeat(steps, dims[position] // blocks).reshape([-1 if axis == position else 1 for axis in range(len(dims))])
    return level


def noise(key, dims, scale, bound, shards=(), kind=jnp.bfloat16):
    entries = scale * jax.random.normal(key, dims, jnp.float32)
    if shards:
        entries = entries * shard_levels(key, dims, shards, -0.22, 0.18)
    return jnp.clip(entries, -bound, bound).astype(kind)


def setup_inputs(seed: int = 0) -> dict:
    key_of = jax.random.split(jax.random.key(seed), 18)
    tokens = noise(key_of[0], (TOKENS, D), 1.0, 6.0, ((0, 32), (1, 4)))
    norm_gain = jnp.clip(1.0 + 0.18 * jax.random.normal(key_of[1], (D,), jnp.float32), 0.1, 1.9)
    attn_query = noise(key_of[2], (D, HEADS * HEAD_DIM), D ** -0.5, 0.1875, ((0, 32), (1, 4)))
    attn_key = noise(key_of[3], (D, KV_HEADS * HEAD_DIM), D ** -0.5, 0.1875, ((0, 32), (1, 4)))
    attn_value = noise(key_of[4], (D, KV_HEADS * HEAD_DIM), D ** -0.5, 0.1875, ((0, 32), (1, 4)))
    sink_logit = jnp.clip(2.0 + 5.0 * jax.random.uniform(key_of[5], (HEADS,), jnp.float32) ** shard_levels(key_of[5], (HEADS,), ((0, 4),), -0.2, 0.2), 2.0, 7.0)
    delta_query = noise(key_of[6], (D, DELTA_HEADS * HEAD_DIM), D ** -0.5, 0.1875, ((0, 32), (1, 4)))
    delta_key = noise(key_of[7], (D, DELTA_HEADS * HEAD_DIM), D ** -0.5, 0.1875, ((0, 32), (1, 4)))
    delta_value = noise(key_of[8], (D, DELTA_HEADS * HEAD_DIM), D ** -0.5, 0.1875, ((0, 32), (1, 4)))
    delta_gate = noise(key_of[9], (D, DELTA_HEADS * HEAD_DIM), D ** -0.5, 0.1875, ((0, 32), (1, 4)))
    beta_weight = noise(key_of[10], (D, DELTA_HEADS, 2), D ** -0.5, 0.1875, ((0, 32), (1, 4)))
    decay_weight = noise(key_of[11], (D, DELTA_HEADS, 2), D ** -0.5, 0.1875, ((0, 32), (1, 4)))
    beta_shift = jnp.clip(-5.0 + 3.0 * jax.random.uniform(key_of[12], (2, DELTA_HEADS), jnp.float32) ** shard_levels(key_of[12], (2, DELTA_HEADS), ((1, 4),), -0.2, 0.2), -5.0, -2.0)
    decay_log = jnp.clip(-2.5 + 3.5 * jax.random.uniform(key_of[13], (2, DELTA_HEADS), jnp.float32) ** shard_levels(key_of[13], (2, DELTA_HEADS), ((1, 4),), -0.2, 0.2), -2.5, 1.0)
    out_gain = jnp.clip(1.0 + 0.18 * jax.random.normal(key_of[14], (HEAD_DIM,), jnp.float32), 0.1, 1.9)
    attn_out = noise(key_of[15], (HEADS * HEAD_DIM, D), 16 ** -0.5, 1.5, ((0, 4), (1, 32)))
    delta_out = noise(key_of[16], (DELTA_HEADS * HEAD_DIM, D), (DELTA_HEADS * HEAD_DIM) ** -0.5, 0.25, ((0, 4), (1, 32)))
    return {"tokens": tokens, "norm_gain": norm_gain, "attn_query": attn_query, "attn_key": attn_key, "attn_value": attn_value, "sink_logit": sink_logit, "delta_query": delta_query, "delta_key": delta_key, "delta_value": delta_value, "delta_gate": delta_gate, "beta_weight": beta_weight, "decay_weight": decay_weight, "beta_shift": beta_shift, "decay_log": decay_log, "out_gain": out_gain, "attn_out": attn_out, "delta_out": delta_out}


norm_eps = 1e-06

def rounded(values):
    return lax.optimization_barrier(values.astype(jnp.bfloat16))

def unit_rows(values):
    return values * lax.rsqrt(lax.optimization_barrier(jnp.sum(values * values, axis=-1, keepdims=True)) + norm_eps)

def delta_recur(queries, key_rows, value_rows, log_decay, strength):

    def advance(carry_state, inputs):
        q_row, k_row, v_row, g_row, b_row = inputs
        recall = jnp.einsum('hd,hde->he', k_row, carry_state, precision=lax.Precision.HIGHEST)
        beta_col = b_row[:, None, None]
        carry_state = jnp.exp(g_row)[:, None, None] * (carry_state - beta_col * k_row[:, :, None] * recall[:, None, :]) + beta_col * k_row[:, :, None] * v_row[:, None, :]
        output = jnp.einsum('hd,hde->he', q_row, carry_state, precision=lax.Precision.HIGHEST)
        return (carry_state, output)
    start_state = jnp.zeros((queries.shape[1], queries.shape[2], value_rows.shape[2]), jnp.float32)
    _, outputs = lax.scan(advance, start_state, (queries, key_rows, value_rows, log_decay, strength))
    return outputs

def reference(tokens, norm_gain, attn_query, attn_key, attn_value, sink_logit, delta_query, delta_key, delta_value, delta_gate, beta_weight, decay_weight, beta_shift, decay_log, out_gain, attn_out, delta_out):
    total_rows = tokens.shape[0]
    wide_rows = tokens.astype(jnp.float32)
    inverse = lax.rsqrt(lax.optimization_barrier(jnp.mean(wide_rows * wide_rows, axis=-1, keepdims=True)) + norm_eps)
    normed = (wide_rows * inverse * norm_gain).astype(jnp.bfloat16)

    def project(weight):
        return jnp.dot(normed, weight.reshape(weight.shape[0], -1), preferred_element_type=jnp.float32)
    group_size = HEADS // KV_HEADS
    queries = rounded(project(attn_query)).reshape(total_rows, KV_HEADS, group_size, HEAD_DIM)
    key_rows = rounded(project(attn_key)).reshape(total_rows, KV_HEADS, HEAD_DIM)
    value_rows = rounded(project(attn_value)).reshape(total_rows, KV_HEADS, HEAD_DIM)
    key_pad = jnp.pad(key_rows, ((WINDOW, WINDOW), (0, 0), (0, 0)))
    value_pad = jnp.pad(value_rows, ((WINDOW, WINDOW), (0, 0), (0, 0)))
    sink_row = sink_logit.reshape(KV_HEADS, group_size, 1, 1)
    key_span = TOK_DEV + 2 * WINDOW

    def attend(block_index):
        first_row = block_index * TOK_DEV
        q_block = lax.dynamic_slice_in_dim(queries, first_row, TOK_DEV, 0).astype(jnp.float32)
        k_block = lax.dynamic_slice_in_dim(key_pad, first_row, key_span, 0).astype(jnp.float32)
        v_block = lax.dynamic_slice_in_dim(value_pad, first_row, key_span, 0).astype(jnp.float32)
        scores = jnp.einsum('tkgd,jkd->kgtj', q_block, k_block) * HEAD_DIM ** (-0.5)
        q_pos = first_row + jnp.arange(TOK_DEV, dtype=jnp.int32)
        k_pos = first_row - WINDOW + jnp.arange(key_span, dtype=jnp.int32)
        allowed = (jnp.abs(q_pos[:, None] - k_pos[None, :]) <= WINDOW) & (k_pos[None, :] >= 0) & (k_pos[None, :] < total_rows)
        scores = jnp.where(allowed, scores, -jnp.inf)
        row_max = jnp.maximum(lax.optimization_barrier(jnp.max(scores, axis=-1, keepdims=True)), sink_row)
        weights = jnp.exp(scores - row_max)
        weights = weights / (lax.optimization_barrier(jnp.sum(weights, axis=-1, keepdims=True)) + jnp.exp(sink_row - row_max))
        heads_out = jnp.einsum('kgtj,jkd->tkgd', rounded(weights).astype(jnp.float32), v_block)
        return heads_out.reshape(TOK_DEV, HEADS * HEAD_DIM).astype(jnp.bfloat16)
    y_attn = lax.map(attend, jnp.arange(N_SP, dtype=jnp.int32)).reshape(total_rows, HEADS * HEAD_DIM)

    def activate(weight):
        return jax.nn.silu(rounded(project(weight)).astype(jnp.float32)).reshape(total_rows, DELTA_HEADS, HEAD_DIM)
    d_query = unit_rows(activate(delta_query)) * HEAD_DIM ** (-0.5)
    d_key = unit_rows(activate(delta_key))
    d_value = activate(delta_value)
    gate_rows = rounded(project(delta_gate)).astype(jnp.float32).reshape(total_rows, DELTA_HEADS, HEAD_DIM)
    strength = jax.nn.sigmoid(project(beta_weight).reshape(total_rows, DELTA_HEADS, 2) + beta_shift.T)
    log_decay = -jnp.exp(decay_log.T) * jax.nn.softplus(project(decay_weight).reshape(total_rows, DELTA_HEADS, 2)) / total_rows
    forward = delta_recur(d_query, d_key, d_value, log_decay[:, :, 0], strength[:, :, 0])
    backward = jnp.flip(delta_recur(jnp.flip(d_query, 0), jnp.flip(d_key, 0), jnp.flip(d_value, 0), jnp.flip(log_decay[:, :, 1], 0), jnp.flip(strength[:, :, 1], 0)), 0)
    both_ways = forward + backward
    normed_out = both_ways * lax.rsqrt(lax.optimization_barrier(jnp.mean(both_ways * both_ways, axis=-1, keepdims=True)) + norm_eps) * out_gain
    y_delta = (normed_out * jax.nn.silu(gate_rows)).astype(jnp.bfloat16).reshape(total_rows, DELTA_HEADS * HEAD_DIM)
    summed = jnp.dot(y_attn, attn_out, preferred_element_type=jnp.float32) + jnp.dot(y_delta, delta_out, preferred_element_type=jnp.float32)
    return summed.astype(jnp.bfloat16)
```

```python
import jax
import jax.numpy as jnp
from jax import lax
from jax.experimental import pallas as pl
from jax.experimental.pallas import tpu as pltpu
from jax.sharding import PartitionSpec as P

HEAD_DIM = 64
WINDOW = 64
ROWS = 256
TOKENS = 4096
EPS = 1e-6
COPIES = 96
MESH = pl.DeviceIdType.MESH
F32 = jnp.float32
BF16 = jnp.bfloat16
NN = (((1,), (0,)), ((), ()))
NT = (((1,), (1,)), ((), ()))


def mm(a, b, dims=NN):
    return lax.dot_general(a, b, dims, preferred_element_type=F32)


def split(a):
    hi = a.astype(BF16)
    return hi, (a - hi.astype(F32)).astype(BF16)


def dot3(a, b):
    ah, al = split(a)
    bh, bl = split(b)
    return mm(ah, bh) + (mm(ah, bl) + mm(al, bh))


def dot3_deep(a, b):
    ah, al = split(a)
    bh, bl = split(b)
    return mm(jnp.concatenate([ah, ah, al], axis=1), jnp.concatenate([bh, bl, bh], axis=0))


def silu(v):
    return v * jax.nn.sigmoid(v)


def inverse(low, same):
    eye = jnp.where(same(0), 1.0, 0.0)
    d1 = jnp.where(same(4), low, 0.0)
    d2 = dot3(d1, d1)
    x = eye - d1
    x = x + dot3(x, d2)
    d4 = dot3(d2, d2)
    x = x + dot3(x, d4)
    d8 = dot3(d4, d4)
    x = x + dot3(x, d8)
    for k in range(4, 8):
        off = jnp.where(same(k + 1), low, 0.0) - jnp.where(same(k), low, 0.0)
        x = x - dot3(dot3(x, off), x)
    return x


def layer_kernel(
    tokens, gain, aq, ak, av, dq, dk, dv, dz, small, ogain, ao, do, sink, shift, dlog,
    out,
    tok, normed, stage, w1, w2, kv, mats, rowmats, hsend, hall, pbuf, prec, send_sem, recv_sem, own_sem,
):
    sp = lax.axis_index("sp")
    x = lax.axis_index("tp")
    c = lax.rem(sp, 2)
    b = lax.div(sp, 2)
    z = lax.div(b, 4)
    y = lax.rem(b, 4)
    o = 1 - c

    def m4(v):
        return lax.rem(v + 4, 4)

    def dev(zz, yy, cc, xx):
        return {"sp": (zz * 4 + yy) * 2 + cc, "tp": xx}

    def dev_x(d):
        return dev(z, y, c, m4(x + d))

    def dev_y(d):
        return dev(z, m4(y + d), c, x)

    def dev_z(d):
        return dev(m4(z + d), y, c, x)

    def dev_b(d):
        bb = lax.rem(b + d + 16, 16)
        return {"sp": bb * 2 + c, "tp": x}

    partner = dev(z, y, o, x)
    sent = []

    def send(src, dst, device, landed):
        i = len(sent)
        copy = pltpu.make_async_remote_copy(
            src_ref=src, dst_ref=dst, send_sem=send_sem.at[i], recv_sem=recv_sem.at[i],
            device_id=device, device_id_type=MESH,
        )
        copy.start()
        sent.append(copy)
        return pltpu.make_async_remote_copy(
            src_ref=landed, dst_ref=landed, send_sem=send_sem.at[i], recv_sem=recv_sem.at[i],
            device_id=device, device_id_type=MESH,
        )

    attn_t = ao[...].astype(F32).T.astype(BF16)
    delta_t = do[...].astype(F32).T.astype(BF16)
    for cc in range(2):
        cols = slice(64 * cc, 64 * cc + 64)
        stage[cc] = jnp.concatenate(
            [aq[:, cols], dq[:, cols], dk[:, cols], dv[:, cols], dz[:, cols], small[cc], ak[...], av[...],
             attn_t[:, cols], delta_t[:, cols]],
            axis=1,
        )
    w1[z, y, c] = stage[c, :, 0:512]

    barrier = pltpu.get_barrier_semaphore()
    peers = [partner]
    for d in (1, 2, 3):
        peers += [dev_x(d), dev_y(d), dev_z(d)]
    peers += [dev_b(1), dev_b(-1)]
    for peer in peers:
        pl.semaphore_signal(barrier, inc=1, device_id=peer, device_id_type=MESH)
    pl.semaphore_wait(barrier, len(peers))

    class Ring:
        def __init__(self, w, s, y_first):
            self.w, self.s, self.y_first = w, s, y_first

        def slot(self, first, half=None):
            zz, yy = (z, m4(y + first)) if self.y_first else (m4(z + first), y)
            ref = self.w.at[zz, yy, self.s]
            return ref if half is None else ref.at[pl.ds(16 * half, 16)]

        def line(self, second, half=None):
            rows = pl.ds(0, 32) if half is None else pl.ds(16 * half, 16)
            if self.y_first:
                return self.w.at[m4(z + second), :, self.s, rows]
            return self.w.at[:, m4(y + second), self.s, rows]

        def dev1(self, d):
            return dev_y(d) if self.y_first else dev_z(d)

        def dev2(self, d):
            return dev_z(d) if self.y_first else dev_y(d)

        def start1(self):
            self.up = send(self.slot(0), self.slot(0), self.dev1(1), self.slot(-1))
            self.down = send(self.slot(0), self.slot(0), self.dev1(-1), self.slot(1))

        def relay1(self):
            self.up.wait_recv()
            self.up2 = send(self.slot(-1, 0), self.slot(-1, 0), self.dev1(1), self.slot(-2, 0))
            self.down.wait_recv()
            self.down2 = send(self.slot(1, 1), self.slot(1, 1), self.dev1(-1), self.slot(2, 1))

        def start2(self):
            self.up2.wait_recv()
            self.down2.wait_recv()
            self.up = send(self.line(0), self.line(0), self.dev2(1), self.line(-1))
            self.down = send(self.line(0), self.line(0), self.dev2(-1), self.line(1))

        def relay2(self):
            self.up.wait_recv()
            self.up2 = send(self.line(-1, 0), self.line(-1, 0), self.dev2(1), self.line(-2, 0))
            self.down.wait_recv()
            self.down2 = send(self.line(1, 1), self.line(1, 1), self.dev2(-1), self.line(2, 1))

        def finish(self):
            self.up2.wait_recv()
            self.down2.wait_recv()

    half_rows = pl.ds(128 * c, 128)
    other_rows = pl.ds(128 * o, 128)
    in_cols = pl.ds(0, 512)
    out_cols = pl.ds(512, 128)
    x_cols = pl.ds(pl.multiple_of(128 * x, 128), 128)

    def x_cols_of(d):
        return pl.ds(pl.multiple_of(128 * m4(x + d), 128), 128)

    w_swap = send(stage.at[o, :, in_cols], w1.at[z, y, c], partner, w1.at[z, y, o])
    first = Ring(w1, c, True)
    second = Ring(w1, o, False)
    first.start1()
    tok_in = [send(tokens, tok.at[x, half_rows], dev_x(d), tok.at[m4(x - d), half_rows]) for d in (1, 3, 2)]
    tok_swap = [send(tokens, tok.at[x, half_rows], partner, tok.at[x, other_rows])]
    w2_swap = send(stage.at[o, :, out_cols], w2.at[z, y, c, :, x_cols], partner, w2.at[z, y, o, :, x_cols])
    own_tok = pltpu.make_async_copy(tokens, tok.at[x, half_rows], own_sem.at[0])
    own_tok.start()
    own_w2 = pltpu.make_async_copy(stage.at[c, :, out_cols], w2.at[z, y, c, :, x_cols], own_sem.at[1])
    own_w2.start()
    w_swap.wait_recv()
    second.start1()
    first.relay1()
    second.relay1()
    for d, arrived in zip((1, 3, 2), tok_in):
        arrived.wait_recv()
        src = m4(x - d)
        tok_swap.append(send(tok.at[src, half_rows], tok.at[src, half_rows], partner, tok.at[src, other_rows]))
    first.start2()
    second.start2()
    own_w2.wait()
    w2_swap.wait_recv()
    w2_in = [
        send(w2.at[z, y, :, :, x_cols], w2.at[z, y, :, :, x_cols], dev_x(d), w2.at[z, y, :, :, x_cols_of(-d)])
        for d in (1, 3, 2)
    ]
    own_tok.wait()
    for arrived in tok_swap:
        arrived.wait_recv()

    squares = jnp.zeros((ROWS, 1), F32)
    for k in range(4):
        wide = tok[k].astype(F32)
        squares = squares + jnp.sum(wide * wide, axis=-1, keepdims=True)
    inv = lax.rsqrt(squares * (1.0 / 1024.0) + EPS)
    for k in range(4):
        normed[k] = (tok[k].astype(F32) * inv * gain[:, 256 * k : 256 * k + 256]).astype(BF16)

    first.relay2()
    second.relay2()
    first.finish()
    second.finish()
    for arrived in w2_in:
        arrived.wait_recv()
    out_first = Ring(w2, c, True)
    out_second = Ring(w2, o, False)
    out_first.start1()
    out_second.start1()

    proj = mm(normed[0], w1[0].reshape(256, 512))
    for k in range(1, 4):
        proj = proj + mm(normed[k], w1[k].reshape(256, 512))
    t0, t1, t2 = proj[:, 0:128], proj[:, 128:256], proj[:, 256:384]
    kv[64:320, :] = proj[:, 384:512].astype(BF16)
    halo = [
        send(kv.at[pl.ds(256, 64)], kv.at[pl.ds(0, 64)], dev_b(1), kv.at[pl.ds(0, 64)]),
        send(kv.at[pl.ds(64, 64)], kv.at[pl.ds(320, 64)], dev_b(-1), kv.at[pl.ds(320, 64)]),
    ]
    att_q = t0[:, 0:64].astype(BF16)
    act_q = silu(t0[:, 64:128].astype(BF16).astype(F32))
    act_kv = silu(t1.astype(BF16).astype(F32))
    act_k, val = act_kv[:, 0:64], act_kv[:, 64:128]
    q = act_q * lax.rsqrt(jnp.sum(act_q * act_q, axis=-1, keepdims=True) + EPS) * HEAD_DIM**-0.5
    key = act_k * lax.rsqrt(jnp.sum(act_k * act_k, axis=-1, keepdims=True) + EPS)
    gate = silu(t2[:, 0:64].astype(BF16).astype(F32))

    lane = lax.broadcasted_iota(jnp.int32, (1, 128), 1)
    bias = jnp.where(lane == 64, shift[0, c], jnp.where(lane == 65, shift[1, c], 0.0))
    rate = jnp.exp(jnp.where(lane == 66, dlog[0, c], jnp.where(lane == 67, dlog[1, c], 0.0)))
    strength = jax.nn.sigmoid(t2 + bias)
    softplus = jnp.maximum(t2, 0.0) + jnp.log1p(jnp.exp(-jnp.abs(t2)))
    decay = jnp.where((lane == 66) | (lane == 67), -rate * softplus * (1.0 / TOKENS), 0.0)

    row = lax.broadcasted_iota(jnp.int32, (ROWS, ROWS), 0)
    col = lax.broadcasted_iota(jnp.int32, (ROWS, ROWS), 1)
    lower = row >= col
    upper = row <= col

    def same(k):
        return lax.shift_right_logical(row, k) == lax.shift_right_logical(col, k)

    g_hi = decay.astype(BF16)
    rest = decay - g_hi.astype(F32)
    g_mid = rest.astype(BF16)
    g_lo = (rest - g_mid.astype(F32)).astype(BF16)
    g_parts = jnp.concatenate([g_hi[:, 64:128], g_mid[:, 64:128], g_lo[:, 64:128]], axis=1)
    both = []
    for mask in (lower, upper):
        s = mm(jnp.where(mask, 1.0, 0.0).astype(BF16), g_parts)
        both.append(s[:, 0:64] + s[:, 64:128] + s[:, 128:192])
    sub = lax.broadcasted_iota(jnp.int32, (1, 64), 1)
    g_all = jnp.where(sub == 2, both[0], both[1])
    turned = jnp.concatenate([key, g_all], axis=1).T
    key_t = turned[0:64]
    key_h, key_l = split(key)
    q_h, q_l = split(q)
    kt_h, kt_l = split(key_t)
    pairs = mm(
        jnp.concatenate(
            [jnp.concatenate([q_h, q_h, q_l], axis=1), jnp.concatenate([key_h, key_h, key_l], axis=1)], axis=0
        ),
        jnp.concatenate([kt_h, kt_l, kt_h], axis=0),
    )
    qk, kk = pairs[0:ROWS], pairs[ROWS:]

    lane2 = lax.broadcasted_iota(jnp.int32, (64, 128), 1)
    row2 = lax.broadcasted_iota(jnp.int32, (64, 128), 0)
    eye2 = jnp.where(lane2 == row2 + 64, 1.0, 0.0)
    local, reads = [], []
    for way, mask in ((0, lower), (1, upper)):
        beta = strength[:, 64 + way : 65 + way]
        g_col = g_all[:, 2 + way : 3 + way]
        g_row = turned[66 + way : 67 + way]
        g_end = g_col[ROWS - 1 : ROWS] if way == 0 else g_col[0:1]
        decays = jnp.exp(jnp.where(mask, g_col - g_row, -jnp.inf))
        low = jnp.where(row == col, 0.0, beta * kk * decays)
        t_inv = inverse(low, same)
        grown = jnp.exp(g_col)
        uw = dot3(t_inv, jnp.concatenate([beta * val, (beta * grown) * key], axis=1))
        read = dot3(qk * decays, uw)
        local.append(read[:, 0:64])
        reads.append(grown * q - read[:, 64:128])
        final = dot3(key_t * jnp.exp(g_end - g_row), uw)
        mats[y, way] = jnp.where(lane2 < 64, final, jnp.exp(g_end) * eye2 - final)
    scan1 = [send(mats.at[y], mats.at[y], dev_y(d), mats.at[m4(y - d)]) for d in (1, 3, 2)]

    out_first.relay1()
    out_second.relay1()

    for arrived in halo:
        arrived.wait_recv()
    scores = mm(att_q, kv[:, 0:64], NT) * HEAD_DIM**-0.5
    q_pos = lax.broadcasted_iota(jnp.int32, (ROWS, ROWS + 2 * WINDOW), 0)
    k_pos = lax.broadcasted_iota(jnp.int32, (ROWS, ROWS + 2 * WINDOW), 1) - WINDOW
    seen = k_pos + b * ROWS
    allowed = (jnp.abs(q_pos - k_pos) <= WINDOW) & (seen >= 0) & (seen < TOKENS)
    scores = jnp.where(allowed, scores, -jnp.inf)
    top = jnp.maximum(jnp.max(scores, axis=-1, keepdims=True), sink[c])
    weights = jnp.exp(scores - top)
    total = jnp.sum(weights, axis=-1, keepdims=True) + jnp.exp(sink[c] - top)
    weights = (weights / total).astype(BF16)
    attn_heads = mm(weights, kv[:, 64:128])

    out_first.start2()
    out_second.start2()

    for arrived in scan1:
        arrived.wait_recv()

    def after(later, earlier):
        return dot3_deep(later[:, 64:128], earlier) + jnp.where(lane2 < 64, later, 0.0)

    entry = []
    for way in range(2):
        m = [mats[k if way == 0 else 3 - k, way] for k in range(4)]
        place = y if way == 0 else 3 - y
        two = after(m[1], m[0])
        three = after(m[2], two)
        rowmats[z, way] = after(after(m[3], m[2]), two)
        entry.append(
            jnp.where(place == 0, eye2, jnp.where(place == 1, m[0], jnp.where(place == 2, two, three)))
        )
    scan2 = [send(rowmats.at[z], rowmats.at[z], dev_z(d), rowmats.at[m4(z - d)]) for d in (1, 3, 2)]
    out_first.relay2()
    out_second.relay2()
    for arrived in scan2:
        arrived.wait_recv()
    states = []
    for way in range(2):
        m = [rowmats[k if way == 0 else 3 - k, way] for k in range(3)]
        place = z if way == 0 else 3 - z
        s1 = m[0][:, 0:64]
        s2 = dot3_deep(m[1][:, 64:128], s1) + m[1][:, 0:64]
        s3 = dot3_deep(m[2][:, 64:128], s2) + m[2][:, 0:64]
        s = jnp.where(place == 0, 0.0, jnp.where(place == 1, s1, jnp.where(place == 2, s2, s3)))
        states.append(dot3_deep(entry[way][:, 64:128], s) + entry[way][:, 0:64])

    whole = local[0] + local[1] + dot3(jnp.concatenate(reads, axis=1), jnp.concatenate(states, axis=0))
    scaled = whole * lax.rsqrt(jnp.mean(whole * whole, axis=-1, keepdims=True) + EPS) * ogain[...]
    heads = jnp.concatenate([attn_heads, scaled * gate], axis=1).astype(BF16)
    for k in range(4):
        hsend[k, 0:32] = heads[32 * k : 32 * k + 32]
        hsend[k, 32:64] = heads[128 + 32 * k : 160 + 32 * k]
    head_in = [send(hsend.at[m4(x + d)], hall.at[x], dev_x(d), hall.at[m4(x - d)]) for d in (1, 3, 2)]
    hall[x] = hsend[x]
    out_first.finish()
    out_second.finish()
    for arrived in head_in:
        arrived.wait_recv()
    gathered = jnp.concatenate([hall[k] for k in range(4)], axis=1)
    for k in range(4):
        part = mm(gathered, w2[k].reshape(256, 512), NT)
        pbuf[0, :, 256 * k : 256 * k + 256] = part[0:32]
        pbuf[1, :, 256 * k : 256 * k + 256] = part[32:64]
    last = send(pbuf.at[o], prec, partner, prec)
    last.wait_recv()
    out[...] = (pbuf[c] + prec[...]).astype(BF16)
    for copy in sent:
        copy.wait_send()


def per_device(
    tokens, norm_gain, attn_query, attn_key, attn_value, sink_logit, delta_query, delta_key, delta_value,
    delta_gate, beta_weight, decay_weight, beta_shift, decay_log, out_gain, attn_out, delta_out,
):
    small = jnp.concatenate([beta_weight, decay_weight], axis=2).transpose(1, 0, 2)
    small = jnp.pad(small, ((0, 0), (0, 0), (0, 60)))
    vmem = pl.BlockSpec(memory_space=pltpu.VMEM)
    smem = pl.BlockSpec(memory_space=pltpu.SMEM)
    return pl.pallas_call(
        layer_kernel,
        out_shape=jax.ShapeDtypeStruct((32, 1024), BF16),
        in_specs=[vmem] * 13 + [smem] * 3,
        out_specs=vmem,
        scratch_shapes=[
            pltpu.VMEM((4, 256, 256), BF16),
            pltpu.VMEM((4, 256, 256), BF16),
            pltpu.VMEM((2, 32, 640), BF16),
            pltpu.VMEM((4, 4, 2, 32, 512), BF16),
            pltpu.VMEM((4, 4, 2, 32, 512), BF16),
            pltpu.VMEM((384, 128), BF16),
            pltpu.VMEM((4, 2, 64, 128), F32),
            pltpu.VMEM((4, 2, 64, 128), F32),
            pltpu.VMEM((4, 64, 128), BF16),
            pltpu.VMEM((4, 64, 128), BF16),
            pltpu.VMEM((2, 32, 1024), F32),
            pltpu.VMEM((32, 1024), F32),
            pltpu.SemaphoreType.DMA((COPIES,)),
            pltpu.SemaphoreType.DMA((COPIES,)),
            pltpu.SemaphoreType.DMA((2,)),
        ],
        compiler_params=pltpu.CompilerParams(collective_id=0, has_side_effects=True),
    )(
        tokens, norm_gain.reshape(1, -1), attn_query, attn_key, attn_value, delta_query, delta_key, delta_value,
        delta_gate, small, out_gain.reshape(1, -1), attn_out, delta_out, sink_logit, beta_shift, decay_log,
    )


def solution(mesh):
    return jax.shard_map(
        per_device,
        mesh=mesh,
        in_specs=(
            P("sp", "tp"), P(), P("sp", "tp"), P("sp", "tp"), P("sp", "tp"), P("tp"), P("sp", "tp"),
            P("sp", "tp"), P("sp", "tp"), P("sp", "tp"), P("sp", "tp", None), P("sp", "tp", None),
            P(None, "tp"), P(None, "tp"), P(), P("tp", "sp"), P("tp", "sp"),
        ),
        out_specs=P(("sp", "tp"), None),
        check_vma=False,
    )
```

```python
import jax
import jax.numpy as jnp
from jax import lax
from jax.experimental import pallas as pl
from jax.experimental.pallas import tpu as pltpu
from jax.sharding import PartitionSpec as P

HEAD_DIM = 64
WINDOW = 64
ROWS = 256
TOKENS = 4096
EPS = 1e-6
COPIES = 120
MESH = pl.DeviceIdType.MESH
F32 = jnp.float32
BF16 = jnp.bfloat16
LINK = F32
NN = (((1,), (0,)), ((), ()))
NT = (((1,), (1,)), ((), ()))


def mm(a, b, dims=NN):
    return lax.dot_general(a, b, dims, preferred_element_type=F32)


def split(a):
    hi = a.astype(BF16)
    return hi, (a - hi.astype(F32)).astype(BF16)


def left(a):
    hi, lo = split(a)
    return jnp.concatenate([hi, lo], axis=1)


def right(b):
    hi, lo = split(b)
    return jnp.concatenate(
        [jnp.concatenate([hi, lo], axis=1), jnp.concatenate([hi, jnp.zeros_like(lo)], axis=1)], axis=0
    )


def dot3(a, b):
    both = mm(left(a), right(b))
    return both[:, 0:128] + both[:, 128:256]


def dot3_deep(a, b):
    ah, al = split(a)
    bh, bl = split(b)
    return mm(jnp.concatenate([ah, ah, al], axis=1), jnp.concatenate([bh, bl, bh], axis=0))


def silu(v):
    return v * jax.nn.sigmoid(v)


def layer_kernel(
    tokens, gain, aq, ak, av, dq, dk, dv, dz, bw, gw, ogain, ao, do, sink, shift, dlog,
    out,
    tok, normed, stage, w1, w2, kv, mats, rowmats, hsend, hall, pbuf, prec, send_sem, recv_sem, own_sem,
):
    sp = lax.axis_index("sp")
    x = lax.axis_index("tp")
    c = lax.rem(sp, 2)
    b = lax.div(sp, 2)
    z = lax.div(b, 4)
    y = lax.rem(b, 4)
    o = 1 - c

    open_scopes = []

    def phase(name):
        while open_scopes:
            open_scopes.pop().__exit__(None, None, None)
        if name:
            open_scopes.append(jax.named_scope(name))
            open_scopes[0].__enter__()

    def m4(v):
        return lax.rem(v + 4, 4)

    def dev(zz, yy, cc, xx):
        return {"sp": (zz * 4 + yy) * 2 + cc, "tp": xx}

    def dev_x(d):
        return dev(z, y, c, m4(x + d))

    def dev_y(d):
        return dev(z, m4(y + d), c, x)

    def dev_z(d):
        return dev(m4(z + d), y, c, x)

    def dev_b(d):
        bb = lax.rem(b + d + 16, 16)
        return {"sp": bb * 2 + c, "tp": x}

    partner = dev(z, y, o, x)
    sent = []

    def send(src, dst, device, landed):
        i = len(sent)
        copy = pltpu.make_async_remote_copy(
            src_ref=src, dst_ref=dst, send_sem=send_sem.at[i], recv_sem=recv_sem.at[i],
            device_id=device, device_id_type=MESH,
        )
        copy.start()
        sent.append(copy)
        return pltpu.make_async_remote_copy(
            src_ref=landed, dst_ref=landed, send_sem=send_sem.at[i], recv_sem=recv_sem.at[i],
            device_id=device, device_id_type=MESH,
        )

    phase("pack")
    attn_t, delta_t = ao[...], do[...]
    blank = jnp.zeros((60, 32), F32)
    for cc in range(2):
        cols = slice(64 * cc, 64 * cc + 64)
        small = jnp.concatenate([bw[cc].astype(F32), gw[cc].astype(F32), blank], axis=0).T.astype(BF16)
        stage[cc] = jnp.concatenate(
            [aq[:, cols], dq[:, cols], dk[:, cols], dv[:, cols], dz[:, cols], small, ak[...], av[...],
             attn_t[:, cols], delta_t[:, cols]],
            axis=1,
        )
    w1[z, y, c] = stage[c, :, 0:512]

    phase("barrier")
    barrier = pltpu.get_barrier_semaphore()
    peers = [partner]
    for d in (1, 2, 3):
        peers += [dev_x(d), dev_y(d), dev_z(d)]
    peers += [dev_b(1), dev_b(-1)]
    for peer in peers:
        pl.semaphore_signal(barrier, inc=1, device_id=peer, device_id_type=MESH)
    pl.semaphore_wait(barrier, len(peers))

    class Ring:
        def __init__(self, w, s, y_first):
            self.w, self.s, self.y_first = w, s, y_first
            self.waits = {}

        def slot(self, first, second, half=None):
            zz, yy = (z + second, y + first) if self.y_first else (z + first, y + second)
            ref = self.w.at[m4(zz), m4(yy), self.s]
            return ref if half is None else ref.at[pl.ds(16 * half, 16)]

        def dev1(self, d):
            return dev_y(d) if self.y_first else dev_z(d)

        def dev2(self, d):
            return dev_z(d) if self.y_first else dev_y(d)

        def across(self, f):
            for d in (1, -1):
                block = self.slot(f, 0)
                self.waits[f, d] = send(block, block, self.dev2(d), self.slot(f, -d))

        def relay(self, f):
            for d, half in ((1, 0), (-1, 1)):
                self.waits[f, d].wait_recv()
                block = self.slot(f, -d, half)
                self.waits[f, 2 * d] = send(block, block, self.dev2(d), self.slot(f, -2 * d, half))

        def begin(self):
            block = self.slot(0, 0)
            for d in (1, -1):
                self.waits[d] = send(block, block, self.dev1(d), self.slot(-d, 0))

        def near(self):
            for d, half in ((1, 0), (-1, 1)):
                self.waits[d].wait_recv()
                block = self.slot(-d, 0, half)
                self.waits[2 * d] = send(block, block, self.dev1(d), self.slot(-2 * d, 0, half))
            self.across(-1)
            self.across(1)

        def far(self):
            self.waits[2].wait_recv()
            self.waits[-2].wait_recv()
            self.across(2)

        def finish(self):
            for f in (0, -1, 1, 2):
                self.waits[f, 2].wait_recv()
                self.waits[f, -2].wait_recv()

    half_rows = pl.ds(128 * c, 128)
    other_rows = pl.ds(128 * o, 128)
    in_cols = pl.ds(0, 512)
    out_cols = pl.ds(512, 128)
    x_cols = pl.ds(pl.multiple_of(128 * x, 128), 128)

    def x_cols_of(d):
        return pl.ds(pl.multiple_of(128 * m4(x + d), 128), 128)

    phase("start")
    first = Ring(w1, c, True)
    second = Ring(w1, o, False)
    out_first = Ring(w2, c, True)
    out_second = Ring(w2, o, False)
    w_swap = send(stage.at[o, :, in_cols], w1.at[z, y, c], partner, w1.at[z, y, o])
    first.begin()
    tok_in = [send(tokens, tok.at[x, half_rows], dev_x(d), tok.at[m4(x - d), half_rows]) for d in (1, 3, 2)]
    tok_swap = [send(tokens, tok.at[x, half_rows], partner, tok.at[x, other_rows])]
    w2_swap = send(stage.at[o, :, out_cols], w2.at[z, y, c, :, x_cols], partner, w2.at[z, y, o, :, x_cols])
    first.across(0)
    own_tok = pltpu.make_async_copy(tokens, tok.at[x, half_rows], own_sem.at[0])
    own_tok.start()
    own_w2 = pltpu.make_async_copy(stage.at[c, :, out_cols], w2.at[z, y, c, :, x_cols], own_sem.at[1])
    own_w2.start()
    phase("swap")
    w_swap.wait_recv()
    second.begin()
    second.across(0)
    own_w2.wait()
    w2_swap.wait_recv()
    w2_in = [
        send(w2.at[z, y, :, :, x_cols], w2.at[z, y, :, :, x_cols], dev_x(d), w2.at[z, y, :, :, x_cols_of(-d)])
        for d in (1, 3, 2)
    ]
    phase("near")
    first.near()
    second.near()
    phase("tokens")
    for d, arrived in zip((1, 3, 2), tok_in):
        arrived.wait_recv()
        src = m4(x - d)
        tok_swap.append(send(tok.at[src, half_rows], tok.at[src, half_rows], partner, tok.at[src, other_rows]))
    phase("relay0")
    first.relay(0)
    second.relay(0)
    phase("far")
    first.far()
    second.far()
    phase("tokswap")
    own_tok.wait()
    for arrived in tok_swap:
        arrived.wait_recv()

    phase("norm")
    squares = jnp.zeros((ROWS, 1), F32)
    for k in range(4):
        wide = tok[k].astype(F32)
        squares = squares + jnp.sum(wide * wide, axis=-1, keepdims=True)
    inv = lax.rsqrt(squares * (1.0 / 1024.0) + EPS)
    for k in range(4):
        normed[k] = (tok[k].astype(F32) * inv * gain[:, 256 * k : 256 * k + 256]).astype(BF16)

    phase("relay1")
    for f in (-1, 1):
        first.relay(f)
        second.relay(f)
    phase("relay2")
    first.relay(2)
    second.relay(2)
    for arrived in w2_in:
        arrived.wait_recv()
    for ring in (out_first, out_second):
        ring.begin()
        ring.across(0)
    phase("wfinish")
    first.finish()
    second.finish()

    phase("proj")
    proj = mm(normed[0], w1[0].reshape(256, 512))
    for k in range(1, 4):
        proj = proj + mm(normed[k], w1[k].reshape(256, 512))
    t0, t1, t2 = proj[:, 0:128], proj[:, 128:256], proj[:, 256:384]
    kv[64:320, :] = proj[:, 384:512].astype(BF16)
    halo = [
        send(kv.at[pl.ds(256, 64)], kv.at[pl.ds(0, 64)], dev_b(1), kv.at[pl.ds(0, 64)]),
        send(kv.at[pl.ds(64, 64)], kv.at[pl.ds(320, 64)], dev_b(-1), kv.at[pl.ds(320, 64)]),
    ]
    att_q = t0[:, 0:64].astype(BF16)
    act_q = silu(t0[:, 64:128].astype(BF16).astype(F32))
    act_kv = silu(t1.astype(BF16).astype(F32))
    act_k, val = act_kv[:, 0:64], act_kv[:, 64:128]
    q = act_q * lax.rsqrt(jnp.sum(act_q * act_q, axis=-1, keepdims=True) + EPS) * HEAD_DIM**-0.5
    key = act_k * lax.rsqrt(jnp.sum(act_k * act_k, axis=-1, keepdims=True) + EPS)
    gate = silu(t2[:, 0:64].astype(BF16).astype(F32))

    phase("gates")
    lane = lax.broadcasted_iota(jnp.int32, (1, 128), 1)
    bias = jnp.where(lane == 64, shift[0, c], jnp.where(lane == 65, shift[1, c], 0.0))
    rate = jnp.exp(jnp.where(lane == 66, dlog[0, c], jnp.where(lane == 67, dlog[1, c], 0.0)))
    strength = jax.nn.sigmoid(t2 + bias)
    softplus = jnp.maximum(t2, 0.0) + jnp.log1p(jnp.exp(-jnp.abs(t2)))
    decay = jnp.where((lane == 66) | (lane == 67), -rate * softplus * (1.0 / TOKENS), 0.0)

    row = lax.broadcasted_iota(jnp.int32, (128, 128), 0)
    col = lax.broadcasted_iota(jnp.int32, (128, 128), 1)
    masks = (row >= col, row <= col)
    unit = jnp.where(row == col, 1.0, 0.0)
    near16 = lax.shift_right_logical(row, 4) == lax.shift_right_logical(col, 4)

    g_hi = decay.astype(BF16)
    rest = decay - g_hi.astype(F32)
    g_mid = rest.astype(BF16)
    g_lo = (rest - g_mid.astype(F32)).astype(BF16)
    g_parts = jnp.concatenate(
        [part[128 * h : 128 * h + 128, 64:128] for h in range(2) for part in (g_hi, g_mid, g_lo)], axis=1
    )
    sums = [mm(jnp.where(mask, 1.0, 0.0).astype(BF16), g_parts) for mask in masks]
    sub = lax.broadcasted_iota(jnp.int32, (1, 192), 1)
    picked = jnp.where((sub & 63) == 2, sums[0][:, 0:192], sums[1][:, 0:192])
    picked2 = jnp.where((sub & 63) == 2, sums[0][:, 192:384], sums[1][:, 192:384])
    g_all = jnp.concatenate([p[:, 0:64] + p[:, 64:128] + p[:, 128:192] for p in (picked, picked2)], axis=0)
    turned = jnp.concatenate([key, g_all], axis=1).T
    key_t = turned[0:64]
    key_h, key_l = split(key)
    q_h, q_l = split(q)
    kt_h, kt_l = split(key_t)
    q3 = jnp.concatenate([q_h, q_h, q_l], axis=1)
    key3 = jnp.concatenate([key_h, key_h, key_l], axis=1)
    kt3 = jnp.concatenate([kt_h, kt_l, kt_h], axis=0)

    phase("rings1")
    out_first.near()
    out_second.near()

    phase("delta1")
    lane2 = lax.broadcasted_iota(jnp.int32, (64, 128), 1)
    row2 = lax.broadcasted_iota(jnp.int32, (64, 128), 0)
    eye2 = jnp.where(lane2 == row2 + 64, 1.0, 0.0)
    chains = [(way, h) for way in range(2) for h in range(2)]
    low, scores_d, sides, grown, key_end, end, d = {}, {}, {}, {}, {}, {}, {}
    for h in range(2):
        hs = slice(128 * h, 128 * h + 128)
        pairs = mm(jnp.concatenate([q3[hs], key3[hs]], axis=0), kt3[:, hs])
        for way in range(2):
            at = way, h
            beta = strength[hs, 64 + way : 65 + way]
            g_col = g_all[hs, 2 + way : 3 + way]
            g_row = turned[66 + way : 67 + way, hs]
            g_end = g_col[127:128] if way == 0 else g_col[0:1]
            decays = jnp.exp(jnp.where(masks[way], g_col - g_row, -jnp.inf))
            low[at] = jnp.where(row == col, 0.0, beta * pairs[128:256] * decays)
            scores_d[at] = pairs[0:128] * decays
            up = jnp.exp(g_col)
            grown[at] = up * q[hs]
            sides[at] = jnp.concatenate([beta * val[hs], (beta * up) * key[hs]], axis=1)
            key_end[at] = key_t[:, hs] * jnp.exp(g_end - g_row)
            end[at] = jnp.exp(g_end)
    d1 = {at: jnp.where(near16, low[at], 0.0) for at in chains}
    off = {at: jnp.where(near16, 0.0, low[at]) for at in chains}
    d2 = {at: dot3(d1[at], d1[at]) for at in chains}
    inner = {at: unit - d1[at] for at in chains}
    d4 = {at: dot3(d2[at], d2[at]) for at in chains}
    inner = {at: inner[at] + dot3(inner[at], d2[at]) for at in chains}
    d8 = {at: dot3(d4[at], d4[at]) for at in chains}
    inner = {at: inner[at] + dot3(inner[at], d4[at]) for at in chains}
    inner = {at: inner[at] + dot3(inner[at], d8[at]) for at in chains}
    phase("rings2")
    out_first.relay(0)
    out_second.relay(0)
    out_first.far()
    out_second.far()
    phase("delta2")
    m1 = {at: dot3(inner[at], off[at]) for at in chains}
    uw = {at: dot3(inner[at], sides[at]) for at in chains}
    m2 = {at: dot3(m1[at], m1[at]) for at in chains}
    uw = {at: uw[at] - dot3(m1[at], uw[at]) for at in chains}
    m4_ = {at: dot3(m2[at], m2[at]) for at in chains}
    uw = {at: uw[at] + dot3(m2[at], uw[at]) for at in chains}
    uw = {at: uw[at] + dot3(m4_[at], uw[at]) for at in chains}
    phase("rings3")
    for f in (-1, 1, 2):
        out_first.relay(f)
        out_second.relay(f)
    phase("final")

    def after(later, earlier):
        return dot3_deep(later[:, 64:128], earlier) + jnp.where(lane2 < 64, later, 0.0)

    maps = {}
    for at in chains:
        final = dot3(key_end[at], uw[at])
        maps[at] = jnp.where(lane2 < 64, final, end[at] * eye2 - final)
    for way in range(2):
        block_map = after(maps[way, 1 - way], maps[way, way])
        mats[y, way] = (block_map - eye2).astype(LINK)
    phase("scan1send")
    scan1 = [send(mats.at[y], mats.at[y], dev_y(d), mats.at[m4(y - d)]) for d in (1, 3, 2)]

    phase("reads")
    local, reads = {}, {}
    for way, h in chains:
        at = way, h
        read = dot3(scores_d[at], uw[at])
        local[at] = read[:, 0:64]
        reads[at] = grown[at] - read[:, 64:128]
        if h != way:
            passed = dot3_deep(reads[at], maps[way, way])
            local[at] = local[at] + passed[:, 0:64]
            reads[at] = passed[:, 64:128]
    local_sum = jnp.concatenate([local[0, h] + local[1, h] for h in range(2)], axis=0)
    reads_all = jnp.concatenate(
        [jnp.concatenate([reads[0, h], reads[1, h]], axis=1) for h in range(2)], axis=0
    )

    phase("halo")
    for arrived in halo:
        arrived.wait_recv()
    phase("attn")
    scores = mm(att_q, kv[:, 0:64], NT) * HEAD_DIM**-0.5
    q_pos = lax.broadcasted_iota(jnp.int32, (ROWS, ROWS + 2 * WINDOW), 0)
    k_pos = lax.broadcasted_iota(jnp.int32, (ROWS, ROWS + 2 * WINDOW), 1) - WINDOW
    seen = k_pos + b * ROWS
    allowed = (jnp.abs(q_pos - k_pos) <= WINDOW) & (seen >= 0) & (seen < TOKENS)
    scores = jnp.where(allowed, scores, -jnp.inf)
    top = jnp.maximum(jnp.max(scores, axis=-1, keepdims=True), sink[c])
    weights = jnp.exp(scores - top)
    total = jnp.sum(weights, axis=-1, keepdims=True) + jnp.exp(sink[c] - top)
    weights = (weights / total).astype(BF16)
    attn_heads = mm(weights, kv[:, 64:128])

    phase("scan1wait")
    for arrived in scan1:
        arrived.wait_recv()

    phase("compose")
    entry = []
    for way in range(2):
        m = [mats[k if way == 0 else 3 - k, way].astype(F32) + eye2 for k in range(4)]
        place = y if way == 0 else 3 - y
        two = after(m[1], m[0])
        three = after(m[2], two)
        rowmats[z, way] = (after(after(m[3], m[2]), two) - eye2).astype(LINK)
        entry.append(
            jnp.where(place == 0, eye2, jnp.where(place == 1, m[0], jnp.where(place == 2, two, three)))
        )
    phase("scan2send")
    scan2 = [send(rowmats.at[z], rowmats.at[z], dev_z(d), rowmats.at[m4(z - d)]) for d in (1, 3, 2)]
    phase("scan2wait")
    for arrived in scan2:
        arrived.wait_recv()
    phase("states")
    states = []
    for way in range(2):
        m = [rowmats[k if way == 0 else 3 - k, way].astype(F32) + eye2 for k in range(3)]
        place = z if way == 0 else 3 - z
        s1 = m[0][:, 0:64]
        s2 = dot3_deep(m[1][:, 64:128], s1) + m[1][:, 0:64]
        s3 = dot3_deep(m[2][:, 64:128], s2) + m[2][:, 0:64]
        s = jnp.where(place == 0, 0.0, jnp.where(place == 1, s1, jnp.where(place == 2, s2, s3)))
        states.append(dot3_deep(entry[way][:, 64:128], s) + entry[way][:, 0:64])

    reads_h, reads_l = split(reads_all)
    states_h, states_l = split(jnp.concatenate(states, axis=0))
    whole = mm(
        jnp.concatenate([reads_h, reads_l], axis=1),
        jnp.concatenate([states_h, states_h], axis=0),
    )
    whole = local_sum + whole + mm(reads_h, states_l)
    scaled = whole * lax.rsqrt(jnp.mean(whole * whole, axis=-1, keepdims=True) + EPS) * ogain[...]
    heads = jnp.concatenate([attn_heads, scaled * gate], axis=1).astype(BF16)
    for k in range(4):
        hsend[k, 0:32] = heads[32 * k : 32 * k + 32]
        hsend[k, 32:64] = heads[128 + 32 * k : 160 + 32 * k]
    phase("headsend")
    head_in = [send(hsend.at[m4(x + d)], hall.at[x], dev_x(d), hall.at[m4(x - d)]) for d in (1, 3, 2)]
    hall[x] = hsend[x]
    phase("w2finish")
    out_first.finish()
    out_second.finish()
    phase("headwait")
    for arrived in head_in:
        arrived.wait_recv()
    phase("outmm")
    gathered = jnp.concatenate([hall[k] for k in range(4)], axis=1)
    for k in range(4):
        part = mm(gathered, w2[k].reshape(256, 512), NT)
        pbuf[0, :, 256 * k : 256 * k + 256] = part[0:32]
        pbuf[1, :, 256 * k : 256 * k + 256] = part[32:64]
    phase("last")
    last = send(pbuf.at[o], prec, partner, prec)
    last.wait_recv()
    out[...] = pbuf[c] + prec[...]
    phase("drain")
    for copy in sent:
        copy.wait_send()
    phase(None)


def per_device(
    tokens, norm_gain, attn_query, attn_key, attn_value, sink_logit, delta_query, delta_key, delta_value,
    delta_gate, beta_weight, decay_weight, beta_shift, decay_log, out_gain, attn_out, delta_out,
):
    vmem = pl.BlockSpec(memory_space=pltpu.VMEM)
    smem = pl.BlockSpec(memory_space=pltpu.SMEM)
    summed = pl.pallas_call(
        layer_kernel,
        out_shape=jax.ShapeDtypeStruct((32, 1024), F32),
        in_specs=[vmem] * 14 + [smem] * 3,
        out_specs=vmem,
        scratch_shapes=[
            pltpu.VMEM((4, 256, 256), BF16),
            pltpu.VMEM((4, 256, 256), BF16),
            pltpu.VMEM((2, 32, 640), BF16),
            pltpu.VMEM((4, 4, 2, 32, 512), BF16),
            pltpu.VMEM((4, 4, 2, 32, 512), BF16),
            pltpu.VMEM((384, 128), BF16),
            pltpu.VMEM((4, 2, 64, 128), LINK),
            pltpu.VMEM((4, 2, 64, 128), LINK),
            pltpu.VMEM((4, 64, 128), BF16),
            pltpu.VMEM((4, 64, 128), BF16),
            pltpu.VMEM((2, 32, 1024), F32),
            pltpu.VMEM((32, 1024), F32),
            pltpu.SemaphoreType.DMA((COPIES,)),
            pltpu.SemaphoreType.DMA((COPIES,)),
            pltpu.SemaphoreType.DMA((2,)),
        ],
        compiler_params=pltpu.CompilerParams(collective_id=0, has_side_effects=True, vmem_limit_bytes=24 * 2**20),
    )(
        tokens, norm_gain.reshape(1, -1), attn_query, attn_key, attn_value, delta_query, delta_key, delta_value,
        delta_gate, beta_weight.transpose(1, 2, 0), decay_weight.transpose(1, 2, 0), out_gain.reshape(1, -1),
        attn_out.T, delta_out.T, sink_logit, beta_shift, decay_log,
    )
    return summed.astype(BF16)


def solution(mesh):
    return jax.shard_map(
        per_device,
        mesh=mesh,
        in_specs=(
            P("sp", "tp"), P(), P("sp", "tp"), P("sp", "tp"), P("sp", "tp"), P("tp"), P("sp", "tp"),
            P("sp", "tp"), P("sp", "tp"), P("sp", "tp"), P("sp", "tp", None), P("sp", "tp", None),
            P(None, "tp"), P(None, "tp"), P(), P("tp", "sp"), P("tp", "sp"),
        ),
        out_specs=P(("sp", "tp"), None),
        check_vma=False,
    )
```

```python
import jax
import jax.numpy as jnp
from jax import lax
from jax.experimental import pallas as pl
from jax.experimental.pallas import tpu as pltpu
from jax.sharding import PartitionSpec as P

HEAD_DIM = 64
WINDOW = 64
ROWS = 256
TOKENS = 4096
EPS = 1e-6
COPIES = 120
MESH = pl.DeviceIdType.MESH
F32 = jnp.float32
BF16 = jnp.bfloat16
LINK = F32
NN = (((1,), (0,)), ((), ()))
NT = (((1,), (1,)), ((), ()))


def mm(a, b, dims=NN):
    return lax.dot_general(a, b, dims, preferred_element_type=F32)


def split(a):
    hi = a.astype(BF16)
    return hi, (a - hi.astype(F32)).astype(BF16)


def left(a):
    hi, lo = split(a)
    return jnp.concatenate([hi, lo], axis=1)


def right(b):
    hi, lo = split(b)
    return jnp.concatenate(
        [jnp.concatenate([hi, lo], axis=1), jnp.concatenate([hi, jnp.zeros_like(lo)], axis=1)], axis=0
    )


def dot3(a, b):
    both = mm(left(a), right(b))
    return both[:, 0:128] + both[:, 128:256]


def dot3_deep(a, b):
    ah, al = split(a)
    bh, bl = split(b)
    return mm(jnp.concatenate([ah, ah, al], axis=1), jnp.concatenate([bh, bl, bh], axis=0))


def silu(v):
    return v * jax.nn.sigmoid(v)


def layer_kernel(
    tokens_in, gain_in, aq_in, ak_in, av_in, dq_in, dk_in, dv_in, dz_in, bw_in, gw_in, ogain_in, ao_in, do_in,
    sink_in, shift_in, dlog_in,
    out,
    gain, aq, ak, av, dq, dk, dv, dz, bw, gw, ogain, ao, do, sink, shift, dlog,
    tok, normed, stage, w1, w2, kv, mats, rowmats, hsend, hall, pbuf, prec, send_sem, recv_sem, own_sem,
):
    sp = lax.axis_index("sp")
    x = lax.axis_index("tp")
    c = lax.rem(sp, 2)
    b = lax.div(sp, 2)
    z = lax.div(b, 4)
    y = lax.rem(b, 4)
    o = 1 - c

    open_scopes = []

    def phase(name):
        while open_scopes:
            open_scopes.pop().__exit__(None, None, None)
        if name:
            open_scopes.append(jax.named_scope(name))
            open_scopes[0].__enter__()

    def m4(v):
        return lax.rem(v + 4, 4)

    def dev(zz, yy, cc, xx):
        return {"sp": (zz * 4 + yy) * 2 + cc, "tp": xx}

    def dev_x(d):
        return dev(z, y, c, m4(x + d))

    def dev_y(d, core=c):
        return dev(z, m4(y + d), core, x)

    def dev_z(d, core=c):
        return dev(m4(z + d), y, core, x)

    def dev_b(d):
        bb = lax.rem(b + d + 16, 16)
        return {"sp": bb * 2 + c, "tp": x}

    partner = dev(z, y, o, x)
    sent = []

    def send(src, dst, device, landed):
        i = len(sent)
        copy = pltpu.make_async_remote_copy(
            src_ref=src, dst_ref=dst, send_sem=send_sem.at[i], recv_sem=recv_sem.at[i],
            device_id=device, device_id_type=MESH,
        )
        copy.start()
        sent.append(copy)
        return pltpu.make_async_remote_copy(
            src_ref=landed, dst_ref=landed, send_sem=send_sem.at[i], recv_sem=recv_sem.at[i],
            device_id=device, device_id_type=MESH,
        )

    phase("load")
    half_rows = pl.ds(128 * c, 128)
    other_rows = pl.ds(128 * o, 128)
    tokens = tok.at[x, half_rows]
    loads = [
        pltpu.make_async_copy(src, dst, own_sem.at[i])
        for i, (src, dst) in enumerate(
            [(aq_in, aq), (ak_in, ak), (av_in, av), (dq_in, dq), (dk_in, dk), (dv_in, dv), (dz_in, dz), (bw_in, bw),
             (gw_in, gw), (ao_in, ao), (do_in, do), (tokens_in, tokens), (gain_in, gain), (ogain_in, ogain),
             (sink_in, sink), (shift_in, shift), (dlog_in, dlog)]
        )
    ]
    for load in loads:
        load.start()
    barrier = pltpu.get_barrier_semaphore()
    peers = [partner]
    for d in (1, 2, 3):
        peers += [dev_x(d), dev_y(d), dev_z(d), dev_y(d, o), dev_z(d, o)]
    peers += [dev_b(1), dev_b(-1)]
    for peer in peers:
        pl.semaphore_signal(barrier, inc=1, device_id=peer, device_id_type=MESH)
    for load in loads[:11]:
        load.wait()
    phase("pack")
    attn_t, delta_t = ao[...], do[...]
    blank = jnp.zeros((60, 32), F32)
    for cc in range(2):
        cols = slice(64 * cc, 64 * cc + 64)
        small = jnp.concatenate([bw[cc].astype(F32), gw[cc].astype(F32), blank], axis=0).T.astype(BF16)
        stage[cc] = jnp.concatenate(
            [aq[:, cols], dq[:, cols], dk[:, cols], dv[:, cols], dz[:, cols], small, ak[...], av[...],
             attn_t[:, cols], delta_t[:, cols]],
            axis=1,
        )
    w1[z, y, c] = stage[c, :, 0:512]

    phase("barrier")
    pl.semaphore_wait(barrier, len(peers))

    class Ring:
        def __init__(self, w, s, y_first, source=None):
            self.w, self.s, self.y_first, self.source = w, s, y_first, source
            self.waits = {}

        def slot(self, first, second, half=None):
            zz, yy = (z + second, y + first) if self.y_first else (z + first, y + second)
            ref = self.w.at[m4(zz), m4(yy), self.s]
            return ref if half is None else ref.at[pl.ds(16 * half, 16)]

        def twin(self, _):
            return self.w.at[z, y, 1 - self.s]

        def dev1(self, d, core=c):
            return dev_y(d, core) if self.y_first else dev_z(d, core)

        def dev2(self, d, core=c):
            return dev_z(d, core) if self.y_first else dev_y(d, core)

        def across(self, f):
            for d in (1, -1):
                if f == 0 and self.source is not None:
                    self.waits[f, d] = send(self.source, self.twin(0), self.dev2(d, o), self.slot(f, -d))
                else:
                    block = self.slot(f, 0)
                    self.waits[f, d] = send(block, block, self.dev2(d), self.slot(f, -d))

        def relay(self, f):
            for d, half in ((1, 0), (-1, 1)):
                self.waits[f, d].wait_recv()
                block = self.slot(f, -d, half)
                self.waits[f, 2 * d] = send(block, block, self.dev2(d), self.slot(f, -2 * d, half))

        def begin(self):
            block = self.slot(0, 0)
            for d in (1, -1):
                if self.source is not None:
                    self.waits[d] = send(self.source, self.twin(0), self.dev1(d, o), self.slot(-d, 0))
                else:
                    self.waits[d] = send(block, block, self.dev1(d), self.slot(-d, 0))

        def near(self):
            for d, half in ((1, 0), (-1, 1)):
                self.waits[d].wait_recv()
                block = self.slot(-d, 0, half)
                self.waits[2 * d] = send(block, block, self.dev1(d), self.slot(-2 * d, 0, half))
            self.across(-1)
            self.across(1)

        def far(self):
            self.waits[2].wait_recv()
            self.waits[-2].wait_recv()
            self.across(2)

        def finish(self):
            for f in (0, -1, 1, 2):
                self.waits[f, 2].wait_recv()
                self.waits[f, -2].wait_recv()

    in_cols = pl.ds(0, 512)
    out_cols = pl.ds(512, 128)
    x_cols = pl.ds(pl.multiple_of(128 * x, 128), 128)

    def x_cols_of(d):
        return pl.ds(pl.multiple_of(128 * m4(x + d), 128), 128)

    phase("start")
    first = Ring(w1, c, True)
    second = Ring(w1, o, False, stage.at[o, :, in_cols])
    out_first = Ring(w2, c, True)
    out_second = Ring(w2, o, False)
    first.begin()
    second.begin()
    first.across(0)
    second.across(0)
    for load in loads[11:]:
        load.wait()
    tok_in = [send(tokens, tokens, dev_x(d), tok.at[m4(x - d), half_rows]) for d in (1, 3, 2)]
    w_swap = send(stage.at[o, :, in_cols], w1.at[z, y, c], partner, w1.at[z, y, o])
    tok_swap = [send(tokens, tokens, partner, tok.at[x, other_rows])]
    w2_swap = send(stage.at[o, :, out_cols], w2.at[z, y, c, :, x_cols], partner, w2.at[z, y, o, :, x_cols])
    own_w2 = pltpu.make_async_copy(stage.at[c, :, out_cols], w2.at[z, y, c, :, x_cols], own_sem.at[17])
    own_w2.start()
    phase("swap")
    w_swap.wait_recv()
    own_w2.wait()
    w2_swap.wait_recv()
    w2_in = [
        send(w2.at[z, y, :, :, x_cols], w2.at[z, y, :, :, x_cols], dev_x(d), w2.at[z, y, :, :, x_cols_of(-d)])
        for d in (1, 3, 2)
    ]
    phase("near")
    first.near()
    second.near()
    phase("tokens")
    for d, arrived in zip((1, 3, 2), tok_in):
        arrived.wait_recv()
        src = m4(x - d)
        tok_swap.append(send(tok.at[src, half_rows], tok.at[src, half_rows], partner, tok.at[src, other_rows]))
    phase("relay0")
    first.relay(0)
    second.relay(0)
    phase("far")
    first.far()
    second.far()
    phase("tokswap")
    for arrived in tok_swap:
        arrived.wait_recv()

    phase("norm")
    squares = jnp.zeros((ROWS, 1), F32)
    for k in range(4):
        wide = tok[k].astype(F32)
        squares = squares + jnp.sum(wide * wide, axis=-1, keepdims=True)
    inv = lax.rsqrt(squares * (1.0 / 1024.0) + EPS)
    for k in range(4):
        normed[k] = (tok[k].astype(F32) * inv * gain[:, 256 * k : 256 * k + 256]).astype(BF16)

    phase("relay1")
    for f in (-1, 1):
        first.relay(f)
        second.relay(f)
    phase("relay2")
    first.relay(2)
    second.relay(2)
    for arrived in w2_in:
        arrived.wait_recv()
    for ring in (out_first, out_second):
        ring.begin()
        ring.across(0)
    phase("wfinish")
    first.finish()
    second.finish()

    phase("proj")
    proj = mm(normed[0], w1[0].reshape(256, 512))
    for k in range(1, 4):
        proj = proj + mm(normed[k], w1[k].reshape(256, 512))
    t0, t1, t2 = proj[:, 0:128], proj[:, 128:256], proj[:, 256:384]
    kv[64:320, :] = proj[:, 384:512].astype(BF16)
    halo = [
        send(kv.at[pl.ds(256, 64)], kv.at[pl.ds(0, 64)], dev_b(1), kv.at[pl.ds(0, 64)]),
        send(kv.at[pl.ds(64, 64)], kv.at[pl.ds(320, 64)], dev_b(-1), kv.at[pl.ds(320, 64)]),
    ]
    att_q = t0[:, 0:64].astype(BF16)
    act_q = silu(t0[:, 64:128].astype(BF16).astype(F32))
    act_kv = silu(t1.astype(BF16).astype(F32))
    act_k, val = act_kv[:, 0:64], act_kv[:, 64:128]
    q = act_q * lax.rsqrt(jnp.sum(act_q * act_q, axis=-1, keepdims=True) + EPS) * HEAD_DIM**-0.5
    key = act_k * lax.rsqrt(jnp.sum(act_k * act_k, axis=-1, keepdims=True) + EPS)
    gate = silu(t2[:, 0:64].astype(BF16).astype(F32))

    phase("gates")
    lane = lax.broadcasted_iota(jnp.int32, (1, 128), 1)
    bias = jnp.where(lane == 64, shift[0, c], jnp.where(lane == 65, shift[1, c], 0.0))
    rate = jnp.exp(jnp.where(lane == 66, dlog[0, c], jnp.where(lane == 67, dlog[1, c], 0.0)))
    strength = jax.nn.sigmoid(t2 + bias)
    softplus = jnp.maximum(t2, 0.0) + jnp.log1p(jnp.exp(-jnp.abs(t2)))
    decay = jnp.where((lane == 66) | (lane == 67), -rate * softplus * (1.0 / TOKENS), 0.0)

    row = lax.broadcasted_iota(jnp.int32, (128, 128), 0)
    col = lax.broadcasted_iota(jnp.int32, (128, 128), 1)
    masks = (row >= col, row <= col)
    unit = jnp.where(row == col, 1.0, 0.0)
    near16 = lax.shift_right_logical(row, 4) == lax.shift_right_logical(col, 4)

    g_hi = decay.astype(BF16)
    rest = decay - g_hi.astype(F32)
    g_mid = rest.astype(BF16)
    g_lo = (rest - g_mid.astype(F32)).astype(BF16)
    g_parts = jnp.concatenate(
        [part[128 * h : 128 * h + 128, 64:128] for h in range(2) for part in (g_hi, g_mid, g_lo)], axis=1
    )
    sums = [mm(jnp.where(mask, 1.0, 0.0).astype(BF16), g_parts) for mask in masks]
    sub = lax.broadcasted_iota(jnp.int32, (1, 192), 1)
    picked = jnp.where((sub & 63) == 2, sums[0][:, 0:192], sums[1][:, 0:192])
    picked2 = jnp.where((sub & 63) == 2, sums[0][:, 192:384], sums[1][:, 192:384])
    g_all = jnp.concatenate([p[:, 0:64] + p[:, 64:128] + p[:, 128:192] for p in (picked, picked2)], axis=0)
    turned = jnp.concatenate([key, g_all], axis=1).T
    key_t = turned[0:64]
    key_h, key_l = split(key)
    q_h, q_l = split(q)
    kt_h, kt_l = split(key_t)
    q3 = jnp.concatenate([q_h, q_h, q_l], axis=1)
    key3 = jnp.concatenate([key_h, key_h, key_l], axis=1)
    kt3 = jnp.concatenate([kt_h, kt_l, kt_h], axis=0)

    phase("rings1")
    out_first.near()
    out_second.near()

    phase("delta1")
    lane2 = lax.broadcasted_iota(jnp.int32, (64, 128), 1)
    row2 = lax.broadcasted_iota(jnp.int32, (64, 128), 0)
    eye2 = jnp.where(lane2 == row2 + 64, 1.0, 0.0)
    chains = [(way, h) for way in range(2) for h in range(2)]
    low, scores_d, sides, grown, key_end, end, d = {}, {}, {}, {}, {}, {}, {}
    for h in range(2):
        hs = slice(128 * h, 128 * h + 128)
        pairs = mm(jnp.concatenate([q3[hs], key3[hs]], axis=0), kt3[:, hs])
        for way in range(2):
            at = way, h
            beta = strength[hs, 64 + way : 65 + way]
            g_col = g_all[hs, 2 + way : 3 + way]
            g_row = turned[66 + way : 67 + way, hs]
            g_end = g_col[127:128] if way == 0 else g_col[0:1]
            decays = jnp.exp(jnp.where(masks[way], g_col - g_row, -jnp.inf))
            low[at] = jnp.where(row == col, 0.0, beta * pairs[128:256] * decays)
            scores_d[at] = pairs[0:128] * decays
            up = jnp.exp(g_col)
            grown[at] = up * q[hs]
            sides[at] = jnp.concatenate([beta * val[hs], (beta * up) * key[hs]], axis=1)
            key_end[at] = key_t[:, hs] * jnp.exp(g_end - g_row)
            end[at] = jnp.exp(g_end)
    d1 = {at: jnp.where(near16, low[at], 0.0) for at in chains}
    off = {at: jnp.where(near16, 0.0, low[at]) for at in chains}
    d2 = {at: dot3(d1[at], d1[at]) for at in chains}
    inner = {at: unit - d1[at] for at in chains}
    d4 = {at: dot3(d2[at], d2[at]) for at in chains}
    inner = {at: inner[at] + dot3(inner[at], d2[at]) for at in chains}
    d8 = {at: dot3(d4[at], d4[at]) for at in chains}
    inner = {at: inner[at] + dot3(inner[at], d4[at]) for at in chains}
    inner = {at: inner[at] + dot3(inner[at], d8[at]) for at in chains}
    phase("delta2")
    m1 = {at: dot3(inner[at], off[at]) for at in chains}
    uw = {at: dot3(inner[at], sides[at]) for at in chains}
    m2 = {at: dot3(m1[at], m1[at]) for at in chains}
    uw = {at: uw[at] - dot3(m1[at], uw[at]) for at in chains}
    m4_ = {at: dot3(m2[at], m2[at]) for at in chains}
    uw = {at: uw[at] + dot3(m2[at], uw[at]) for at in chains}
    uw = {at: uw[at] + dot3(m4_[at], uw[at]) for at in chains}
    phase("final")

    def after(later, earlier):
        return dot3_deep(later[:, 64:128], earlier) + jnp.where(lane2 < 64, later, 0.0)

    maps = {}
    for at in chains:
        final = dot3(key_end[at], uw[at])
        maps[at] = jnp.where(lane2 < 64, final, end[at] * eye2 - final)
    for way in range(2):
        block_map = after(maps[way, 1 - way], maps[way, way])
        mats[y, way] = (block_map - eye2).astype(LINK)
    phase("scan1send")
    scan1 = [send(mats.at[y], mats.at[y], dev_y(d), mats.at[m4(y - d)]) for d in (1, 3, 2)]

    phase("rings2")
    out_first.relay(0)
    out_second.relay(0)
    out_first.far()
    out_second.far()
    phase("reads")
    local, reads = {}, {}
    for way, h in chains:
        at = way, h
        read = dot3(scores_d[at], uw[at])
        local[at] = read[:, 0:64]
        reads[at] = grown[at] - read[:, 64:128]
        if h != way:
            passed = dot3_deep(reads[at], maps[way, way])
            local[at] = local[at] + passed[:, 0:64]
            reads[at] = passed[:, 64:128]
    local_sum = jnp.concatenate([local[0, h] + local[1, h] for h in range(2)], axis=0)
    reads_all = jnp.concatenate(
        [jnp.concatenate([reads[0, h], reads[1, h]], axis=1) for h in range(2)], axis=0
    )

    phase("halo")
    for arrived in halo:
        arrived.wait_recv()
    phase("attn")
    scores = mm(att_q, kv[:, 0:64], NT) * HEAD_DIM**-0.5
    q_pos = lax.broadcasted_iota(jnp.int32, (ROWS, ROWS + 2 * WINDOW), 0)
    k_pos = lax.broadcasted_iota(jnp.int32, (ROWS, ROWS + 2 * WINDOW), 1) - WINDOW
    seen = k_pos + b * ROWS
    allowed = (jnp.abs(q_pos - k_pos) <= WINDOW) & (seen >= 0) & (seen < TOKENS)
    scores = jnp.where(allowed, scores, -jnp.inf)
    top = jnp.maximum(jnp.max(scores, axis=-1, keepdims=True), sink[c])
    weights = jnp.exp(scores - top)
    total = jnp.sum(weights, axis=-1, keepdims=True) + jnp.exp(sink[c] - top)
    weights = (weights / total).astype(BF16)
    attn_heads = mm(weights, kv[:, 64:128])

    phase("scan1wait")
    for arrived in scan1:
        arrived.wait_recv()

    phase("compose")
    entry = []
    for way in range(2):
        m = [mats[k if way == 0 else 3 - k, way].astype(F32) + eye2 for k in range(4)]
        place = y if way == 0 else 3 - y
        two = after(m[1], m[0])
        three = after(m[2], two)
        rowmats[z, way] = (after(after(m[3], m[2]), two) - eye2).astype(LINK)
        entry.append(
            jnp.where(place == 0, eye2, jnp.where(place == 1, m[0], jnp.where(place == 2, two, three)))
        )
    phase("scan2send")
    scan2 = [send(rowmats.at[z], rowmats.at[z], dev_z(d), rowmats.at[m4(z - d)]) for d in (1, 3, 2)]
    phase("rings3")
    for f in (-1, 1, 2):
        out_first.relay(f)
        out_second.relay(f)
    phase("scan2wait")
    for arrived in scan2:
        arrived.wait_recv()
    phase("states")
    states = []
    for way in range(2):
        m = [rowmats[k if way == 0 else 3 - k, way].astype(F32) + eye2 for k in range(3)]
        place = z if way == 0 else 3 - z
        s1 = m[0][:, 0:64]
        s2 = dot3_deep(m[1][:, 64:128], s1) + m[1][:, 0:64]
        s3 = dot3_deep(m[2][:, 64:128], s2) + m[2][:, 0:64]
        s = jnp.where(place == 0, 0.0, jnp.where(place == 1, s1, jnp.where(place == 2, s2, s3)))
        states.append(dot3_deep(entry[way][:, 64:128], s) + entry[way][:, 0:64])

    reads_h, reads_l = split(reads_all)
    states_h, states_l = split(jnp.concatenate(states, axis=0))
    whole = mm(
        jnp.concatenate([reads_h, reads_l], axis=1),
        jnp.concatenate([states_h, states_h], axis=0),
    )
    whole = local_sum + whole + mm(reads_h, states_l)
    scaled = whole * lax.rsqrt(jnp.mean(whole * whole, axis=-1, keepdims=True) + EPS) * ogain[...]
    heads = jnp.concatenate([attn_heads, scaled * gate], axis=1).astype(BF16)
    for k in range(4):
        hsend[k, 0:32] = heads[32 * k : 32 * k + 32]
        hsend[k, 32:64] = heads[128 + 32 * k : 160 + 32 * k]
    phase("headsend")
    head_in = [send(hsend.at[m4(x + d)], hall.at[x], dev_x(d), hall.at[m4(x - d)]) for d in (1, 3, 2)]
    hall[x] = hsend[x]
    phase("w2finish")
    out_first.finish()
    out_second.finish()
    phase("headwait")
    for arrived in head_in:
        arrived.wait_recv()
    phase("outmm")
    gathered = jnp.concatenate([hall[k] for k in range(4)], axis=1)
    for k in range(4):
        part = mm(gathered, w2[k].reshape(256, 512), NT)
        pbuf[0, :, 256 * k : 256 * k + 256] = part[0:32]
        pbuf[1, :, 256 * k : 256 * k + 256] = part[32:64]
    phase("last")
    last = send(pbuf.at[o], prec, partner, prec)
    last.wait_recv()
    out[...] = pbuf[c] + prec[...]
    phase("drain")
    for copy in sent:
        copy.wait_send()
    phase(None)


def per_device(
    tokens, norm_gain, attn_query, attn_key, attn_value, sink_logit, delta_query, delta_key, delta_value,
    delta_gate, beta_weight, decay_weight, beta_shift, decay_log, out_gain, attn_out, delta_out,
):
    operands = (
        tokens, norm_gain.reshape(1, -1), attn_query, attn_key, attn_value, delta_query, delta_key, delta_value,
        delta_gate, beta_weight.transpose(1, 2, 0), decay_weight.transpose(1, 2, 0), out_gain.reshape(1, -1),
        attn_out.T, delta_out.T, sink_logit, beta_shift, decay_log,
    )
    hbm = pl.BlockSpec(memory_space=pltpu.HBM)
    vmem = pl.BlockSpec(memory_space=pltpu.VMEM)
    summed = pl.pallas_call(
        layer_kernel,
        out_shape=jax.ShapeDtypeStruct((32, 1024), F32),
        in_specs=[hbm] * 17,
        out_specs=vmem,
        scratch_shapes=[
            pltpu.VMEM((1, 1024), F32),
            pltpu.VMEM((32, 128), BF16),
            pltpu.VMEM((32, 64), BF16),
            pltpu.VMEM((32, 64), BF16),
            pltpu.VMEM((32, 128), BF16),
            pltpu.VMEM((32, 128), BF16),
            pltpu.VMEM((32, 128), BF16),
            pltpu.VMEM((32, 128), BF16),
            pltpu.VMEM((2, 2, 32), BF16),
            pltpu.VMEM((2, 2, 32), BF16),
            pltpu.VMEM((1, 64), F32),
            pltpu.VMEM((32, 128), BF16),
            pltpu.VMEM((32, 128), BF16),
            pltpu.SMEM((2,), F32),
            pltpu.SMEM((2, 2), F32),
            pltpu.SMEM((2, 2), F32),
            pltpu.VMEM((4, 256, 256), BF16),
            pltpu.VMEM((4, 256, 256), BF16),
            pltpu.VMEM((2, 32, 640), BF16),
            pltpu.VMEM((4, 4, 2, 32, 512), BF16),
            pltpu.VMEM((4, 4, 2, 32, 512), BF16),
            pltpu.VMEM((384, 128), BF16),
            pltpu.VMEM((4, 2, 64, 128), LINK),
            pltpu.VMEM((4, 2, 64, 128), LINK),
            pltpu.VMEM((4, 64, 128), BF16),
            pltpu.VMEM((4, 64, 128), BF16),
            pltpu.VMEM((2, 32, 1024), F32),
            pltpu.VMEM((32, 1024), F32),
            pltpu.SemaphoreType.DMA((COPIES,)),
            pltpu.SemaphoreType.DMA((COPIES,)),
            pltpu.SemaphoreType.DMA((18,)),
        ],
        compiler_params=pltpu.CompilerParams(collective_id=0, has_side_effects=True, vmem_limit_bytes=24 * 2**20),
    )(*(pltpu.with_memory_space_constraint(operand, pltpu.HBM) for operand in operands))
    return summed.astype(BF16)


def solution(mesh):
    return jax.shard_map(
        per_device,
        mesh=mesh,
        in_specs=(
            P("sp", "tp"), P(), P("sp", "tp"), P("sp", "tp"), P("sp", "tp"), P("tp"), P("sp", "tp"),
            P("sp", "tp"), P("sp", "tp"), P("sp", "tp"), P("sp", "tp", None), P("sp", "tp", None),
            P(None, "tp"), P(None, "tp"), P(), P("tp", "sp"), P("tp", "sp"),
        ),
        out_specs=P(("sp", "tp"), None),
        check_vma=False,
    )
```

```python
import jax
import jax.numpy as jnp
from jax import lax
from jax.experimental import pallas as pl
from jax.experimental.pallas import tpu as pltpu
from jax.sharding import PartitionSpec as P

HEAD_DIM = 64
WINDOW = 64
ROWS = 256
TOKENS = 4096
EPS = 1e-6
COPIES = 120
MESH = pl.DeviceIdType.MESH
F32 = jnp.float32
BF16 = jnp.bfloat16
LINK = F32
NN = (((1,), (0,)), ((), ()))
NT = (((1,), (1,)), ((), ()))


def mm(a, b, dims=NN):
    return lax.dot_general(a, b, dims, preferred_element_type=F32)


def split(a):
    hi = a.astype(BF16)
    return hi, (a - hi.astype(F32)).astype(BF16)


def left(a):
    hi, lo = split(a)
    return jnp.concatenate([hi, lo], axis=1)


def right(b):
    hi, lo = split(b)
    return jnp.concatenate(
        [jnp.concatenate([hi, lo], axis=1), jnp.concatenate([hi, jnp.zeros_like(lo)], axis=1)], axis=0
    )


def dot3(a, b):
    both = mm(left(a), right(b))
    return both[:, 0:128] + both[:, 128:256]


def dot3_deep(a, b):
    ah, al = split(a)
    bh, bl = split(b)
    return mm(jnp.concatenate([ah, ah, al], axis=1), jnp.concatenate([bh, bl, bh], axis=0))


def silu(v):
    return v * jax.nn.sigmoid(v)


def layer_kernel(
    tokens_in, gain_in, aq_in, ak_in, av_in, dq_in, dk_in, dv_in, dz_in, bw_in, gw_in, ogain_in, ao_in, do_in,
    sink_in, shift_in, dlog_in,
    out,
    gain, aq, ak, av, dq, dk, dv, dz, bw, gw, ogain, ao, do, sink, shift, dlog,
    tok, normed, stage, w1, w2, kv, mats, rowmats, hsend, hall, pbuf, prec, send_sem, recv_sem, own_sem,
):
    sp = lax.axis_index("sp")
    x = lax.axis_index("tp")
    c = lax.rem(sp, 2)
    b = lax.div(sp, 2)
    z = lax.div(b, 4)
    y = lax.rem(b, 4)
    o = 1 - c

    open_scopes = []

    def phase(name):
        while open_scopes:
            open_scopes.pop().__exit__(None, None, None)
        if name:
            open_scopes.append(jax.named_scope(name))
            open_scopes[0].__enter__()

    def m4(v):
        return lax.rem(v + 4, 4)

    def dev(zz, yy, cc, xx):
        return {"sp": (zz * 4 + yy) * 2 + cc, "tp": xx}

    def dev_x(d):
        return dev(z, y, c, m4(x + d))

    def dev_y(d, core=c):
        return dev(z, m4(y + d), core, x)

    def dev_z(d, core=c):
        return dev(m4(z + d), y, core, x)

    def dev_b(d):
        bb = lax.rem(b + d + 16, 16)
        return {"sp": bb * 2 + c, "tp": x}

    partner = dev(z, y, o, x)
    sent = []

    def send(src, dst, device, landed):
        i = len(sent)
        copy = pltpu.make_async_remote_copy(
            src_ref=src, dst_ref=dst, send_sem=send_sem.at[i], recv_sem=recv_sem.at[i],
            device_id=device, device_id_type=MESH,
        )
        copy.start()
        sent.append(copy)
        return pltpu.make_async_remote_copy(
            src_ref=landed, dst_ref=landed, send_sem=send_sem.at[i], recv_sem=recv_sem.at[i],
            device_id=device, device_id_type=MESH,
        )

    phase("load")
    half_rows = pl.ds(128 * c, 128)
    other_rows = pl.ds(128 * o, 128)
    tokens = tok.at[x, half_rows]
    loads = [
        pltpu.make_async_copy(src, dst, own_sem.at[i])
        for i, (src, dst) in enumerate(
            [(aq_in, aq), (ak_in, ak), (av_in, av), (dq_in, dq), (dk_in, dk), (dv_in, dv), (dz_in, dz), (bw_in, bw),
             (gw_in, gw), (ao_in, ao), (do_in, do), (tokens_in, tokens), (gain_in, gain), (ogain_in, ogain),
             (sink_in, sink), (shift_in, shift), (dlog_in, dlog)]
        )
    ]
    for load in loads:
        load.start()
    barrier = pltpu.get_barrier_semaphore()
    peers = [partner]
    for d in (1, 2, 3):
        peers += [dev_x(d), dev_y(d), dev_z(d), dev_y(d, o), dev_z(d, o)]
    peers += [dev_b(1), dev_b(-1)]
    for peer in peers:
        pl.semaphore_signal(barrier, inc=1, device_id=peer, device_id_type=MESH)
    for load in loads[:11]:
        load.wait()
    phase("pack")
    attn_t, delta_t = ao[...], do[...]
    blank = jnp.zeros((60, 32), F32)
    for cc in range(2):
        cols = slice(64 * cc, 64 * cc + 64)
        small = jnp.concatenate([bw[cc].astype(F32), gw[cc].astype(F32), blank], axis=0).T.astype(BF16)
        stage[cc] = jnp.concatenate(
            [aq[:, cols], dq[:, cols], dk[:, cols], dv[:, cols], dz[:, cols], small, ak[...], av[...],
             attn_t[:, cols], delta_t[:, cols]],
            axis=1,
        )
    w1[z, y, c] = stage[c, :, 0:512]

    phase("barrier")
    pl.semaphore_wait(barrier, len(peers))

    class Gather:
        def __init__(self, w, s, y_first, source=None):
            self.w, self.s, self.y_first, self.source = w, s, y_first, source
            self.waits = {}

        def slot(self, first, second):
            zz, yy = (z + second, y + first) if self.y_first else (z + first, y + second)
            return self.w.at[m4(zz), m4(yy), self.s]

        def own(self, device):
            if self.source is None:
                return self.slot(0, 0), self.slot(0, 0), device(c)
            return self.source, self.w.at[z, y, 1 - self.s], device(o)

        def along(self, axis, d, core):
            return dev_y(d, core) if axis == self.y_first else dev_z(d, core)

        def begin(self):
            for d in (1, 3, 2):
                source, place, device = self.own(lambda core, d=d: self.along(True, d, core))
                self.waits[d] = send(source, place, device, self.slot(-d, 0))

        def across(self, f):
            for d in (1, 3, 2):
                if f == 0:
                    source, place, device = self.own(lambda core, d=d: self.along(False, d, core))
                else:
                    source, place, device = self.slot(f, 0), self.slot(f, 0), self.along(False, d, c)
                self.waits[f, d] = send(source, place, device, self.slot(f, -d))

        def forward(self, d):
            self.waits[d].wait_recv()
            self.across(-d)

        def finish(self):
            for d in (1, 3, 2):
                for f in (0, -1, -3, -2):
                    self.waits[f, d].wait_recv()

    in_cols = pl.ds(0, 512)
    out_cols = pl.ds(512, 128)
    x_cols = pl.ds(pl.multiple_of(128 * x, 128), 128)

    def x_cols_of(d):
        return pl.ds(pl.multiple_of(128 * m4(x + d), 128), 128)

    phase("start")
    first = Gather(w1, c, True)
    second = Gather(w1, o, False, stage.at[o, :, in_cols])
    out_first = Gather(w2, c, True)
    out_second = Gather(w2, o, False)
    first.begin()
    second.begin()
    first.across(0)
    second.across(0)
    for load in loads[11:]:
        load.wait()
    tok_in = [send(tokens, tokens, dev_x(d), tok.at[m4(x - d), half_rows]) for d in (1, 3, 2)]
    w_swap = send(stage.at[o, :, in_cols], w1.at[z, y, c], partner, w1.at[z, y, o])
    tok_swap = [send(tokens, tokens, partner, tok.at[x, other_rows])]
    w2_swap = send(stage.at[o, :, out_cols], w2.at[z, y, c, :, x_cols], partner, w2.at[z, y, o, :, x_cols])
    own_w2 = pltpu.make_async_copy(stage.at[c, :, out_cols], w2.at[z, y, c, :, x_cols], own_sem.at[17])
    own_w2.start()
    phase("swap")
    w_swap.wait_recv()
    own_w2.wait()
    w2_swap.wait_recv()
    w2_in = [
        send(w2.at[z, y, :, :, x_cols], w2.at[z, y, :, :, x_cols], dev_x(d), w2.at[z, y, :, :, x_cols_of(-d)])
        for d in (1, 3, 2)
    ]
    phase("near")
    for d in (1, 3, 2):
        first.forward(d)
        second.forward(d)
    phase("tokens")
    for d, arrived in zip((1, 3, 2), tok_in):
        arrived.wait_recv()
        src = m4(x - d)
        tok_swap.append(send(tok.at[src, half_rows], tok.at[src, half_rows], partner, tok.at[src, other_rows]))
    phase("tokswap")
    for arrived in tok_swap:
        arrived.wait_recv()

    phase("norm")
    squares = jnp.zeros((ROWS, 1), F32)
    for k in range(4):
        wide = tok[k].astype(F32)
        squares = squares + jnp.sum(wide * wide, axis=-1, keepdims=True)
    inv = lax.rsqrt(squares * (1.0 / 1024.0) + EPS)
    for k in range(4):
        normed[k] = (tok[k].astype(F32) * inv * gain[:, 256 * k : 256 * k + 256]).astype(BF16)

    phase("w2in")
    for arrived in w2_in:
        arrived.wait_recv()
    for ring in (out_first, out_second):
        ring.begin()
        ring.across(0)
    phase("wfinish")
    first.finish()
    second.finish()

    phase("proj")
    proj = mm(normed[0], w1[0].reshape(256, 512))
    for k in range(1, 4):
        proj = proj + mm(normed[k], w1[k].reshape(256, 512))
    phase("rings")
    for d in (1, 3, 2):
        out_first.forward(d)
        out_second.forward(d)
    phase("gates0")
    t0, t1, t2 = proj[:, 0:128], proj[:, 128:256], proj[:, 256:384]
    kv[64:320, :] = proj[:, 384:512].astype(BF16)
    halo = [
        send(kv.at[pl.ds(256, 64)], kv.at[pl.ds(0, 64)], dev_b(1), kv.at[pl.ds(0, 64)]),
        send(kv.at[pl.ds(64, 64)], kv.at[pl.ds(320, 64)], dev_b(-1), kv.at[pl.ds(320, 64)]),
    ]
    att_q = t0[:, 0:64].astype(BF16)
    act_q = silu(t0[:, 64:128].astype(BF16).astype(F32))
    act_kv = silu(t1.astype(BF16).astype(F32))
    act_k, val = act_kv[:, 0:64], act_kv[:, 64:128]
    q = act_q * lax.rsqrt(jnp.sum(act_q * act_q, axis=-1, keepdims=True) + EPS) * HEAD_DIM**-0.5
    key = act_k * lax.rsqrt(jnp.sum(act_k * act_k, axis=-1, keepdims=True) + EPS)
    gate = silu(t2[:, 0:64].astype(BF16).astype(F32))

    phase("gates")
    lane = lax.broadcasted_iota(jnp.int32, (1, 128), 1)
    bias = jnp.where(lane == 64, shift[0, c], jnp.where(lane == 65, shift[1, c], 0.0))
    rate = jnp.exp(jnp.where(lane == 66, dlog[0, c], jnp.where(lane == 67, dlog[1, c], 0.0)))
    strength = jax.nn.sigmoid(t2 + bias)
    softplus = jnp.maximum(t2, 0.0) + jnp.log1p(jnp.exp(-jnp.abs(t2)))
    decay = jnp.where((lane == 66) | (lane == 67), -rate * softplus * (1.0 / TOKENS), 0.0)

    row = lax.broadcasted_iota(jnp.int32, (128, 128), 0)
    col = lax.broadcasted_iota(jnp.int32, (128, 128), 1)
    masks = (row >= col, row <= col)
    unit = jnp.where(row == col, 1.0, 0.0)
    near16 = lax.shift_right_logical(row, 4) == lax.shift_right_logical(col, 4)

    g_hi = decay.astype(BF16)
    rest = decay - g_hi.astype(F32)
    g_mid = rest.astype(BF16)
    g_lo = (rest - g_mid.astype(F32)).astype(BF16)
    g_parts = jnp.concatenate(
        [part[128 * h : 128 * h + 128, 64:128] for h in range(2) for part in (g_hi, g_mid, g_lo)], axis=1
    )
    sums = [mm(jnp.where(mask, 1.0, 0.0).astype(BF16), g_parts) for mask in masks]
    sub = lax.broadcasted_iota(jnp.int32, (1, 192), 1)
    picked = jnp.where((sub & 63) == 2, sums[0][:, 0:192], sums[1][:, 0:192])
    picked2 = jnp.where((sub & 63) == 2, sums[0][:, 192:384], sums[1][:, 192:384])
    g_all = jnp.concatenate([p[:, 0:64] + p[:, 64:128] + p[:, 128:192] for p in (picked, picked2)], axis=0)
    turned = jnp.concatenate([key, g_all], axis=1).T
    key_t = turned[0:64]
    key_h, key_l = split(key)
    q_h, q_l = split(q)
    kt_h, kt_l = split(key_t)
    q3 = jnp.concatenate([q_h, q_h, q_l], axis=1)
    key3 = jnp.concatenate([key_h, key_h, key_l], axis=1)
    kt3 = jnp.concatenate([kt_h, kt_l, kt_h], axis=0)

    phase("delta1")
    lane2 = lax.broadcasted_iota(jnp.int32, (64, 128), 1)
    row2 = lax.broadcasted_iota(jnp.int32, (64, 128), 0)
    eye2 = jnp.where(lane2 == row2 + 64, 1.0, 0.0)
    chains = [(way, h) for way in range(2) for h in range(2)]
    low, scores_d, sides, grown, key_end, end, d = {}, {}, {}, {}, {}, {}, {}
    for h in range(2):
        hs = slice(128 * h, 128 * h + 128)
        pairs = mm(jnp.concatenate([q3[hs], key3[hs]], axis=0), kt3[:, hs])
        for way in range(2):
            at = way, h
            beta = strength[hs, 64 + way : 65 + way]
            g_col = g_all[hs, 2 + way : 3 + way]
            g_row = turned[66 + way : 67 + way, hs]
            g_end = g_col[127:128] if way == 0 else g_col[0:1]
            decays = jnp.exp(jnp.where(masks[way], g_col - g_row, -jnp.inf))
            low[at] = jnp.where(row == col, 0.0, beta * pairs[128:256] * decays)
            scores_d[at] = pairs[0:128] * decays
            up = jnp.exp(g_col)
            grown[at] = up * q[hs]
            sides[at] = jnp.concatenate([beta * val[hs], (beta * up) * key[hs]], axis=1)
            key_end[at] = key_t[:, hs] * jnp.exp(g_end - g_row)
            end[at] = jnp.exp(g_end)
    d1 = {at: jnp.where(near16, low[at], 0.0) for at in chains}
    off = {at: jnp.where(near16, 0.0, low[at]) for at in chains}
    d2 = {at: dot3(d1[at], d1[at]) for at in chains}
    inner = {at: unit - d1[at] for at in chains}
    d4 = {at: dot3(d2[at], d2[at]) for at in chains}
    inner = {at: inner[at] + dot3(inner[at], d2[at]) for at in chains}
    d8 = {at: dot3(d4[at], d4[at]) for at in chains}
    inner = {at: inner[at] + dot3(inner[at], d4[at]) for at in chains}
    inner = {at: inner[at] + dot3(inner[at], d8[at]) for at in chains}
    phase("delta2")
    m1 = {at: dot3(inner[at], off[at]) for at in chains}
    uw = {at: dot3(inner[at], sides[at]) for at in chains}
    m2 = {at: dot3(m1[at], m1[at]) for at in chains}
    uw = {at: uw[at] - dot3(m1[at], uw[at]) for at in chains}
    m4_ = {at: dot3(m2[at], m2[at]) for at in chains}
    uw = {at: uw[at] + dot3(m2[at], uw[at]) for at in chains}
    uw = {at: uw[at] + dot3(m4_[at], uw[at]) for at in chains}
    phase("final")

    def after(later, earlier):
        return dot3_deep(later[:, 64:128], earlier) + jnp.where(lane2 < 64, later, 0.0)

    maps = {}
    for at in chains:
        final = dot3(key_end[at], uw[at])
        maps[at] = jnp.where(lane2 < 64, final, end[at] * eye2 - final)
    for way in range(2):
        block_map = after(maps[way, 1 - way], maps[way, way])
        mats[y, way] = (block_map - eye2).astype(LINK)
    phase("scan1send")
    scan1 = [send(mats.at[y], mats.at[y], dev_y(d), mats.at[m4(y - d)]) for d in (1, 3, 2)]

    phase("reads")
    local, reads = {}, {}
    for way, h in chains:
        at = way, h
        read = dot3(scores_d[at], uw[at])
        local[at] = read[:, 0:64]
        reads[at] = grown[at] - read[:, 64:128]
        if h != way:
            passed = dot3_deep(reads[at], maps[way, way])
            local[at] = local[at] + passed[:, 0:64]
            reads[at] = passed[:, 64:128]
    local_sum = jnp.concatenate([local[0, h] + local[1, h] for h in range(2)], axis=0)
    reads_all = jnp.concatenate(
        [jnp.concatenate([reads[0, h], reads[1, h]], axis=1) for h in range(2)], axis=0
    )

    phase("halo")
    for arrived in halo:
        arrived.wait_recv()
    phase("attn")
    scores = mm(att_q, kv[:, 0:64], NT) * HEAD_DIM**-0.5
    q_pos = lax.broadcasted_iota(jnp.int32, (ROWS, ROWS + 2 * WINDOW), 0)
    k_pos = lax.broadcasted_iota(jnp.int32, (ROWS, ROWS + 2 * WINDOW), 1) - WINDOW
    seen = k_pos + b * ROWS
    allowed = (jnp.abs(q_pos - k_pos) <= WINDOW) & (seen >= 0) & (seen < TOKENS)
    scores = jnp.where(allowed, scores, -jnp.inf)
    top = jnp.maximum(jnp.max(scores, axis=-1, keepdims=True), sink[c])
    weights = jnp.exp(scores - top)
    total = jnp.sum(weights, axis=-1, keepdims=True) + jnp.exp(sink[c] - top)
    weights = (weights / total).astype(BF16)
    attn_heads = mm(weights, kv[:, 64:128])

    phase("scan1wait")
    for arrived in scan1:
        arrived.wait_recv()

    phase("compose")
    entry = []
    for way in range(2):
        m = [mats[k if way == 0 else 3 - k, way].astype(F32) + eye2 for k in range(4)]
        place = y if way == 0 else 3 - y
        two = after(m[1], m[0])
        three = after(m[2], two)
        rowmats[z, way] = (after(after(m[3], m[2]), two) - eye2).astype(LINK)
        entry.append(
            jnp.where(place == 0, eye2, jnp.where(place == 1, m[0], jnp.where(place == 2, two, three)))
        )
    phase("scan2send")
    scan2 = []
    for d in (1, 3, 2):
        goes = jnp.where(z + d < 4, 0, 1)
        comes = jnp.where(z - d >= 0, 0, 1)
        scan2.append(
            send(rowmats.at[z, goes], rowmats.at[z, goes], dev_z(d), rowmats.at[m4(z - d), comes])
        )
    phase("scan2wait")
    for arrived in scan2:
        arrived.wait_recv()
    phase("states")
    states = []
    for way in range(2):
        m = [rowmats[k if way == 0 else 3 - k, way].astype(F32) + eye2 for k in range(3)]
        place = z if way == 0 else 3 - z
        none = jnp.zeros((64, 64), F32)
        two = dot3_deep(m[1][:, 64:128], m[0][:, 0:64]) + m[1][:, 0:64]
        before = jnp.where(place == 3, two, jnp.where(place == 2, m[0][:, 0:64], none))
        last_map = jnp.where(
            place == 3, m[2], jnp.where(place == 2, m[1], jnp.where(place == 1, m[0], eye2))
        )
        joined = after(entry[way], last_map)
        states.append(dot3_deep(joined[:, 64:128], before) + joined[:, 0:64])

    reads_h, reads_l = split(reads_all)
    states_h, states_l = split(jnp.concatenate(states, axis=0))
    whole = mm(
        jnp.concatenate([reads_h, reads_l], axis=1),
        jnp.concatenate([states_h, states_h], axis=0),
    )
    whole = local_sum + whole + mm(reads_h, states_l)
    scaled = whole * lax.rsqrt(jnp.mean(whole * whole, axis=-1, keepdims=True) + EPS) * ogain[...]
    heads = jnp.concatenate([attn_heads, scaled * gate], axis=1).astype(BF16)
    for k in range(4):
        hsend[k, 0:32] = heads[32 * k : 32 * k + 32]
        hsend[k, 32:64] = heads[128 + 32 * k : 160 + 32 * k]
    phase("headsend")
    head_in = [send(hsend.at[m4(x + d)], hall.at[x], dev_x(d), hall.at[m4(x - d)]) for d in (1, 3, 2)]
    hall[x] = hsend[x]
    phase("w2finish")
    out_first.finish()
    out_second.finish()
    phase("headwait")
    for arrived in head_in:
        arrived.wait_recv()
    phase("outmm")
    gathered = jnp.concatenate([hall[k] for k in range(4)], axis=1)
    for k in range(4):
        part = mm(gathered, w2[k].reshape(256, 512), NT)
        pbuf[0, :, 256 * k : 256 * k + 256] = part[0:32]
        pbuf[1, :, 256 * k : 256 * k + 256] = part[32:64]
    phase("last")
    last = send(pbuf.at[o], prec, partner, prec)
    last.wait_recv()
    out[...] = pbuf[c] + prec[...]
    phase("drain")
    for copy in sent:
        copy.wait_send()
    phase(None)


def per_device(
    tokens, norm_gain, attn_query, attn_key, attn_value, sink_logit, delta_query, delta_key, delta_value,
    delta_gate, beta_weight, decay_weight, beta_shift, decay_log, out_gain, attn_out, delta_out,
):
    operands = (
        tokens, norm_gain.reshape(1, -1), attn_query, attn_key, attn_value, delta_query, delta_key, delta_value,
        delta_gate, beta_weight.transpose(1, 2, 0), decay_weight.transpose(1, 2, 0), out_gain.reshape(1, -1),
        attn_out.T, delta_out.T, sink_logit, beta_shift, decay_log,
    )
    hbm = pl.BlockSpec(memory_space=pltpu.HBM)
    vmem = pl.BlockSpec(memory_space=pltpu.VMEM)
    summed = pl.pallas_call(
        layer_kernel,
        out_shape=jax.ShapeDtypeStruct((32, 1024), F32),
        in_specs=[hbm] * 17,
        out_specs=vmem,
        scratch_shapes=[
            pltpu.VMEM((1, 1024), F32),
            pltpu.VMEM((32, 128), BF16),
            pltpu.VMEM((32, 64), BF16),
            pltpu.VMEM((32, 64), BF16),
            pltpu.VMEM((32, 128), BF16),
            pltpu.VMEM((32, 128), BF16),
            pltpu.VMEM((32, 128), BF16),
            pltpu.VMEM((32, 128), BF16),
            pltpu.VMEM((2, 2, 32), BF16),
            pltpu.VMEM((2, 2, 32), BF16),
            pltpu.VMEM((1, 64), F32),
            pltpu.VMEM((32, 128), BF16),
            pltpu.VMEM((32, 128), BF16),
            pltpu.SMEM((2,), F32),
            pltpu.SMEM((2, 2), F32),
            pltpu.SMEM((2, 2), F32),
            pltpu.VMEM((4, 256, 256), BF16),
            pltpu.VMEM((4, 256, 256), BF16),
            pltpu.VMEM((2, 32, 640), BF16),
            pltpu.VMEM((4, 4, 2, 32, 512), BF16),
            pltpu.VMEM((4, 4, 2, 32, 512), BF16),
            pltpu.VMEM((384, 128), BF16),
            pltpu.VMEM((4, 2, 64, 128), LINK),
            pltpu.VMEM((4, 2, 64, 128), LINK),
            pltpu.VMEM((4, 64, 128), BF16),
            pltpu.VMEM((4, 64, 128), BF16),
            pltpu.VMEM((2, 32, 1024), F32),
            pltpu.VMEM((32, 1024), F32),
            pltpu.SemaphoreType.DMA((COPIES,)),
            pltpu.SemaphoreType.DMA((COPIES,)),
            pltpu.SemaphoreType.DMA((18,)),
        ],
        compiler_params=pltpu.CompilerParams(collective_id=0, has_side_effects=True, vmem_limit_bytes=24 * 2**20),
    )(*(pltpu.with_memory_space_constraint(operand, pltpu.HBM) for operand in operands))
    return summed.astype(BF16)


def solution(mesh):
    return jax.shard_map(
        per_device,
        mesh=mesh,
        in_specs=(
            P("sp", "tp"), P(), P("sp", "tp"), P("sp", "tp"), P("sp", "tp"), P("tp"), P("sp", "tp"),
            P("sp", "tp"), P("sp", "tp"), P("sp", "tp"), P("sp", "tp", None), P("sp", "tp", None),
            P(None, "tp"), P(None, "tp"), P(), P("tp", "sp"), P("tp", "sp"),
        ),
        out_specs=P(("sp", "tp"), None),
        check_vma=False,
    )
```

```python
import jax
import jax.numpy as jnp
from jax import lax
from jax.experimental import pallas as pl
from jax.experimental.pallas import tpu as pltpu
from jax.sharding import PartitionSpec as P

HEAD_DIM = 64
WINDOW = 64
ROWS = 256
TOKENS = 4096
EPS = 1e-6
COPIES = 120
MESH = pl.DeviceIdType.MESH
F32 = jnp.float32
BF16 = jnp.bfloat16
LINK = BF16
NN = (((1,), (0,)), ((), ()))
NT = (((1,), (1,)), ((), ()))


def mm(a, b, dims=NN):
    return lax.dot_general(a, b, dims, preferred_element_type=F32)


def split(a):
    hi = a.astype(BF16)
    return hi, (a - hi.astype(F32)).astype(BF16)


def left(a):
    hi, lo = split(a)
    return jnp.concatenate([hi, lo], axis=1)


def right(b):
    hi, lo = split(b)
    return jnp.concatenate(
        [jnp.concatenate([hi, lo], axis=1), jnp.concatenate([hi, jnp.zeros_like(lo)], axis=1)], axis=0
    )


def dot3(a, b):
    both = mm(left(a), right(b))
    return both[:, 0:128] + both[:, 128:256]


def dot3_deep(a, b):
    ah, al = split(a)
    bh, bl = split(b)
    return mm(jnp.concatenate([ah, ah, al], axis=1), jnp.concatenate([bh, bl, bh], axis=0))


def silu(v):
    return v * jax.nn.sigmoid(v)


def layer_kernel(
    tokens_in, gain_in, aq_in, ak_in, av_in, dq_in, dk_in, dv_in, dz_in, bw_in, gw_in, ogain_in, ao_in, do_in,
    sink_in, shift_in, dlog_in,
    out,
    gain, aq, ak, av, dq, dk, dv, dz, bw, gw, ogain, ao, do, sink, shift, dlog,
    tok, normed, stage, w1, w2, kv, own_map, maps_in, hsend, hall, pbuf, prec, send_sem, recv_sem, own_sem,
):
    sp = lax.axis_index("sp")
    x = lax.axis_index("tp")
    c = lax.rem(sp, 2)
    b = lax.div(sp, 2)
    z = lax.div(b, 4)
    y = lax.rem(b, 4)
    o = 1 - c

    open_scopes = []

    def phase(name):
        while open_scopes:
            open_scopes.pop().__exit__(None, None, None)
        if name:
            open_scopes.append(jax.named_scope(name))
            open_scopes[0].__enter__()

    def m4(v):
        return lax.rem(v + 4, 4)

    def dev(zz, yy, cc, xx):
        return {"sp": (zz * 4 + yy) * 2 + cc, "tp": xx}

    def dev_x(d):
        return dev(z, y, c, m4(x + d))

    def dev_y(d, core=c):
        return dev(z, m4(y + d), core, x)

    def dev_z(d, core=c):
        return dev(m4(z + d), y, core, x)

    def dev_b(d):
        bb = lax.rem(b + d + 16, 16)
        return {"sp": bb * 2 + c, "tp": x}

    partner = dev(z, y, o, x)
    sent = []

    def send(src, dst, device, landed):
        i = len(sent)
        copy = pltpu.make_async_remote_copy(
            src_ref=src, dst_ref=dst, send_sem=send_sem.at[i], recv_sem=recv_sem.at[i],
            device_id=device, device_id_type=MESH,
        )
        copy.start()
        sent.append(copy)
        return pltpu.make_async_remote_copy(
            src_ref=landed, dst_ref=landed, send_sem=send_sem.at[i], recv_sem=recv_sem.at[i],
            device_id=device, device_id_type=MESH,
        )

    phase("load")
    half_rows = pl.ds(128 * c, 128)
    other_rows = pl.ds(128 * o, 128)
    tokens = tok.at[x, half_rows]
    loads = [
        pltpu.make_async_copy(src, dst, own_sem.at[i])
        for i, (src, dst) in enumerate(
            [(aq_in, aq), (ak_in, ak), (av_in, av), (dq_in, dq), (dk_in, dk), (dv_in, dv), (dz_in, dz), (bw_in, bw),
             (gw_in, gw), (ao_in, ao), (do_in, do), (tokens_in, tokens), (gain_in, gain), (ogain_in, ogain),
             (sink_in, sink), (shift_in, shift), (dlog_in, dlog)]
        )
    ]
    for load in loads:
        load.start()
    barrier = pltpu.get_barrier_semaphore()
    peers = [partner]
    for d in (1, 2, 3):
        peers += [dev_x(d), dev_y(d), dev_z(d), dev_y(d, o), dev_z(d, o)]
    for peer in peers:
        pl.semaphore_signal(barrier, inc=1, device_id=peer, device_id_type=MESH)
    for load in loads[:11]:
        load.wait()
    phase("pack")
    attn_t, delta_t = ao[...], do[...]
    blank = jnp.zeros((60, 32), F32)
    for cc in range(2):
        cols = slice(64 * cc, 64 * cc + 64)
        small = jnp.concatenate([bw[cc].astype(F32), gw[cc].astype(F32), blank], axis=0).T.astype(BF16)
        stage[cc] = jnp.concatenate(
            [aq[:, cols], dq[:, cols], dk[:, cols], dv[:, cols], dz[:, cols], small, ak[...], av[...],
             attn_t[:, cols], delta_t[:, cols]],
            axis=1,
        )
    w1[z, y, c] = stage[c, :, 0:512]
    w2[x, z, y, c] = stage[c, :, 512:640]

    phase("barrier")
    pl.semaphore_wait(barrier, len(peers))

    class Gather:
        def __init__(self, w, s, y_first, source=None):
            self.w, self.s, self.y_first, self.source = w, s, y_first, source
            self.waits = {}

        def slot(self, first, second):
            zz, yy = (z + second, y + first) if self.y_first else (z + first, y + second)
            return self.w.at[m4(zz), m4(yy), self.s]

        def own(self, device):
            if self.source is None:
                return self.slot(0, 0), self.slot(0, 0), device(c)
            return self.source, self.w.at[z, y, 1 - self.s], device(o)

        def along(self, axis, d, core):
            return dev_y(d, core) if axis == self.y_first else dev_z(d, core)

        def begin(self):
            for d in (1, 3, 2):
                source, place, device = self.own(lambda core, d=d: self.along(True, d, core))
                self.waits[d] = send(source, place, device, self.slot(-d, 0))

        def across(self, f):
            for d in (1, 3, 2):
                if f == 0:
                    source, place, device = self.own(lambda core, d=d: self.along(False, d, core))
                else:
                    source, place, device = self.slot(f, 0), self.slot(f, 0), self.along(False, d, c)
                self.waits[f, d] = send(source, place, device, self.slot(f, -d))

        def forward(self, d):
            self.waits[d].wait_recv()
            self.across(-d)

        def finish(self):
            for d in (1, 3, 2):
                for f in (0, -1, -3, -2):
                    self.waits[f, d].wait_recv()

    in_cols = pl.ds(0, 512)
    out_cols = pl.ds(512, 128)
    phase("start")
    first = Gather(w1, c, True)
    second = Gather(w1, o, False, stage.at[o, :, in_cols])
    out_first = Gather(w2.at[x], c, True)
    out_second = Gather(w2.at[x], o, False, stage.at[o, :, out_cols])
    first.begin()
    second.begin()
    first.across(0)
    second.across(0)
    for load in loads[11:]:
        load.wait()
    tok_in = [send(tokens, tokens, dev_x(d), tok.at[m4(x - d), half_rows]) for d in (1, 3, 2)]
    w_swap = send(stage.at[o, :, in_cols], w1.at[z, y, c], partner, w1.at[z, y, o])
    tok_swap = [send(tokens, tokens, partner, tok.at[x, other_rows])]
    w2_swap = send(stage.at[o, :, out_cols], w2.at[x, z, y, c], partner, w2.at[x, z, y, o])
    phase("near")
    for d in (1, 3, 2):
        first.forward(d)
        second.forward(d)
    for ring in (out_first, out_second):
        ring.begin()
        ring.across(0)
    phase("tokens")
    for d, arrived in zip((1, 3, 2), tok_in):
        arrived.wait_recv()
        src = m4(x - d)
        tok_swap.append(send(tok.at[src, half_rows], tok.at[src, half_rows], partner, tok.at[src, other_rows]))
    phase("tokswap")
    for arrived in tok_swap:
        arrived.wait_recv()

    phase("norm")
    squares = jnp.zeros((ROWS, 1), F32)
    for k in range(4):
        wide = tok[k].astype(F32)
        squares = squares + jnp.sum(wide * wide, axis=-1, keepdims=True)
    inv = lax.rsqrt(squares * (1.0 / 1024.0) + EPS)
    for k in range(4):
        normed[k] = (tok[k].astype(F32) * inv * gain[:, 256 * k : 256 * k + 256]).astype(BF16)

    phase("w2near")
    for d in (1, 3, 2):
        out_first.forward(d)
        out_second.forward(d)
    phase("wfinish")
    w_swap.wait_recv()
    first.finish()
    second.finish()

    phase("proj")
    proj = mm(normed[0], w1[0].reshape(256, 512))
    for k in range(1, 4):
        proj = proj + mm(normed[k], w1[k].reshape(256, 512))
    phase("gates0")
    t0, t1, t2 = proj[:, 0:128], proj[:, 128:256], proj[:, 256:384]
    kv[64:320, :] = proj[:, 384:512].astype(BF16)
    halo = [
        send(kv.at[pl.ds(256, 64)], kv.at[pl.ds(0, 64)], dev_b(1), kv.at[pl.ds(0, 64)]),
        send(kv.at[pl.ds(64, 64)], kv.at[pl.ds(320, 64)], dev_b(-1), kv.at[pl.ds(320, 64)]),
    ]
    att_q = t0[:, 0:64].astype(BF16)
    act_q = silu(t0[:, 64:128].astype(BF16).astype(F32))
    act_kv = silu(t1.astype(BF16).astype(F32))
    act_k, val = act_kv[:, 0:64], act_kv[:, 64:128]
    q = act_q * lax.rsqrt(jnp.sum(act_q * act_q, axis=-1, keepdims=True) + EPS) * HEAD_DIM**-0.5
    key = act_k * lax.rsqrt(jnp.sum(act_k * act_k, axis=-1, keepdims=True) + EPS)
    gate = silu(t2[:, 0:64].astype(BF16).astype(F32))

    phase("gates")
    lane = lax.broadcasted_iota(jnp.int32, (1, 128), 1)
    bias = jnp.where(lane == 64, shift[0, c], jnp.where(lane == 65, shift[1, c], 0.0))
    rate = jnp.exp(jnp.where(lane == 66, dlog[0, c], jnp.where(lane == 67, dlog[1, c], 0.0)))
    strength = jax.nn.sigmoid(t2 + bias)
    softplus = jnp.maximum(t2, 0.0) + jnp.log1p(jnp.exp(-jnp.abs(t2)))
    decay = jnp.where((lane == 66) | (lane == 67), -rate * softplus * (1.0 / TOKENS), 0.0)

    row = lax.broadcasted_iota(jnp.int32, (128, 128), 0)
    col = lax.broadcasted_iota(jnp.int32, (128, 128), 1)
    masks = (row >= col, row <= col)
    unit = jnp.where(row == col, 1.0, 0.0)
    near16 = lax.shift_right_logical(row, 4) == lax.shift_right_logical(col, 4)

    g_hi = decay.astype(BF16)
    rest = decay - g_hi.astype(F32)
    g_mid = rest.astype(BF16)
    g_lo = (rest - g_mid.astype(F32)).astype(BF16)
    g_parts = jnp.concatenate(
        [part[128 * h : 128 * h + 128, 64:128] for h in range(2) for part in (g_hi, g_mid, g_lo)], axis=1
    )
    sums = [mm(jnp.where(mask, 1.0, 0.0).astype(BF16), g_parts) for mask in masks]
    sub = lax.broadcasted_iota(jnp.int32, (1, 192), 1)
    picked = jnp.where((sub & 63) == 2, sums[0][:, 0:192], sums[1][:, 0:192])
    picked2 = jnp.where((sub & 63) == 2, sums[0][:, 192:384], sums[1][:, 192:384])
    g_all = jnp.concatenate([p[:, 0:64] + p[:, 64:128] + p[:, 128:192] for p in (picked, picked2)], axis=0)
    turned = jnp.concatenate([key, g_all], axis=1).T
    key_t = turned[0:64]
    key_h, key_l = split(key)
    q_h, q_l = split(q)
    kt_h, kt_l = split(key_t)
    q3 = jnp.concatenate([q_h, q_h, q_l], axis=1)
    key3 = jnp.concatenate([key_h, key_h, key_l], axis=1)
    kt3 = jnp.concatenate([kt_h, kt_l, kt_h], axis=0)

    phase("rings")
    w2_swap.wait_recv()
    out_first.finish()
    out_second.finish()
    w2_in = [send(w2.at[x], w2.at[x], dev_x(d), w2.at[m4(x - d)]) for d in (1, 3, 2)]
    phase("delta1")
    lane2 = lax.broadcasted_iota(jnp.int32, (64, 128), 1)
    row2 = lax.broadcasted_iota(jnp.int32, (64, 128), 0)
    eye2 = jnp.where(lane2 == row2 + 64, 1.0, 0.0)
    chains = [(way, h) for way in range(2) for h in range(2)]
    low, scores_d, sides, grown, key_end, end, d = {}, {}, {}, {}, {}, {}, {}
    for h in range(2):
        hs = slice(128 * h, 128 * h + 128)
        pairs = mm(jnp.concatenate([q3[hs], key3[hs]], axis=0), kt3[:, hs])
        for way in range(2):
            at = way, h
            beta = strength[hs, 64 + way : 65 + way]
            g_col = g_all[hs, 2 + way : 3 + way]
            g_row = turned[66 + way : 67 + way, hs]
            g_end = g_col[127:128] if way == 0 else g_col[0:1]
            decays = jnp.exp(jnp.where(masks[way], g_col - g_row, -jnp.inf))
            low[at] = jnp.where(row == col, 0.0, beta * pairs[128:256] * decays)
            scores_d[at] = pairs[0:128] * decays
            up = jnp.exp(g_col)
            grown[at] = up * q[hs]
            sides[at] = jnp.concatenate([beta * val[hs], (beta * up) * key[hs]], axis=1)
            key_end[at] = key_t[:, hs] * jnp.exp(g_end - g_row)
            end[at] = jnp.exp(g_end)
    d1 = {at: jnp.where(near16, low[at], 0.0) for at in chains}
    off = {at: jnp.where(near16, 0.0, low[at]) for at in chains}
    d2 = {at: dot3(d1[at], d1[at]) for at in chains}
    inner = {at: unit - d1[at] for at in chains}
    d4 = {at: dot3(d2[at], d2[at]) for at in chains}
    inner = {at: inner[at] + dot3(inner[at], d2[at]) for at in chains}
    d8 = {at: dot3(d4[at], d4[at]) for at in chains}
    inner = {at: inner[at] + dot3(inner[at], d4[at]) for at in chains}
    inner = {at: inner[at] + dot3(inner[at], d8[at]) for at in chains}
    phase("delta2")
    m1 = {at: dot3(inner[at], off[at]) for at in chains}
    uw = {at: dot3(inner[at], sides[at]) for at in chains}
    m2 = {at: dot3(m1[at], m1[at]) for at in chains}
    uw = {at: uw[at] - dot3(m1[at], uw[at]) for at in chains}
    m4_ = {at: dot3(m2[at], m2[at]) for at in chains}
    uw = {at: uw[at] + dot3(m2[at], uw[at]) for at in chains}
    uw = {at: uw[at] + dot3(m4_[at], uw[at]) for at in chains}
    phase("final")

    def after(later, earlier):
        return dot3_deep(later[:, 64:128], earlier) + later + earlier

    maps = {}
    for at in chains:
        final = dot3(key_end[at], uw[at])
        maps[at] = jnp.where(lane2 < 64, final, (end[at] - 1.0) * eye2 - final)
    for way in range(2):
        own_map[way] = after(maps[way, 1 - way], maps[way, way]).astype(LINK)
    phase("scan1send")
    scan = []
    steps = [(dz, dy) for dz in range(4) for dy in range(4) if (dz, dy) != (0, 0)]
    for dz, dy in sorted(steps, key=lambda step: -(min(step[0], 4 - step[0]) + min(step[1], 4 - step[1]))):
        zz, yy = m4(z + dz), m4(y + dy)
        goes = jnp.where(zz * 4 + yy > b, 0, 1)
        scan.append(
            send(own_map.at[goes], maps_in.at[z, y], dev(zz, yy, c, x), maps_in.at[m4(z - dz), m4(y - dy)])
        )
    phase("reads")
    local, reads = {}, {}
    for way, h in chains:
        at = way, h
        read = dot3(scores_d[at], uw[at])
        local[at] = read[:, 0:64]
        reads[at] = grown[at] - read[:, 64:128]
        if h != way:
            passed = dot3_deep(reads[at], maps[way, way])
            local[at] = local[at] + passed[:, 0:64]
            reads[at] = reads[at] + passed[:, 64:128]
    local_sum = jnp.concatenate([local[0, h] + local[1, h] for h in range(2)], axis=0)
    reads_all = jnp.concatenate(
        [jnp.concatenate([reads[0, h], reads[1, h]], axis=1) for h in range(2)], axis=0
    )

    phase("halo")
    for arrived in halo:
        arrived.wait_recv()
    phase("attn")
    scores = mm(att_q, kv[:, 0:64], NT) * HEAD_DIM**-0.5
    q_pos = lax.broadcasted_iota(jnp.int32, (ROWS, ROWS + 2 * WINDOW), 0)
    k_pos = lax.broadcasted_iota(jnp.int32, (ROWS, ROWS + 2 * WINDOW), 1) - WINDOW
    seen = k_pos + b * ROWS
    allowed = (jnp.abs(q_pos - k_pos) <= WINDOW) & (seen >= 0) & (seen < TOKENS)
    scores = jnp.where(allowed, scores, -jnp.inf)
    top = jnp.maximum(jnp.max(scores, axis=-1, keepdims=True), sink[c])
    weights = jnp.exp(scores - top)
    total = jnp.sum(weights, axis=-1, keepdims=True) + jnp.exp(sink[c] - top)
    weights = (weights / total).astype(BF16)
    attn_heads = mm(weights, kv[:, 64:128])

    phase("scanwait")
    for arrived in scan:
        arrived.wait_recv()
    phase("states")
    states = []
    for way in range(2):
        order = range(16) if way == 0 else range(15, -1, -1)
        chain = []
        for k in order:
            inside = (b > k) if way == 0 else (b < k)
            chain.append(jnp.where(inside, maps_in[k // 4, k % 4], jnp.zeros((64, 128), LINK)))
        level = []
        for k in range(0, 14, 2):
            earlier, later = chain[k], chain[k + 1]
            level.append(mm(later[:, 64:128], earlier) + later.astype(F32) + earlier.astype(F32))
        level.append(chain[14].astype(F32))
        while len(level) > 2:
            level = [after(level[k + 1], level[k]) for k in range(0, len(level), 2)]
        start = level[0][:, 0:64]
        states.append(dot3_deep(level[1][:, 64:128], start) + start + level[1][:, 0:64])

    reads_h, reads_l = split(reads_all)
    states_h, states_l = split(jnp.concatenate(states, axis=0))
    whole = mm(
        jnp.concatenate([reads_h, reads_l], axis=1),
        jnp.concatenate([states_h, states_h], axis=0),
    )
    whole = local_sum + whole + mm(reads_h, states_l)
    scaled = whole * lax.rsqrt(jnp.mean(whole * whole, axis=-1, keepdims=True) + EPS) * ogain[...]
    heads = jnp.concatenate([attn_heads, scaled * gate], axis=1).astype(BF16)
    phase("headsend0")
    for k in range(4):
        hsend[k, 0:32] = heads[32 * k : 32 * k + 32]
        hsend[k, 32:64] = heads[128 + 32 * k : 160 + 32 * k]
    phase("headsend")
    head_in = [send(hsend.at[m4(x + d)], hall.at[x], dev_x(d), hall.at[m4(x - d)]) for d in (1, 3, 2)]
    hall[x] = hsend[x]
    phase("w2finish")
    for arrived in w2_in:
        arrived.wait_recv()
    phase("headwait")
    for arrived in head_in:
        arrived.wait_recv()
    phase("outmm")
    gathered = jnp.concatenate([hall[k] for k in range(4)], axis=1)
    for k in range(4):
        rows = jnp.concatenate([w2[kx, k].reshape(256, 128) for kx in range(4)], axis=1)
        part = mm(gathered, rows, NT)
        pbuf[0, :, 256 * k : 256 * k + 256] = part[0:32]
        pbuf[1, :, 256 * k : 256 * k + 256] = part[32:64]
    phase("last")
    last = send(pbuf.at[o], prec, partner, prec)
    last.wait_recv()
    out[...] = pbuf[c] + prec[...]
    phase("drain")
    for copy in sent:
        copy.wait_send()
    phase(None)


def per_device(
    tokens, norm_gain, attn_query, attn_key, attn_value, sink_logit, delta_query, delta_key, delta_value,
    delta_gate, beta_weight, decay_weight, beta_shift, decay_log, out_gain, attn_out, delta_out,
):
    operands = (
        tokens, norm_gain.reshape(1, -1), attn_query, attn_key, attn_value, delta_query, delta_key, delta_value,
        delta_gate, beta_weight.transpose(1, 2, 0), decay_weight.transpose(1, 2, 0), out_gain.reshape(1, -1),
        attn_out.T, delta_out.T, sink_logit, beta_shift, decay_log,
    )
    hbm = pl.BlockSpec(memory_space=pltpu.HBM)
    vmem = pl.BlockSpec(memory_space=pltpu.VMEM)
    summed = pl.pallas_call(
        layer_kernel,
        out_shape=jax.ShapeDtypeStruct((32, 1024), F32),
        in_specs=[hbm] * 17,
        out_specs=vmem,
        scratch_shapes=[
            pltpu.VMEM((1, 1024), F32),
            pltpu.VMEM((32, 128), BF16),
            pltpu.VMEM((32, 64), BF16),
            pltpu.VMEM((32, 64), BF16),
            pltpu.VMEM((32, 128), BF16),
            pltpu.VMEM((32, 128), BF16),
            pltpu.VMEM((32, 128), BF16),
            pltpu.VMEM((32, 128), BF16),
            pltpu.VMEM((2, 2, 32), BF16),
            pltpu.VMEM((2, 2, 32), BF16),
            pltpu.VMEM((1, 64), F32),
            pltpu.VMEM((32, 128), BF16),
            pltpu.VMEM((32, 128), BF16),
            pltpu.SMEM((2,), F32),
            pltpu.SMEM((2, 2), F32),
            pltpu.SMEM((2, 2), F32),
            pltpu.VMEM((4, 256, 256), BF16),
            pltpu.VMEM((4, 256, 256), BF16),
            pltpu.VMEM((2, 32, 640), BF16),
            pltpu.VMEM((4, 4, 2, 32, 512), BF16),
            pltpu.VMEM((4, 4, 4, 2, 32, 128), BF16),
            pltpu.VMEM((384, 128), BF16),
            pltpu.VMEM((2, 64, 128), LINK),
            pltpu.VMEM((4, 4, 64, 128), LINK),
            pltpu.VMEM((4, 64, 128), BF16),
            pltpu.VMEM((4, 64, 128), BF16),
            pltpu.VMEM((2, 32, 1024), F32),
            pltpu.VMEM((32, 1024), F32),
            pltpu.SemaphoreType.DMA((COPIES,)),
            pltpu.SemaphoreType.DMA((COPIES,)),
            pltpu.SemaphoreType.DMA((18,)),
        ],
        compiler_params=pltpu.CompilerParams(collective_id=0, has_side_effects=True, vmem_limit_bytes=24 * 2**20),
    )(*(pltpu.with_memory_space_constraint(operand, pltpu.HBM) for operand in operands))
    return summed.astype(BF16)


def solution(mesh):
    return jax.shard_map(
        per_device,
        mesh=mesh,
        in_specs=(
            P("sp", "tp"), P(), P("sp", "tp"), P("sp", "tp"), P("sp", "tp"), P("tp"), P("sp", "tp"),
            P("sp", "tp"), P("sp", "tp"), P("sp", "tp"), P("sp", "tp", None), P("sp", "tp", None),
            P(None, "tp"), P(None, "tp"), P(), P("tp", "sp"), P("tp", "sp"),
        ),
        out_specs=P(("sp", "tp"), None),
        check_vma=False,
    )
```

```python
import jax
import jax.numpy as jnp
from jax import lax
from jax.experimental import pallas as pl
from jax.experimental.pallas import tpu as pltpu
from jax.sharding import PartitionSpec as P

HEAD_DIM = 64
WINDOW = 64
ROWS = 256
TOKENS = 4096
EPS = 1e-6
COPIES = 120
MESH = pl.DeviceIdType.MESH
F32 = jnp.float32
BF16 = jnp.bfloat16
LINK = BF16
NN = (((1,), (0,)), ((), ()))
NT = (((1,), (1,)), ((), ()))


def mm(a, b, dims=NN):
    return lax.dot_general(a, b, dims, preferred_element_type=F32)


def split(a):
    hi = a.astype(BF16)
    return hi, (a - hi.astype(F32)).astype(BF16)


def left(a):
    hi, lo = split(a)
    return jnp.concatenate([hi, lo], axis=1)


def right(b):
    hi, lo = split(b)
    return jnp.concatenate(
        [jnp.concatenate([hi, lo], axis=1), jnp.concatenate([hi, jnp.zeros_like(lo)], axis=1)], axis=0
    )


def dot3(a, b):
    both = mm(left(a), right(b))
    return both[:, 0:128] + both[:, 128:256]


def right64(b):
    hi, lo = split(b)
    none = jnp.zeros_like(lo)
    blank = jnp.concatenate([none, none], axis=1)
    return jnp.concatenate(
        [jnp.concatenate([hi, lo], axis=1), blank, jnp.concatenate([hi, none], axis=1), blank], axis=0
    )


def dot64(a, b):
    both = mm(left(a), right64(b))
    return both[:, 0:128] + both[:, 128:256]


def silu(v):
    return v * jax.nn.sigmoid(v)


def layer_kernel(
    tokens_in, gain_in, aq_in, ak_in, av_in, dq_in, dk_in, dv_in, dz_in, bw_in, gw_in, ogain_in, ao_in, do_in,
    sink_in, shift_in, dlog_in,
    out,
    gain, aq, ak, av, dq, dk, dv, dz, bw, gw, ogain, ao, do, sink, shift, dlog,
    tok, normed, stage, w1, w2, kv, own_map, maps_in, hsend, hall, pbuf, prec, send_sem, recv_sem, own_sem,
):
    sp = lax.axis_index("sp")
    x = lax.axis_index("tp")
    c = lax.rem(sp, 2)
    b = lax.div(sp, 2)
    z = lax.div(b, 4)
    y = lax.rem(b, 4)
    o = 1 - c

    open_scopes = []

    def phase(name):
        while open_scopes:
            open_scopes.pop().__exit__(None, None, None)
        if name:
            open_scopes.append(jax.named_scope(name))
            open_scopes[0].__enter__()

    def m4(v):
        return lax.rem(v + 4, 4)

    def dev(zz, yy, cc, xx):
        return {"sp": (zz * 4 + yy) * 2 + cc, "tp": xx}

    def dev_x(d):
        return dev(z, y, c, m4(x + d))

    def dev_y(d, core=c):
        return dev(z, m4(y + d), core, x)

    def dev_z(d, core=c):
        return dev(m4(z + d), y, core, x)

    def dev_b(d):
        bb = lax.rem(b + d + 16, 16)
        return {"sp": bb * 2 + c, "tp": x}

    partner = dev(z, y, o, x)
    sent = []

    def send(src, dst, device, landed):
        i = len(sent)
        copy = pltpu.make_async_remote_copy(
            src_ref=src, dst_ref=dst, send_sem=send_sem.at[i], recv_sem=recv_sem.at[i],
            device_id=device, device_id_type=MESH,
        )
        copy.start()
        sent.append(copy)
        return pltpu.make_async_remote_copy(
            src_ref=landed, dst_ref=landed, send_sem=send_sem.at[i], recv_sem=recv_sem.at[i],
            device_id=device, device_id_type=MESH,
        )

    phase("load")
    half_rows = pl.ds(128 * c, 128)
    other_rows = pl.ds(128 * o, 128)
    tokens = tok.at[x, half_rows]
    loads = [
        pltpu.make_async_copy(src, dst, own_sem.at[i])
        for i, (src, dst) in enumerate(
            [(aq_in, aq), (ak_in, ak), (av_in, av), (dq_in, dq), (dk_in, dk), (dv_in, dv), (dz_in, dz), (bw_in, bw),
             (gw_in, gw), (ao_in, ao), (do_in, do), (tokens_in, tokens), (gain_in, gain), (ogain_in, ogain),
             (sink_in, sink), (shift_in, shift), (dlog_in, dlog)]
        )
    ]
    for load in loads:
        load.start()
    barrier = pltpu.get_barrier_semaphore()
    peers = [partner]
    for d in (1, 2, 3):
        peers += [dev_x(d), dev_y(d), dev_z(d), dev_y(d, o), dev_z(d, o)]
    for peer in peers:
        pl.semaphore_signal(barrier, inc=1, device_id=peer, device_id_type=MESH)
    for load in loads[:11]:
        load.wait()
    phase("pack")
    attn_t, delta_t = ao[...], do[...]
    blank = jnp.zeros((60, 32), F32)
    for cc in range(2):
        cols = slice(64 * cc, 64 * cc + 64)
        small = jnp.concatenate([bw[cc].astype(F32), gw[cc].astype(F32), blank], axis=0).T.astype(BF16)
        stage[cc] = jnp.concatenate(
            [dq[:, cols], aq[:, cols], dk[:, cols], dv[:, cols], dz[:, cols], small, av[...], ak[...],
             attn_t[:, cols], delta_t[:, cols]],
            axis=1,
        )
    w1[z, y, c] = stage[c, :, 0:512]
    w2[x, z, y, c] = stage[c, :, 512:640]

    phase("barrier")
    pl.semaphore_wait(barrier, len(peers))

    class Gather:
        def __init__(self, place, y_first, source=None, twin=None):
            self.place, self.y_first, self.source, self.twin = place, y_first, source, twin
            self.waits = {}

        def slot(self, first, second):
            zz, yy = (z + second, y + first) if self.y_first else (z + first, y + second)
            return self.place(m4(zz), m4(yy))

        def own(self, axis, d):
            device = dev_y if axis == self.y_first else dev_z
            if self.source is None:
                return self.slot(0, 0), self.slot(0, 0), device(d)
            return self.source, self.twin, device(d, o)

        def begin(self):
            for d in (1, 3, 2):
                self.waits[d] = send(*self.own(True, d), self.slot(-d, 0))
            for d in (1, 3, 2):
                self.waits[0, d] = send(*self.own(False, d), self.slot(0, -d))

        def forward(self, d):
            self.waits[d].wait_recv()
            block = self.slot(-d, 0)
            for e in (1, 3, 2):
                device = dev_z(e) if self.y_first else dev_y(e)
                self.waits[-d, e] = send(block, block, device, self.slot(-d, -e))

        def finish(self):
            for e in (1, 3, 2):
                for f in (0, -1, -3, -2):
                    self.waits[f, e].wait_recv()

    in_cols = pl.ds(0, 512)
    out_cols = pl.ds(512, 128)
    phase("start")
    first = Gather(lambda zz, yy: w1.at[zz, yy, c], True)
    second = Gather(lambda zz, yy: w1.at[zz, yy, o], False, stage.at[o, :, in_cols], w1.at[z, y, c])
    out_low = Gather(lambda zz, yy: w2.at[:, zz, yy, c, pl.ds(0, 16)], True)
    out_high = Gather(lambda zz, yy: w2.at[:, zz, yy, c, pl.ds(16, 16)], False)
    out_twin = Gather(
        lambda zz, yy: w2.at[x, zz, yy, o], False, stage.at[o, :, out_cols], w2.at[x, z, y, c]
    )
    first.begin()
    second.begin()
    out_twin.begin()
    for load in loads[11:]:
        load.wait()
    tok_in = [send(tokens, tokens, dev_x(d), tok.at[m4(x - d), half_rows]) for d in (1, 3, 2)]
    w2_own = [
        send(stage.at[c, :, out_cols], w2.at[x, z, y, c], dev_x(d), w2.at[m4(x - d), z, y, c]) for d in (1, 3, 2)
    ]
    w_swap = send(stage.at[o, :, in_cols], w1.at[z, y, c], partner, w1.at[z, y, o])
    tok_swap = [send(tokens, tokens, partner, tok.at[x, other_rows])]
    w2_swap = send(stage.at[o, :, out_cols], w2.at[x, z, y, c], partner, w2.at[x, z, y, o])
    phase("near")
    for d in (1, 3, 2):
        first.forward(d)
        second.forward(d)
    for d in (1, 3, 2):
        out_twin.forward(d)
    for arrived in w2_own:
        arrived.wait_recv()
    out_low.begin()
    out_high.begin()
    phase("tokens")
    for d, arrived in zip((1, 3, 2), tok_in):
        arrived.wait_recv()
        src = m4(x - d)
        tok_swap.append(send(tok.at[src, half_rows], tok.at[src, half_rows], partner, tok.at[src, other_rows]))
    phase("tokswap")
    for arrived in tok_swap:
        arrived.wait_recv()

    phase("norm")
    squares = jnp.zeros((ROWS, 1), F32)
    for k in range(4):
        wide = tok[k].astype(F32)
        squares = squares + jnp.sum(wide * wide, axis=-1, keepdims=True)
    inv = lax.rsqrt(squares * (1.0 / 1024.0) + EPS)
    for k in range(4):
        normed[k] = (tok[k].astype(F32) * inv * gain[:, 256 * k : 256 * k + 256]).astype(BF16)

    phase("wfinish")
    w_swap.wait_recv()
    first.finish()
    second.finish()

    phase("proj")
    proj = mm(normed[0], w1[0].reshape(256, 512))
    for k in range(1, 4):
        proj = proj + mm(normed[k], w1[k].reshape(256, 512))
    phase("gates0")
    t0, t1, t2 = proj[:, 0:128], proj[:, 128:256], proj[:, 256:384]
    kv[64:320, :] = proj[:, 384:512].astype(BF16)
    halo = [
        send(kv.at[pl.ds(256, 64)], kv.at[pl.ds(0, 64)], dev_b(1), kv.at[pl.ds(0, 64)]),
        send(kv.at[pl.ds(64, 64)], kv.at[pl.ds(320, 64)], dev_b(-1), kv.at[pl.ds(320, 64)]),
    ]
    lane = lax.broadcasted_iota(jnp.int32, (1, 128), 1)
    head = lane < 64
    act = silu(t0.astype(BF16).astype(F32))
    act = jnp.where(head, act, 0.0)
    q = act * (lax.rsqrt(jnp.sum(act * act, axis=-1, keepdims=True) + EPS) * HEAD_DIM**-0.5)
    act = silu(t1.astype(BF16).astype(F32))
    act_k = jnp.where(head, act, 0.0)
    key_val = jnp.where(head, act * lax.rsqrt(jnp.sum(act_k * act_k, axis=-1, keepdims=True) + EPS), act)

    phase("gates")
    bias = jnp.where(lane == 64, shift[0, c], jnp.where(lane == 65, shift[1, c], 0.0))
    rate = jnp.exp(jnp.where(lane == 66, dlog[0, c], jnp.where(lane == 67, dlog[1, c], 0.0)))
    strength = jax.nn.sigmoid(t2 + bias)
    softplus = jnp.maximum(t2, 0.0) + jnp.log1p(jnp.exp(-jnp.abs(t2)))
    decay = jnp.where((lane == 66) | (lane == 67), -rate * softplus * (1.0 / TOKENS), 0.0)

    row = lax.broadcasted_iota(jnp.int32, (128, 128), 0)
    col = lax.broadcasted_iota(jnp.int32, (128, 128), 1)
    masks = (row >= col, row <= col)
    unit = jnp.where(row == col, 1.0, 0.0)
    near16 = lax.shift_right_logical(row, 4) == lax.shift_right_logical(col, 4)

    g_hi = decay.astype(BF16)
    rest = decay - g_hi.astype(F32)
    g_mid = rest.astype(BF16)
    g_lo = (rest - g_mid.astype(F32)).astype(BF16)
    g_parts = jnp.concatenate(
        [jnp.concatenate([part[0:128], part[128:256]], axis=1) for part in (g_hi, g_mid, g_lo)], axis=0
    )
    ones = jnp.concatenate([jnp.where(mask, 1.0, 0.0).astype(BF16) for mask in masks], axis=0)
    sums = mm(jnp.concatenate([ones, ones, ones], axis=1), g_parts)
    g_all = jnp.where(
        lane == 66,
        jnp.concatenate([sums[0:128, 0:128], sums[0:128, 128:256]], axis=0),
        jnp.concatenate([sums[128:256, 0:128], sums[128:256, 128:256]], axis=0),
    )
    turned = jnp.where(head, key_val, g_all).T
    key_t = turned[0:64]
    q_left, key_left = left(q), left(key_val)

    phase("rings")
    w2_swap.wait_recv()
    for d in (1, 3, 2):
        out_low.forward(d)
        out_high.forward(d)
    out_twin.finish()
    w2_in = [send(w2.at[x, :, :, o], w2.at[x, :, :, o], dev_x(d), w2.at[m4(x - d), :, :, o]) for d in (1, 3, 2)]

    phase("delta1")
    lane2 = lax.broadcasted_iota(jnp.int32, (64, 128), 1)
    row2 = lax.broadcasted_iota(jnp.int32, (64, 128), 0)
    eye2 = jnp.where(lane2 == row2, 1.0, 0.0)
    chains = [(way, h) for way in range(2) for h in range(2)]
    low, scores_d, sides, grown, key_end, end = {}, {}, {}, {}, {}, {}
    for h in range(2):
        hs = slice(128 * h, 128 * h + 128)
        pairs = mm(jnp.concatenate([q_left[hs], key_left[hs]], axis=0), right64(key_t[:, hs]))
        pairs = pairs[:, 0:128] + pairs[:, 128:256]
        for way in range(2):
            at = way, h
            beta = strength[hs, 64 + way : 65 + way]
            g_col = g_all[hs, 66 + way : 67 + way]
            g_row = turned[66 + way : 67 + way, hs]
            g_end = g_col[127:128] if way == 0 else g_col[0:1]
            decays = jnp.exp(jnp.where(masks[way], g_col - g_row, -jnp.inf))
            low[at] = jnp.where(row == col, 0.0, beta * pairs[128:256] * decays)
            scores_d[at] = pairs[0:128] * decays
            up = jnp.exp(g_col)
            grown[at] = up * q[hs]
            sides[at] = key_val[hs] * jnp.where(head, beta * up, beta)
            key_end[at] = key_t[:, hs] * jnp.exp(g_end - g_row)
            end[at] = jnp.exp(g_end)
    d1 = {at: jnp.where(near16, low[at], 0.0) for at in chains}
    off = {at: jnp.where(near16, 0.0, low[at]) for at in chains}
    d2 = {at: dot3(d1[at], d1[at]) for at in chains}
    inner = {at: unit - d1[at] for at in chains}
    d4 = {at: dot3(d2[at], d2[at]) for at in chains}
    inner = {at: inner[at] + dot3(inner[at], d2[at]) for at in chains}
    d8 = {at: dot3(d4[at], d4[at]) for at in chains}
    inner = {at: inner[at] + dot3(inner[at], d4[at]) for at in chains}
    inner = {at: inner[at] + dot3(inner[at], d8[at]) for at in chains}
    phase("delta2")
    m1 = {at: dot3(inner[at], off[at]) for at in chains}
    wu = {at: dot3(inner[at], sides[at]) for at in chains}
    m2 = {at: dot3(m1[at], m1[at]) for at in chains}
    wu = {at: wu[at] - dot3(m1[at], wu[at]) for at in chains}
    m4_ = {at: dot3(m2[at], m2[at]) for at in chains}
    wu = {at: wu[at] + dot3(m2[at], wu[at]) for at in chains}
    wu = {at: wu[at] + dot3(m4_[at], wu[at]) for at in chains}
    phase("final")

    def after(later, earlier):
        return dot64(later, earlier) + later + earlier

    maps = {}
    for at in chains:
        final = dot3(key_end[at], wu[at])
        maps[at] = jnp.where(lane2 < 64, (end[at] - 1.0) * eye2 - final, final)
    for way in range(2):
        own_map[way] = after(maps[way, 1 - way], maps[way, way]).astype(LINK)
    phase("scan1send")
    scan = []
    steps = [(dz, dy) for dz in range(4) for dy in range(4) if (dz, dy) != (0, 0)]
    for dz, dy in sorted(steps, key=lambda step: -(min(step[0], 4 - step[0]) + min(step[1], 4 - step[1]))):
        zz, yy = m4(z + dz), m4(y + dy)
        goes = jnp.where(zz * 4 + yy > b, 0, 1)
        scan.append(
            send(own_map.at[goes], maps_in.at[z, y], dev(zz, yy, c, x), maps_in.at[m4(z - dz), m4(y - dy)])
        )
    phase("reads")
    reads = {}
    for way, h in chains:
        at = way, h
        read = dot3(scores_d[at], wu[at])
        reads[at] = jnp.where(head, grown[at] - read, read)
        if h != way:
            reads[at] = reads[at] + dot64(reads[at], maps[way, way])
    reads = [jnp.concatenate([reads[way, 0], reads[way, 1]], axis=0) for way in range(2)]
    reads_left = [left(r) for r in reads]
    local = reads[0] + reads[1]
    gate = silu(t2.astype(BF16).astype(F32))
    gate = jnp.concatenate([gate[:, 64:128], gate[:, 0:64]], axis=1)
    gain_row = jnp.concatenate([ogain[...], ogain[...]], axis=1)

    phase("halo")
    for arrived in halo:
        arrived.wait_recv()
    phase("attn")
    att_q = jnp.where(head, 0.0, t0).astype(BF16)
    scores = mm(att_q, kv[...], NT) * HEAD_DIM**-0.5
    q_pos = lax.broadcasted_iota(jnp.int32, (ROWS, ROWS + 2 * WINDOW), 0)
    k_pos = lax.broadcasted_iota(jnp.int32, (ROWS, ROWS + 2 * WINDOW), 1) - WINDOW
    seen = k_pos + b * ROWS
    allowed = (jnp.abs(q_pos - k_pos) <= WINDOW) & (seen >= 0) & (seen < TOKENS)
    scores = jnp.where(allowed, scores, -jnp.inf)
    top = jnp.maximum(jnp.max(scores, axis=-1, keepdims=True), sink[c])
    weights = jnp.exp(scores - top)
    total = jnp.sum(weights, axis=-1, keepdims=True) + jnp.exp(sink[c] - top)
    weights = (weights / total).astype(BF16)
    attn_heads = mm(weights, kv[...])

    phase("scanwait")
    for arrived in scan:
        arrived.wait_recv()
    phase("states")
    states = []
    for way in range(2):
        order = range(16) if way == 0 else range(15, -1, -1)
        chain = []
        for k in order:
            inside = (b > k) if way == 0 else (b < k)
            chain.append(jnp.where(inside, maps_in[k // 4, k % 4], jnp.zeros((64, 128), LINK)))
        level = []
        for k in range(0, 14, 2):
            earlier, later = chain[k], chain[k + 1]
            level.append(
                mm(later, jnp.concatenate([earlier, jnp.zeros_like(earlier)], axis=0))
                + later.astype(F32)
                + earlier.astype(F32)
            )
        level.append(chain[14].astype(F32))
        while len(level) > 1:
            level = [after(level[k + 1], level[k]) for k in range(0, len(level), 2)]
        states.append(jnp.where(lane2 < 64, 0.0, level[0]))

    phase("whole")
    both = mm(reads_left[0], right64(states[0])) + mm(reads_left[1], right64(states[1]))
    whole = jnp.where(head, 0.0, local + both[:, 0:128] + both[:, 128:256])
    scaled = whole * lax.rsqrt(jnp.sum(whole * whole, axis=-1, keepdims=True) * (1.0 / HEAD_DIM) + EPS) * gain_row
    heads = jnp.where(head, attn_heads, scaled * gate).astype(BF16)
    phase("headsend0")
    for k in range(4):
        hsend[k, 0:32] = heads[32 * k : 32 * k + 32]
        hsend[k, 32:64] = heads[128 + 32 * k : 160 + 32 * k]
    phase("headsend")
    head_in = [send(hsend.at[m4(x + d)], hall.at[x], dev_x(d), hall.at[m4(x - d)]) for d in (1, 3, 2)]
    hall[x] = hsend[x]
    phase("w2finish")
    out_low.finish()
    out_high.finish()
    for arrived in w2_in:
        arrived.wait_recv()
    phase("headwait")
    for arrived in head_in:
        arrived.wait_recv()
    phase("outmm")
    gathered = jnp.concatenate([hall[k] for k in range(4)], axis=1)
    for k in range(4):
        rows = jnp.concatenate([w2[kx, k].reshape(256, 128) for kx in range(4)], axis=1)
        part = mm(gathered, rows, NT)
        pbuf[0, :, 256 * k : 256 * k + 256] = part[0:32]
        pbuf[1, :, 256 * k : 256 * k + 256] = part[32:64]
    phase("last")
    last = send(pbuf.at[o], prec, partner, prec)
    last.wait_recv()
    out[...] = pbuf[c] + prec[...]
    phase("drain")
    for copy in sent:
        copy.wait_send()
    phase(None)


def per_device(
    tokens, norm_gain, attn_query, attn_key, attn_value, sink_logit, delta_query, delta_key, delta_value,
    delta_gate, beta_weight, decay_weight, beta_shift, decay_log, out_gain, attn_out, delta_out,
):
    operands = (
        tokens, norm_gain.reshape(1, -1), attn_query, attn_key, attn_value, delta_query, delta_key, delta_value,
        delta_gate, beta_weight.transpose(1, 2, 0), decay_weight.transpose(1, 2, 0), out_gain.reshape(1, -1),
        attn_out.T, delta_out.T, sink_logit, beta_shift, decay_log,
    )
    hbm = pl.BlockSpec(memory_space=pltpu.HBM)
    vmem = pl.BlockSpec(memory_space=pltpu.VMEM)
    summed = pl.pallas_call(
        layer_kernel,
        out_shape=jax.ShapeDtypeStruct((32, 1024), F32),
        in_specs=[hbm] * 17,
        out_specs=vmem,
        scratch_shapes=[
            pltpu.VMEM((1, 1024), F32),
            pltpu.VMEM((32, 128), BF16),
            pltpu.VMEM((32, 64), BF16),
            pltpu.VMEM((32, 64), BF16),
            pltpu.VMEM((32, 128), BF16),
            pltpu.VMEM((32, 128), BF16),
            pltpu.VMEM((32, 128), BF16),
            pltpu.VMEM((32, 128), BF16),
            pltpu.VMEM((2, 2, 32), BF16),
            pltpu.VMEM((2, 2, 32), BF16),
            pltpu.VMEM((1, 64), F32),
            pltpu.VMEM((32, 128), BF16),
            pltpu.VMEM((32, 128), BF16),
            pltpu.SMEM((2,), F32),
            pltpu.SMEM((2, 2), F32),
            pltpu.SMEM((2, 2), F32),
            pltpu.VMEM((4, 256, 256), BF16),
            pltpu.VMEM((4, 256, 256), BF16),
            pltpu.VMEM((2, 32, 640), BF16),
            pltpu.VMEM((4, 4, 2, 32, 512), BF16),
            pltpu.VMEM((4, 4, 4, 2, 32, 128), BF16),
            pltpu.VMEM((384, 128), BF16),
            pltpu.VMEM((2, 64, 128), LINK),
            pltpu.VMEM((4, 4, 64, 128), LINK),
            pltpu.VMEM((4, 64, 128), BF16),
            pltpu.VMEM((4, 64, 128), BF16),
            pltpu.VMEM((2, 32, 1024), F32),
            pltpu.VMEM((32, 1024), F32),
            pltpu.SemaphoreType.DMA((COPIES,)),
            pltpu.SemaphoreType.DMA((COPIES,)),
            pltpu.SemaphoreType.DMA((18,)),
        ],
        compiler_params=pltpu.CompilerParams(collective_id=0, has_side_effects=True, vmem_limit_bytes=24 * 2**20),
    )(*(pltpu.with_memory_space_constraint(operand, pltpu.HBM) for operand in operands))
    return summed.astype(BF16)


def solution(mesh):
    return jax.shard_map(
        per_device,
        mesh=mesh,
        in_specs=(
            P("sp", "tp"), P(), P("sp", "tp"), P("sp", "tp"), P("sp", "tp"), P("tp"), P("sp", "tp"),
            P("sp", "tp"), P("sp", "tp"), P("sp", "tp"), P("sp", "tp", None), P("sp", "tp", None),
            P(None, "tp"), P(None, "tp"), P(), P("tp", "sp"), P("tp", "sp"),
        ),
        out_specs=P(("sp", "tp"), None),
        check_vma=False,
    )
```

```python
import jax
import jax.numpy as jnp
from jax import lax
from jax.experimental import pallas as pl
from jax.experimental.pallas import tpu as pltpu
from jax.sharding import PartitionSpec as P

HEAD_DIM = 64
WINDOW = 64
ROWS = 256
TOKENS = 4096
EPS = 1e-6
COPIES = 168
MESH = pl.DeviceIdType.MESH
F32 = jnp.float32
BF16 = jnp.bfloat16
LINK = BF16
NN = (((1,), (0,)), ((), ()))
NT = (((1,), (1,)), ((), ()))


def mm(a, b, dims=NN):
    return lax.dot_general(a, b, dims, preferred_element_type=F32)


def split(a):
    hi = a.astype(BF16)
    return hi, (a - hi.astype(F32)).astype(BF16)


def left(a):
    hi, lo = split(a)
    return jnp.concatenate([hi, lo], axis=1)


def right(b):
    hi, lo = split(b)
    return jnp.concatenate(
        [jnp.concatenate([hi, lo], axis=1), jnp.concatenate([hi, jnp.zeros_like(lo)], axis=1)], axis=0
    )


def dot3(a, b):
    both = mm(left(a), right(b))
    return both[:, 0:128] + both[:, 128:256]


def right64(b):
    hi, lo = split(b)
    none = jnp.zeros_like(lo)
    blank = jnp.concatenate([none, none], axis=1)
    return jnp.concatenate(
        [jnp.concatenate([hi, lo], axis=1), blank, jnp.concatenate([hi, none], axis=1), blank], axis=0
    )


def dot64(a, b):
    both = mm(left(a), right64(b))
    return both[:, 0:128] + both[:, 128:256]


def silu(v):
    return v * jax.nn.sigmoid(v)


def layer_kernel(
    tokens_in, gain_in, aq_in, ak_in, av_in, dq_in, dk_in, dv_in, dz_in, bw_in, gw_in, ogain_in, ao_in, do_in,
    sink_in, shift_in, dlog_in,
    out,
    gain, aq, ak, av, dq, dk, dv, dz, bw, gw, ogain, ao, do, sink, shift, dlog,
    tok, normed, stage, w1, wq, wkv, w2, kv, own_map, maps_in, hsend, hall, pbuf, prec, send_sem, recv_sem, own_sem,
):
    sp = lax.axis_index("sp")
    x = lax.axis_index("tp")
    c = lax.rem(sp, 2)
    b = lax.div(sp, 2)
    z = lax.div(b, 4)
    y = lax.rem(b, 4)
    o = 1 - c

    open_scopes = []

    def phase(name):
        while open_scopes:
            open_scopes.pop().__exit__(None, None, None)
        if name:
            open_scopes.append(jax.named_scope(name))
            open_scopes[0].__enter__()

    def m4(v):
        return lax.rem(v + 4, 4)

    def dev(zz, yy, cc, xx):
        return {"sp": (zz * 4 + yy) * 2 + cc, "tp": xx}

    def dev_x(d):
        return dev(z, y, c, m4(x + d))

    def dev_y(d, core=c):
        return dev(z, m4(y + d), core, x)

    def dev_z(d, core=c):
        return dev(m4(z + d), y, core, x)

    def dev_b(d):
        bb = lax.rem(b + d + 16, 16)
        return {"sp": bb * 2 + c, "tp": x}

    partner = dev(z, y, o, x)
    sent = []

    def send(src, dst, device, landed):
        i = len(sent)
        copy = pltpu.make_async_remote_copy(
            src_ref=src, dst_ref=dst, send_sem=send_sem.at[i], recv_sem=recv_sem.at[i],
            device_id=device, device_id_type=MESH,
        )
        copy.start()
        sent.append(copy)
        return pltpu.make_async_remote_copy(
            src_ref=landed, dst_ref=landed, send_sem=send_sem.at[i], recv_sem=recv_sem.at[i],
            device_id=device, device_id_type=MESH,
        )

    phase("load")
    half_rows = pl.ds(128 * c, 128)
    other_rows = pl.ds(128 * o, 128)
    tokens = tok.at[x, half_rows]
    loads = [
        pltpu.make_async_copy(src, dst, own_sem.at[i])
        for i, (src, dst) in enumerate(
            [(aq_in, aq), (ak_in, ak), (av_in, av), (dq_in, dq), (dk_in, dk), (dv_in, dv), (dz_in, dz), (bw_in, bw),
             (gw_in, gw), (ao_in, ao), (do_in, do), (tokens_in, tokens), (gain_in, gain), (ogain_in, ogain),
             (sink_in, sink), (shift_in, shift), (dlog_in, dlog)]
        )
    ]
    for load in loads:
        load.start()
    barrier = pltpu.get_barrier_semaphore()
    peers = [partner]
    for d in (1, 2, 3):
        peers += [dev_x(d), dev_y(d), dev_z(d), dev_y(d, o), dev_z(d, o)]
    for peer in peers:
        pl.semaphore_signal(barrier, inc=1, device_id=peer, device_id_type=MESH)
    for load in loads[:11]:
        load.wait()
    phase("pack")
    attn_t, delta_t = ao[...], do[...]
    blank = jnp.zeros((60, 32), F32)
    for cc in range(2):
        cols = slice(64 * cc, 64 * cc + 64)
        small = jnp.concatenate([bw[cc].astype(F32), gw[cc].astype(F32), blank], axis=0).T.astype(BF16)
        stage[cc] = jnp.concatenate(
            [dk[:, cols], dv[:, cols], dz[:, cols], small, dq[:, cols], aq[:, cols], av[...], ak[...],
             attn_t[:, cols], delta_t[:, cols]],
            axis=1,
        )
    w1[z, y, c] = stage[c, :, 0:256]
    wq[z, y, c] = stage[c, :, 256:384]
    wkv[z, y, c] = stage[c, :, 384:512]
    w2[x, z, y, c] = stage[c, :, 512:640]

    phase("barrier")
    pl.semaphore_wait(barrier, len(peers))

    class Gather:
        def __init__(self, place, y_first, source=None, twin=None):
            self.place, self.y_first, self.source, self.twin = place, y_first, source, twin
            self.waits = {}

        def slot(self, first, second):
            zz, yy = (z + second, y + first) if self.y_first else (z + first, y + second)
            return self.place(m4(zz), m4(yy))

        def own(self, axis, d):
            device = dev_y if axis == self.y_first else dev_z
            if self.source is None:
                return self.slot(0, 0), self.slot(0, 0), device(d)
            return self.source, self.twin, device(d, o)

        def begin(self):
            for d in (1, 3, 2):
                self.waits[d] = send(*self.own(True, d), self.slot(-d, 0))

        def across(self):
            for d in (1, 3, 2):
                self.waits[0, d] = send(*self.own(False, d), self.slot(0, -d))

        def forward(self, d):
            self.waits[d].wait_recv()
            block = self.slot(-d, 0)
            for e in (1, 3, 2):
                device = dev_z(e) if self.y_first else dev_y(e)
                self.waits[-d, e] = send(block, block, device, self.slot(-d, -e))

        def finish(self):
            for e in (1, 3, 2):
                for f in (0, -1, -3, -2):
                    self.waits[f, e].wait_recv()

    in_cols = pl.ds(0, 256)
    query_cols = pl.ds(256, 128)
    out_cols = pl.ds(512, 128)
    phase("start")
    first = Gather(lambda zz, yy: w1.at[zz, yy, c], True)
    second = Gather(lambda zz, yy: w1.at[zz, yy, o], False, stage.at[o, :, in_cols], w1.at[z, y, c])
    out_low = Gather(lambda zz, yy: w2.at[:, zz, yy, c, pl.ds(0, 16)], True)
    out_high = Gather(lambda zz, yy: w2.at[:, zz, yy, c, pl.ds(16, 16)], False)
    out_twin = Gather(
        lambda zz, yy: w2.at[x, zz, yy, o], False, stage.at[o, :, out_cols], w2.at[x, z, y, c]
    )
    query = Gather(lambda zz, yy: wq.at[zz, yy, c], True)
    query_twin = Gather(lambda zz, yy: wq.at[zz, yy, o], False, stage.at[o, :, query_cols], wq.at[z, y, c])
    keys = Gather(lambda zz, yy: wkv.at[zz, yy, c], True)
    later = (query, query_twin, keys, out_twin)
    first.begin()
    second.begin()
    first.across()
    second.across()
    for ring in later:
        ring.begin()
        ring.across()
    for load in loads[11:]:
        load.wait()
    w2_own = [
        send(stage.at[c, :, out_cols], w2.at[x, z, y, c], dev_x(d), w2.at[m4(x - d), z, y, c]) for d in (1, 3, 2)
    ]
    tok_in = [send(tokens, tokens, dev_x(d), tok.at[m4(x - d), half_rows]) for d in (2, 1, 3)]
    w_swap = send(stage.at[o, :, in_cols], w1.at[z, y, c], partner, w1.at[z, y, o])
    tok_swap = [send(tokens, tokens, partner, tok.at[x, other_rows])]
    wq_swap = send(stage.at[o, :, query_cols], wq.at[z, y, c], partner, wq.at[z, y, o])
    w2_swap = send(stage.at[o, :, out_cols], w2.at[x, z, y, c], partner, w2.at[x, z, y, o])
    phase("near")
    for d in (1, 3, 2):
        first.forward(d)
        second.forward(d)
    phase("tokens")
    for d, arrived in zip((1, 3, 2), tok_in[1:] + tok_in[:1]):
        arrived.wait_recv()
        src = m4(x - d)
        tok_swap.append(send(tok.at[src, half_rows], tok.at[src, half_rows], partner, tok.at[src, other_rows]))
    phase("near2")
    for ring in later:
        for d in (1, 3, 2):
            ring.forward(d)
    phase("tokswap")
    for arrived in tok_swap:
        arrived.wait_recv()

    phase("norm")
    squares = jnp.zeros((ROWS, 1), F32)
    for k in range(4):
        wide = tok[k].astype(F32)
        squares = squares + jnp.sum(wide * wide, axis=-1, keepdims=True)
    inv = lax.rsqrt(squares * (1.0 / 1024.0) + EPS)
    for k in range(4):
        normed[k] = (tok[k].astype(F32) * inv * gain[:, 256 * k : 256 * k + 256]).astype(BF16)

    phase("outbegin")
    for arrived in w2_own:
        arrived.wait_recv()
    for ring in (out_low, out_high):
        ring.begin()
        ring.across()
    phase("wfinish")
    w_swap.wait_recv()
    first.finish()
    second.finish()

    phase("proj")
    def project(w):
        total = mm(normed[0], w(0))
        for k in range(1, 4):
            total = total + mm(normed[k], w(k))
        return total

    proj = project(lambda k: w1[k].reshape(256, 256))
    phase("gates0")
    t1, t2 = proj[:, 0:128], proj[:, 128:256]
    lane = lax.broadcasted_iota(jnp.int32, (1, 128), 1)
    head = lane < 64
    act = silu(t1.astype(BF16).astype(F32))
    act_k = jnp.where(head, act, 0.0)
    key_val = jnp.where(head, act * lax.rsqrt(jnp.sum(act_k * act_k, axis=-1, keepdims=True) + EPS), act)

    phase("gates")
    bias = jnp.where(lane == 64, shift[0, c], jnp.where(lane == 65, shift[1, c], 0.0))
    rate = jnp.exp(jnp.where(lane == 66, dlog[0, c], jnp.where(lane == 67, dlog[1, c], 0.0)))
    strength = jax.nn.sigmoid(t2 + bias)
    softplus = jnp.maximum(t2, 0.0) + jnp.log1p(jnp.exp(-jnp.abs(t2)))
    decay = jnp.where((lane == 66) | (lane == 67), -rate * softplus * (1.0 / TOKENS), 0.0)

    row = lax.broadcasted_iota(jnp.int32, (128, 128), 0)
    col = lax.broadcasted_iota(jnp.int32, (128, 128), 1)
    masks = (row >= col, row <= col)
    unit = jnp.where(row == col, 1.0, 0.0)
    near16 = lax.shift_right_logical(row, 4) == lax.shift_right_logical(col, 4)

    g_hi = decay.astype(BF16)
    rest = decay - g_hi.astype(F32)
    g_mid = rest.astype(BF16)
    g_lo = (rest - g_mid.astype(F32)).astype(BF16)
    g_parts = jnp.concatenate(
        [jnp.concatenate([part[0:128], part[128:256]], axis=1) for part in (g_hi, g_mid, g_lo)], axis=0
    )
    ones = jnp.concatenate([jnp.where(mask, 1.0, 0.0).astype(BF16) for mask in masks], axis=0)
    sums = mm(jnp.concatenate([ones, ones, ones], axis=1), g_parts)
    g_all = jnp.where(
        lane == 66,
        jnp.concatenate([sums[0:128, 0:128], sums[0:128, 128:256]], axis=0),
        jnp.concatenate([sums[128:256, 0:128], sums[128:256, 128:256]], axis=0),
    )
    turned = jnp.where(head, key_val, g_all).T
    key_t = turned[0:64]
    key_left = left(key_val)

    phase("delta1")
    lane2 = lax.broadcasted_iota(jnp.int32, (64, 128), 1)
    row2 = lax.broadcasted_iota(jnp.int32, (64, 128), 0)
    eye2 = jnp.where(lane2 == row2, 1.0, 0.0)
    chains = [(way, h) for way in range(2) for h in range(2)]
    low, decays, sides, grown, key_end, end = {}, {}, {}, {}, {}, {}
    for h in range(2):
        hs = slice(128 * h, 128 * h + 128)
        pairs = mm(key_left[hs], right64(key_t[:, hs]))
        pairs = pairs[:, 0:128] + pairs[:, 128:256]
        for way in range(2):
            at = way, h
            beta = strength[hs, 64 + way : 65 + way]
            g_col = g_all[hs, 66 + way : 67 + way]
            g_row = turned[66 + way : 67 + way, hs]
            g_end = g_col[127:128] if way == 0 else g_col[0:1]
            decays[at] = jnp.exp(jnp.where(masks[way], g_col - g_row, -jnp.inf))
            low[at] = jnp.where(row == col, 0.0, beta * pairs * decays[at])
            up = jnp.exp(g_col)
            grown[at] = up
            sides[at] = key_val[hs] * jnp.where(head, beta * up, beta)
            key_end[at] = key_t[:, hs] * jnp.exp(g_end - g_row)
            end[at] = jnp.exp(g_end)
    d1 = {at: jnp.where(near16, low[at], 0.0) for at in chains}
    off = {at: jnp.where(near16, 0.0, low[at]) for at in chains}
    d2 = {at: dot3(d1[at], d1[at]) for at in chains}
    inner = {at: unit - d1[at] for at in chains}
    d4 = {at: dot3(d2[at], d2[at]) for at in chains}
    inner = {at: inner[at] + dot3(inner[at], d2[at]) for at in chains}
    d8 = {at: dot3(d4[at], d4[at]) for at in chains}
    inner = {at: inner[at] + dot3(inner[at], d4[at]) for at in chains}
    inner = {at: inner[at] + dot3(inner[at], d8[at]) for at in chains}
    phase("rings")
    keys.finish()
    kv_swap = send(wkv.at[:, :, c], wkv.at[:, :, c], partner, wkv.at[:, :, o])
    w2_swap.wait_recv()
    out_twin.finish()
    w2_in = [send(w2.at[x, :, :, o], w2.at[x, :, :, o], dev_x(d), w2.at[m4(x - d), :, :, o]) for d in (1, 3, 2)]

    phase("delta2")
    m1 = {at: dot3(inner[at], off[at]) for at in chains}
    wu = {at: dot3(inner[at], sides[at]) for at in chains}
    m2 = {at: dot3(m1[at], m1[at]) for at in chains}
    wu = {at: wu[at] - dot3(m1[at], wu[at]) for at in chains}
    m4_ = {at: dot3(m2[at], m2[at]) for at in chains}
    wu = {at: wu[at] + dot3(m2[at], wu[at]) for at in chains}
    wu = {at: wu[at] + dot3(m4_[at], wu[at]) for at in chains}
    phase("outfwd")
    for d in (1, 3, 2):
        out_low.forward(d)
        out_high.forward(d)
    phase("final")

    def after(later, earlier):
        return dot64(later, earlier) + later + earlier

    maps = {}
    for at in chains:
        final = dot3(key_end[at], wu[at])
        maps[at] = jnp.where(lane2 < 64, (end[at] - 1.0) * eye2 - final, final)
    for way in range(2):
        own_map[way] = after(maps[way, 1 - way], maps[way, way]).astype(LINK)
    phase("kvproj")
    kv_swap.wait_recv()
    kv[64:320, :] = project(lambda k: wkv[k].reshape(256, 128)).astype(BF16)
    halo = [
        send(kv.at[pl.ds(256, 64)], kv.at[pl.ds(0, 64)], dev_b(1), kv.at[pl.ds(0, 64)]),
        send(kv.at[pl.ds(64, 64)], kv.at[pl.ds(320, 64)], dev_b(-1), kv.at[pl.ds(320, 64)]),
    ]
    phase("scan1send")
    scan = []
    steps = [(dz, dy) for dz in range(4) for dy in range(4) if (dz, dy) != (0, 0)]
    for dz, dy in sorted(steps, key=lambda step: -(min(step[0], 4 - step[0]) + min(step[1], 4 - step[1]))):
        zz, yy = m4(z + dz), m4(y + dy)
        goes = jnp.where(zz * 4 + yy > b, 0, 1)
        scan.append(
            send(own_map.at[goes], maps_in.at[z, y], dev(zz, yy, c, x), maps_in.at[m4(z - dz), m4(y - dy)])
        )
    phase("qproj")
    wq_swap.wait_recv()
    query.finish()
    query_twin.finish()
    t0 = project(lambda k: wq[k].reshape(256, 128))
    act = jnp.where(head, silu(t0.astype(BF16).astype(F32)), 0.0)
    q = act * (lax.rsqrt(jnp.sum(act * act, axis=-1, keepdims=True) + EPS) * HEAD_DIM**-0.5)
    q_left = left(q)

    phase("reads")
    reads = {}
    pairs = []
    for h in range(2):
        hs = slice(128 * h, 128 * h + 128)
        pair = mm(q_left[hs], right64(key_t[:, hs]))
        pairs.append(pair[:, 0:128] + pair[:, 128:256])
    for way, h in chains:
        at = way, h
        read = dot3(pairs[h] * decays[at], wu[at])
        reads[at] = jnp.where(head, grown[at] * q[128 * h : 128 * h + 128] - read, read)
        if h != way:
            reads[at] = reads[at] + dot64(reads[at], maps[way, way])
    reads = [jnp.concatenate([reads[way, 0], reads[way, 1]], axis=0) for way in range(2)]
    reads_left = [left(r) for r in reads]
    local = reads[0] + reads[1]
    gate = silu(t2.astype(BF16).astype(F32))
    gate = jnp.concatenate([gate[:, 64:128], gate[:, 0:64]], axis=1)
    gain_row = jnp.concatenate([ogain[...], ogain[...]], axis=1)

    phase("halo")
    for arrived in halo:
        arrived.wait_recv()
    phase("attn")
    att_q = jnp.where(head, 0.0, t0).astype(BF16)
    scores = mm(att_q, kv[...], NT) * HEAD_DIM**-0.5
    q_pos = lax.broadcasted_iota(jnp.int32, (ROWS, ROWS + 2 * WINDOW), 0)
    k_pos = lax.broadcasted_iota(jnp.int32, (ROWS, ROWS + 2 * WINDOW), 1) - WINDOW
    seen = k_pos + b * ROWS
    allowed = (jnp.abs(q_pos - k_pos) <= WINDOW) & (seen >= 0) & (seen < TOKENS)
    scores = jnp.where(allowed, scores, -jnp.inf)
    top = jnp.maximum(jnp.max(scores, axis=-1, keepdims=True), sink[c])
    weights = jnp.exp(scores - top)
    total = jnp.sum(weights, axis=-1, keepdims=True) + jnp.exp(sink[c] - top)
    weights = (weights / total).astype(BF16)
    attn_heads = mm(weights, kv[...])

    phase("scanwait")
    for arrived in scan:
        arrived.wait_recv()
    phase("states")
    states = []
    for way in range(2):
        order = range(16) if way == 0 else range(15, -1, -1)
        chain = []
        for k in order:
            inside = (b > k) if way == 0 else (b < k)
            chain.append(jnp.where(inside, maps_in[k // 4, k % 4], jnp.zeros((64, 128), LINK)))
        level = []
        for k in range(0, 14, 2):
            earlier, later = chain[k], chain[k + 1]
            level.append(
                mm(later, jnp.concatenate([earlier, jnp.zeros_like(earlier)], axis=0))
                + later.astype(F32)
                + earlier.astype(F32)
            )
        level.append(chain[14].astype(F32))
        while len(level) > 1:
            level = [after(level[k + 1], level[k]) for k in range(0, len(level), 2)]
        states.append(jnp.where(lane2 < 64, 0.0, level[0]))

    phase("whole")
    both = mm(reads_left[0], right64(states[0])) + mm(reads_left[1], right64(states[1]))
    whole = jnp.where(head, 0.0, local + both[:, 0:128] + both[:, 128:256])
    scaled = whole * lax.rsqrt(jnp.sum(whole * whole, axis=-1, keepdims=True) * (1.0 / HEAD_DIM) + EPS) * gain_row
    heads = jnp.where(head, attn_heads, scaled * gate).astype(BF16)
    phase("headsend0")
    for k in range(4):
        hsend[k, 0:32] = heads[32 * k : 32 * k + 32]
        hsend[k, 32:64] = heads[128 + 32 * k : 160 + 32 * k]
    phase("headsend")
    head_in = [send(hsend.at[m4(x + d)], hall.at[x], dev_x(d), hall.at[m4(x - d)]) for d in (2, 1, 3)]
    hall[x] = hsend[x]
    phase("w2finish")
    out_low.finish()
    out_high.finish()
    for arrived in w2_in:
        arrived.wait_recv()
    phase("headwait")
    for arrived in head_in:
        arrived.wait_recv()
    phase("outmm")
    gathered = jnp.concatenate([hall[k] for k in range(4)], axis=1)
    last = []
    for k in range(4):
        rows = jnp.concatenate([w2[kx, k].reshape(256, 128) for kx in range(4)], axis=1)
        part = mm(gathered, rows, NT)
        pbuf[k, 0] = part[0:32]
        pbuf[k, 1] = part[32:64]
        if k % 2:
            pair = pl.ds(k - 1, 2)
            last.append(send(pbuf.at[pair, o], prec.at[pair], partner, prec.at[pair]))
    phase("last")
    for k in range(4):
        if k % 2 == 0:
            last[k // 2].wait_recv()
        out[:, 256 * k : 256 * k + 256] = pbuf[k, c] + prec[k]
    phase("drain")
    for copy in sent:
        copy.wait_send()
    phase(None)


def per_device(
    tokens, norm_gain, attn_query, attn_key, attn_value, sink_logit, delta_query, delta_key, delta_value,
    delta_gate, beta_weight, decay_weight, beta_shift, decay_log, out_gain, attn_out, delta_out,
):
    operands = (
        tokens, norm_gain.reshape(1, -1), attn_query, attn_key, attn_value, delta_query, delta_key, delta_value,
        delta_gate, beta_weight.transpose(1, 2, 0), decay_weight.transpose(1, 2, 0), out_gain.reshape(1, -1),
        attn_out.T, delta_out.T, sink_logit, beta_shift, decay_log,
    )
    hbm = pl.BlockSpec(memory_space=pltpu.HBM)
    vmem = pl.BlockSpec(memory_space=pltpu.VMEM)
    summed = pl.pallas_call(
        layer_kernel,
        out_shape=jax.ShapeDtypeStruct((32, 1024), F32),
        in_specs=[hbm] * 17,
        out_specs=vmem,
        scratch_shapes=[
            pltpu.VMEM((1, 1024), F32),
            pltpu.VMEM((32, 128), BF16),
            pltpu.VMEM((32, 64), BF16),
            pltpu.VMEM((32, 64), BF16),
            pltpu.VMEM((32, 128), BF16),
            pltpu.VMEM((32, 128), BF16),
            pltpu.VMEM((32, 128), BF16),
            pltpu.VMEM((32, 128), BF16),
            pltpu.VMEM((2, 2, 32), BF16),
            pltpu.VMEM((2, 2, 32), BF16),
            pltpu.VMEM((1, 64), F32),
            pltpu.VMEM((32, 128), BF16),
            pltpu.VMEM((32, 128), BF16),
            pltpu.SMEM((2,), F32),
            pltpu.SMEM((2, 2), F32),
            pltpu.SMEM((2, 2), F32),
            pltpu.VMEM((4, 256, 256), BF16),
            pltpu.VMEM((4, 256, 256), BF16),
            pltpu.VMEM((2, 32, 640), BF16),
            pltpu.VMEM((4, 4, 2, 32, 256), BF16),
            pltpu.VMEM((4, 4, 2, 32, 128), BF16),
            pltpu.VMEM((4, 4, 2, 32, 128), BF16),
            pltpu.VMEM((4, 4, 4, 2, 32, 128), BF16),
            pltpu.VMEM((384, 128), BF16),
            pltpu.VMEM((2, 64, 128), LINK),
            pltpu.VMEM((4, 4, 64, 128), LINK),
            pltpu.VMEM((4, 64, 128), BF16),
            pltpu.VMEM((4, 64, 128), BF16),
            pltpu.VMEM((4, 2, 32, 256), F32),
            pltpu.VMEM((4, 32, 256), F32),
            pltpu.SemaphoreType.DMA((COPIES,)),
            pltpu.SemaphoreType.DMA((COPIES,)),
            pltpu.SemaphoreType.DMA((18,)),
        ],
        compiler_params=pltpu.CompilerParams(collective_id=0, has_side_effects=True, vmem_limit_bytes=24 * 2**20),
    )(*(pltpu.with_memory_space_constraint(operand, pltpu.HBM) for operand in operands))
    return summed.astype(BF16)


def solution(mesh):
    return jax.shard_map(
        per_device,
        mesh=mesh,
        in_specs=(
            P("sp", "tp"), P(), P("sp", "tp"), P("sp", "tp"), P("sp", "tp"), P("tp"), P("sp", "tp"),
            P("sp", "tp"), P("sp", "tp"), P("sp", "tp"), P("sp", "tp", None), P("sp", "tp", None),
            P(None, "tp"), P(None, "tp"), P(), P("tp", "sp"), P("tp", "sp"),
        ),
        out_specs=P(("sp", "tp"), None),
        check_vma=False,
    )
```

```python
import jax
import jax.numpy as jnp
from jax import lax
from jax.experimental import pallas as pl
from jax.experimental.pallas import tpu as pltpu
from jax.sharding import PartitionSpec as P

HEAD_DIM = 64
WINDOW = 64
ROWS = 256
TOKENS = 4096
EPS = 1e-6
COPIES = 168
MESH = pl.DeviceIdType.MESH
F32 = jnp.float32
BF16 = jnp.bfloat16
LINK = BF16
NN = (((1,), (0,)), ((), ()))
NT = (((1,), (1,)), ((), ()))


def mm(a, b, dims=NN):
    return lax.dot_general(a, b, dims, preferred_element_type=F32)


def split(a):
    hi = a.astype(BF16)
    return hi, (a - hi.astype(F32)).astype(BF16)


def left(a):
    hi, lo = split(a)
    return jnp.concatenate([hi, lo], axis=1)


def right(b):
    hi, lo = split(b)
    return jnp.concatenate(
        [jnp.concatenate([hi, lo], axis=1), jnp.concatenate([hi, jnp.zeros_like(lo)], axis=1)], axis=0
    )


def dot3(a, b):
    both = mm(left(a), right(b))
    return both[:, 0:128] + both[:, 128:256]


def right64(b):
    hi, lo = split(b)
    none = jnp.zeros_like(lo)
    blank = jnp.concatenate([none, none], axis=1)
    return jnp.concatenate(
        [jnp.concatenate([hi, lo], axis=1), blank, jnp.concatenate([hi, none], axis=1), blank], axis=0
    )


def dot64(a, b):
    both = mm(left(a), right64(b))
    return both[:, 0:128] + both[:, 128:256]


def silu(v):
    return v * jax.nn.sigmoid(v)


def layer_kernel(
    tokens_in, gain_in, aq_in, ak_in, av_in, dq_in, dk_in, dv_in, dz_in, bw_in, gw_in, ogain_in, ao_in, do_in,
    sink_in, shift_in, dlog_in,
    out,
    gain, aq, ak, av, dq, dk, dv, dz, bw, gw, ogain, ao, do, sink, shift, dlog,
    tok, normed, stage, w1, wq, wkv, w2, kv, own_map, maps_in, hsend, hall, pbuf, prec, send_sem, recv_sem, own_sem,
):
    sp = lax.axis_index("sp")
    x = lax.axis_index("tp")
    c = lax.rem(sp, 2)
    b = lax.div(sp, 2)
    z = lax.div(b, 4)
    y = lax.rem(b, 4)
    o = 1 - c

    open_scopes = []

    def phase(name):
        while open_scopes:
            open_scopes.pop().__exit__(None, None, None)
        if name:
            open_scopes.append(jax.named_scope(name))
            open_scopes[0].__enter__()

    def m4(v):
        return lax.rem(v + 4, 4)

    def dev(zz, yy, cc, xx):
        return {"sp": (zz * 4 + yy) * 2 + cc, "tp": xx}

    def dev_x(d):
        return dev(z, y, c, m4(x + d))

    def dev_y(d, core=c):
        return dev(z, m4(y + d), core, x)

    def dev_z(d, core=c):
        return dev(m4(z + d), y, core, x)

    def dev_b(d):
        bb = lax.rem(b + d + 16, 16)
        return {"sp": bb * 2 + c, "tp": x}

    partner = dev(z, y, o, x)
    sent = []

    def send(src, dst, device, landed):
        i = len(sent)
        copy = pltpu.make_async_remote_copy(
            src_ref=src, dst_ref=dst, send_sem=send_sem.at[i], recv_sem=recv_sem.at[i],
            device_id=device, device_id_type=MESH,
        )
        copy.start()
        sent.append(copy)
        return pltpu.make_async_remote_copy(
            src_ref=landed, dst_ref=landed, send_sem=send_sem.at[i], recv_sem=recv_sem.at[i],
            device_id=device, device_id_type=MESH,
        )

    phase("load")
    half_rows = pl.ds(128 * c, 128)
    other_rows = pl.ds(128 * o, 128)
    tokens = tok.at[x, half_rows]
    loads = [
        pltpu.make_async_copy(src, dst, own_sem.at[i])
        for i, (src, dst) in enumerate(
            [(aq_in, aq), (ak_in, ak), (av_in, av), (dq_in, dq), (dk_in, dk), (dv_in, dv), (dz_in, dz), (bw_in, bw),
             (gw_in, gw), (ao_in, ao), (do_in, do), (tokens_in, tokens), (gain_in, gain), (ogain_in, ogain),
             (sink_in, sink), (shift_in, shift), (dlog_in, dlog)]
        )
    ]
    for load in loads:
        load.start()
    barrier = pltpu.get_barrier_semaphore()
    peers = [partner]
    for d in (1, 2, 3):
        peers += [dev_x(d), dev_y(d), dev_z(d), dev_y(d, o), dev_z(d, o)]
    for peer in peers:
        pl.semaphore_signal(barrier, inc=1, device_id=peer, device_id_type=MESH)
    for load in loads[:11]:
        load.wait()
    phase("pack")
    attn_t, delta_t = ao[...], do[...]
    blank = jnp.zeros((60, 32), F32)
    for cc in range(2):
        cols = slice(64 * cc, 64 * cc + 64)
        small = jnp.concatenate([bw[cc].astype(F32), gw[cc].astype(F32), blank], axis=0).T.astype(BF16)
        stage[cc] = jnp.concatenate(
            [dk[:, cols], dv[:, cols], dz[:, cols], small, dq[:, cols], aq[:, cols], av[...], ak[...],
             attn_t[:, cols], delta_t[:, cols]],
            axis=1,
        )
    w1[z, y, c] = stage[c, :, 0:256]
    wq[z, y, c] = stage[c, :, 256:384]
    wkv[z, y, c] = stage[c, :, 384:512]
    w2[x, z, y, c] = stage[c, :, 512:640]

    phase("barrier")
    pl.semaphore_wait(barrier, len(peers))

    class Gather:
        def __init__(self, place, y_first, source=None, twin=None):
            self.place, self.y_first, self.source, self.twin = place, y_first, source, twin
            self.waits = {}

        def slot(self, first, second):
            zz, yy = (z + second, y + first) if self.y_first else (z + first, y + second)
            return self.place(m4(zz), m4(yy))

        def own(self, axis, d):
            device = dev_y if axis == self.y_first else dev_z
            if self.source is None:
                return self.slot(0, 0), self.slot(0, 0), device(d)
            return self.source, self.twin, device(d, o)

        def begin(self):
            for d in (1, 3, 2):
                self.waits[d] = send(*self.own(True, d), self.slot(-d, 0))

        def across(self):
            for d in (1, 3, 2):
                self.waits[0, d] = send(*self.own(False, d), self.slot(0, -d))

        def forward(self, d):
            self.waits[d].wait_recv()
            block = self.slot(-d, 0)
            for e in (1, 3, 2):
                device = dev_z(e) if self.y_first else dev_y(e)
                self.waits[-d, e] = send(block, block, device, self.slot(-d, -e))

        def finish(self):
            for e in (1, 3, 2):
                for f in (0, -1, -3, -2):
                    self.waits[f, e].wait_recv()

    in_cols = pl.ds(0, 256)
    query_cols = pl.ds(256, 128)
    out_cols = pl.ds(512, 128)
    phase("start")
    first = Gather(lambda zz, yy: w1.at[zz, yy, c], True)
    second = Gather(lambda zz, yy: w1.at[zz, yy, o], False, stage.at[o, :, in_cols], w1.at[z, y, c])
    out_low = Gather(lambda zz, yy: w2.at[:, zz, yy, c, pl.ds(0, 16)], True)
    out_high = Gather(lambda zz, yy: w2.at[:, zz, yy, c, pl.ds(16, 16)], False)
    out_twin = Gather(
        lambda zz, yy: w2.at[x, zz, yy, o], False, stage.at[o, :, out_cols], w2.at[x, z, y, c]
    )
    query = Gather(lambda zz, yy: wq.at[zz, yy, c], True)
    query_twin = Gather(lambda zz, yy: wq.at[zz, yy, o], False, stage.at[o, :, query_cols], wq.at[z, y, c])
    keys = Gather(lambda zz, yy: wkv.at[zz, yy, c], True)
    later = (query, query_twin, keys, out_twin)
    first.begin()
    second.begin()
    first.across()
    second.across()
    for ring in later:
        ring.begin()
        ring.across()
    for load in loads[11:]:
        load.wait()
    w2_own = [
        send(stage.at[c, :, out_cols], w2.at[x, z, y, c], dev_x(d), w2.at[m4(x - d), z, y, c]) for d in (1, 3, 2)
    ]
    tok_in = [send(tokens, tokens, dev_x(d), tok.at[m4(x - d), half_rows]) for d in (2, 1, 3)]
    w_swap = send(stage.at[o, :, in_cols], w1.at[z, y, c], partner, w1.at[z, y, o])
    tok_swap = [send(tokens, tokens, partner, tok.at[x, other_rows])]
    wq_swap = send(stage.at[o, :, query_cols], wq.at[z, y, c], partner, wq.at[z, y, o])
    w2_swap = send(stage.at[o, :, out_cols], w2.at[x, z, y, c], partner, w2.at[x, z, y, o])
    phase("near")
    for d in (1, 3, 2):
        first.forward(d)
        second.forward(d)
    phase("tokens")
    for d, arrived in zip((1, 3, 2), tok_in[1:] + tok_in[:1]):
        arrived.wait_recv()
        src = m4(x - d)
        tok_swap.append(send(tok.at[src, half_rows], tok.at[src, half_rows], partner, tok.at[src, other_rows]))
    phase("near2")
    for ring in later:
        for d in (1, 3, 2):
            ring.forward(d)
    phase("tokswap")
    for arrived in tok_swap:
        arrived.wait_recv()

    phase("norm")
    squares = jnp.zeros((ROWS, 1), F32)
    for k in range(4):
        wide = tok[k].astype(F32)
        squares = squares + jnp.sum(wide * wide, axis=-1, keepdims=True)
    inv = lax.rsqrt(squares * (1.0 / 1024.0) + EPS)
    for k in range(4):
        normed[k] = (tok[k].astype(F32) * inv * gain[:, 256 * k : 256 * k + 256]).astype(BF16)

    phase("outbegin")
    for arrived in w2_own:
        arrived.wait_recv()
    for ring in (out_low, out_high):
        ring.begin()
        ring.across()
    phase("wfinish")
    w_swap.wait_recv()
    first.finish()
    second.finish()

    phase("proj")
    def project(w):
        total = mm(normed[0], w(0))
        for k in range(1, 4):
            total = total + mm(normed[k], w(k))
        return total

    proj = project(lambda k: w1[k].reshape(256, 256))
    phase("gates0")
    t1, t2 = proj[:, 0:128], proj[:, 128:256]
    lane = lax.broadcasted_iota(jnp.int32, (1, 128), 1)
    head = lane < 64
    act = silu(t1.astype(BF16).astype(F32))
    act_k = jnp.where(head, act, 0.0)
    key_val = jnp.where(head, act * lax.rsqrt(jnp.sum(act_k * act_k, axis=-1, keepdims=True) + EPS), act)

    phase("gates")
    bias = jnp.where(lane == 64, shift[0, c], jnp.where(lane == 65, shift[1, c], 0.0))
    rate = jnp.exp(jnp.where(lane == 66, dlog[0, c], jnp.where(lane == 67, dlog[1, c], 0.0)))
    strength = jax.nn.sigmoid(t2 + bias)
    softplus = jnp.maximum(t2, 0.0) + jnp.log1p(jnp.exp(-jnp.abs(t2)))
    decay = jnp.where((lane == 66) | (lane == 67), -rate * softplus * (1.0 / TOKENS), 0.0)

    row = lax.broadcasted_iota(jnp.int32, (128, 128), 0)
    col = lax.broadcasted_iota(jnp.int32, (128, 128), 1)
    masks = (row >= col, row <= col)
    unit = jnp.where(row == col, 1.0, 0.0)
    near16 = lax.shift_right_logical(row, 4) == lax.shift_right_logical(col, 4)

    g_hi = decay.astype(BF16)
    rest = decay - g_hi.astype(F32)
    g_mid = rest.astype(BF16)
    g_lo = (rest - g_mid.astype(F32)).astype(BF16)
    g_parts = jnp.concatenate(
        [jnp.concatenate([part[0:128], part[128:256]], axis=1) for part in (g_hi, g_mid, g_lo)], axis=0
    )
    ones = jnp.concatenate([jnp.where(mask, 1.0, 0.0).astype(BF16) for mask in masks], axis=0)
    sums = mm(jnp.concatenate([ones, ones, ones], axis=1), g_parts)
    g_all = jnp.where(
        lane == 66,
        jnp.concatenate([sums[0:128, 0:128], sums[0:128, 128:256]], axis=0),
        jnp.concatenate([sums[128:256, 0:128], sums[128:256, 128:256]], axis=0),
    )
    turned = jnp.where(head, key_val, g_all).T
    key_t = turned[0:64]
    key_left = left(key_val)

    phase("delta1")
    lane2 = lax.broadcasted_iota(jnp.int32, (64, 128), 1)
    row2 = lax.broadcasted_iota(jnp.int32, (64, 128), 0)
    eye2 = jnp.where(lane2 == row2, 1.0, 0.0)
    chains = [(way, h) for way in range(2) for h in range(2)]
    low, decays, sides, grown, key_end, end = {}, {}, {}, {}, {}, {}
    for h in range(2):
        hs = slice(128 * h, 128 * h + 128)
        pairs = mm(key_left[hs], right64(key_t[:, hs]))
        pairs = pairs[:, 0:128] + pairs[:, 128:256]
        for way in range(2):
            at = way, h
            beta = strength[hs, 64 + way : 65 + way]
            g_col = g_all[hs, 66 + way : 67 + way]
            g_row = turned[66 + way : 67 + way, hs]
            g_end = g_col[127:128] if way == 0 else g_col[0:1]
            decays[at] = jnp.exp(jnp.where(masks[way], g_col - g_row, -jnp.inf))
            low[at] = jnp.where(row == col, 0.0, beta * pairs * decays[at])
            up = jnp.exp(g_col)
            grown[at] = up
            sides[at] = key_val[hs] * jnp.where(head, beta * up, beta)
            key_end[at] = key_t[:, hs] * jnp.exp(g_end - g_row)
            end[at] = jnp.exp(g_end)
    d1 = {at: jnp.where(near16, low[at], 0.0) for at in chains}
    off = {at: jnp.where(near16, 0.0, low[at]) for at in chains}
    d2 = {at: dot3(d1[at], d1[at]) for at in chains}
    inner = {at: unit - d1[at] for at in chains}
    d4 = {at: dot3(d2[at], d2[at]) for at in chains}
    inner = {at: inner[at] + dot3(inner[at], d2[at]) for at in chains}
    d8 = {at: dot3(d4[at], d4[at]) for at in chains}
    inner = {at: inner[at] + dot3(inner[at], d4[at]) for at in chains}
    inner = {at: inner[at] + dot3(inner[at], d8[at]) for at in chains}
    phase("rings")
    keys.finish()
    kv_swap = send(wkv.at[:, :, c], wkv.at[:, :, c], partner, wkv.at[:, :, o])
    w2_swap.wait_recv()
    out_twin.finish()
    w2_in = [send(w2.at[x, :, :, o], w2.at[x, :, :, o], dev_x(d), w2.at[m4(x - d), :, :, o]) for d in (1, 3, 2)]

    phase("delta2")
    m1 = {at: dot3(inner[at], off[at]) for at in chains}
    wu = {at: dot3(inner[at], sides[at]) for at in chains}
    m2 = {at: dot3(m1[at], m1[at]) for at in chains}
    wu = {at: wu[at] - dot3(m1[at], wu[at]) for at in chains}
    m4_ = {at: dot3(m2[at], m2[at]) for at in chains}
    wu = {at: wu[at] + dot3(m2[at], wu[at]) for at in chains}
    wu = {at: wu[at] + dot3(m4_[at], wu[at]) for at in chains}
    phase("final")

    def after(later, earlier):
        return dot64(later, earlier) + later + earlier

    maps = {}
    for at in chains:
        final = dot3(key_end[at], wu[at])
        maps[at] = jnp.where(lane2 < 64, (end[at] - 1.0) * eye2 - final, final)
    for way in range(2):
        own_map[way] = after(maps[way, 1 - way], maps[way, way]).astype(LINK)
    phase("kvproj")
    kv_swap.wait_recv()
    kv[64:320, :] = project(lambda k: wkv[k].reshape(256, 128)).astype(BF16)
    halo = [
        send(kv.at[pl.ds(256, 64)], kv.at[pl.ds(0, 64)], dev_b(1), kv.at[pl.ds(0, 64)]),
        send(kv.at[pl.ds(64, 64)], kv.at[pl.ds(320, 64)], dev_b(-1), kv.at[pl.ds(320, 64)]),
    ]
    phase("scan1send")
    scan = []
    steps = [(dz, dy) for dz in range(4) for dy in range(4) if (dz, dy) != (0, 0)]
    for dz, dy in sorted(steps, key=lambda step: -(min(step[0], 4 - step[0]) + min(step[1], 4 - step[1]))):
        zz, yy = m4(z + dz), m4(y + dy)
        goes = jnp.where(zz * 4 + yy > b, 0, 1)
        scan.append(
            send(own_map.at[goes], maps_in.at[z, y], dev(zz, yy, c, x), maps_in.at[m4(z - dz), m4(y - dy)])
        )
    phase("qproj")
    wq_swap.wait_recv()
    query.finish()
    query_twin.finish()
    t0 = project(lambda k: wq[k].reshape(256, 128))
    act = jnp.where(head, silu(t0.astype(BF16).astype(F32)), 0.0)
    q = act * (lax.rsqrt(jnp.sum(act * act, axis=-1, keepdims=True) + EPS) * HEAD_DIM**-0.5)
    q_left = left(q)

    phase("reads")
    reads = {}
    pairs = []
    for h in range(2):
        hs = slice(128 * h, 128 * h + 128)
        pair = mm(q_left[hs], right64(key_t[:, hs]))
        pairs.append(pair[:, 0:128] + pair[:, 128:256])
    for way, h in chains:
        at = way, h
        read = dot3(pairs[h] * decays[at], wu[at])
        reads[at] = jnp.where(head, grown[at] * q[128 * h : 128 * h + 128] - read, read)
        if h != way:
            reads[at] = reads[at] + dot64(reads[at], maps[way, way])
    reads = [jnp.concatenate([reads[way, 0], reads[way, 1]], axis=0) for way in range(2)]
    reads_left = [left(r) for r in reads]
    local = reads[0] + reads[1]
    gate = silu(t2.astype(BF16).astype(F32))
    gate = jnp.concatenate([gate[:, 64:128], gate[:, 0:64]], axis=1)
    gain_row = jnp.concatenate([ogain[...], ogain[...]], axis=1)

    phase("halo")
    for arrived in halo:
        arrived.wait_recv()
    phase("attn")
    att_q = jnp.where(head, 0.0, t0).astype(BF16)
    scores = mm(att_q, kv[...], NT) * HEAD_DIM**-0.5
    q_pos = lax.broadcasted_iota(jnp.int32, (ROWS, ROWS + 2 * WINDOW), 0)
    k_pos = lax.broadcasted_iota(jnp.int32, (ROWS, ROWS + 2 * WINDOW), 1) - WINDOW
    seen = k_pos + b * ROWS
    allowed = (jnp.abs(q_pos - k_pos) <= WINDOW) & (seen >= 0) & (seen < TOKENS)
    scores = jnp.where(allowed, scores, -jnp.inf)
    top = jnp.maximum(jnp.max(scores, axis=-1, keepdims=True), sink[c])
    weights = jnp.exp(scores - top)
    total = jnp.sum(weights, axis=-1, keepdims=True) + jnp.exp(sink[c] - top)
    weights = (weights / total).astype(BF16)
    attn_heads = mm(weights, kv[...])

    phase("scanwait")
    for arrived in scan:
        arrived.wait_recv()
    phase("outfwd")
    for d in (1, 3, 2):
        out_low.forward(d)
        out_high.forward(d)
    phase("states")
    states = []
    for way in range(2):
        order = range(16) if way == 0 else range(15, -1, -1)
        chain = []
        for k in order:
            inside = (b > k) if way == 0 else (b < k)
            chain.append(jnp.where(inside, maps_in[k // 4, k % 4], jnp.zeros((64, 128), LINK)))
        level = []
        for k in range(0, 14, 2):
            earlier, later = chain[k], chain[k + 1]
            level.append(
                mm(later, jnp.concatenate([earlier, jnp.zeros_like(earlier)], axis=0))
                + later.astype(F32)
                + earlier.astype(F32)
            )
        level.append(chain[14].astype(F32))
        while len(level) > 1:
            level = [after(level[k + 1], level[k]) for k in range(0, len(level), 2)]
        states.append(jnp.where(lane2 < 64, 0.0, level[0]))

    phase("whole")
    both = mm(reads_left[0], right64(states[0])) + mm(reads_left[1], right64(states[1]))
    whole = jnp.where(head, 0.0, local + both[:, 0:128] + both[:, 128:256])
    scaled = whole * lax.rsqrt(jnp.sum(whole * whole, axis=-1, keepdims=True) * (1.0 / HEAD_DIM) + EPS) * gain_row
    heads = jnp.where(head, attn_heads, scaled * gate).astype(BF16)
    phase("headsend0")
    for k in range(4):
        hsend[k, 0:32] = heads[32 * k : 32 * k + 32]
        hsend[k, 32:64] = heads[128 + 32 * k : 160 + 32 * k]
    phase("headsend")
    head_in = [send(hsend.at[m4(x + d)], hall.at[x], dev_x(d), hall.at[m4(x - d)]) for d in (2, 1, 3)]
    hall[x] = hsend[x]
    phase("w2finish")
    out_low.finish()
    out_high.finish()
    for arrived in w2_in:
        arrived.wait_recv()
    phase("headwait")
    for arrived in head_in:
        arrived.wait_recv()
    phase("outmm")
    gathered = jnp.concatenate([hall[k] for k in range(4)], axis=1)
    last = []
    for k in range(4):
        rows = jnp.concatenate([w2[kx, k].reshape(256, 128) for kx in range(4)], axis=1)
        part = mm(gathered, rows, NT)
        pbuf[k, 0] = part[0:32]
        pbuf[k, 1] = part[32:64]
        if k % 2:
            pair = pl.ds(k - 1, 2)
            last.append(send(pbuf.at[pair, o], prec.at[pair], partner, prec.at[pair]))
    phase("last")
    for k in range(4):
        if k % 2 == 0:
            last[k // 2].wait_recv()
        out[:, 256 * k : 256 * k + 256] = pbuf[k, c] + prec[k]
    phase("drain")
    for copy in sent:
        copy.wait_send()
    phase(None)


def per_device(
    tokens, norm_gain, attn_query, attn_key, attn_value, sink_logit, delta_query, delta_key, delta_value,
    delta_gate, beta_weight, decay_weight, beta_shift, decay_log, out_gain, attn_out, delta_out,
):
    operands = (
        tokens, norm_gain.reshape(1, -1), attn_query, attn_key, attn_value, delta_query, delta_key, delta_value,
        delta_gate, beta_weight.transpose(1, 2, 0), decay_weight.transpose(1, 2, 0), out_gain.reshape(1, -1),
        attn_out.T, delta_out.T, sink_logit, beta_shift, decay_log,
    )
    hbm = pl.BlockSpec(memory_space=pltpu.HBM)
    vmem = pl.BlockSpec(memory_space=pltpu.VMEM)
    summed = pl.pallas_call(
        layer_kernel,
        out_shape=jax.ShapeDtypeStruct((32, 1024), F32),
        in_specs=[hbm] * 17,
        out_specs=vmem,
        scratch_shapes=[
            pltpu.VMEM((1, 1024), F32),
            pltpu.VMEM((32, 128), BF16),
            pltpu.VMEM((32, 64), BF16),
            pltpu.VMEM((32, 64), BF16),
            pltpu.VMEM((32, 128), BF16),
            pltpu.VMEM((32, 128), BF16),
            pltpu.VMEM((32, 128), BF16),
            pltpu.VMEM((32, 128), BF16),
            pltpu.VMEM((2, 2, 32), BF16),
            pltpu.VMEM((2, 2, 32), BF16),
            pltpu.VMEM((1, 64), F32),
            pltpu.VMEM((32, 128), BF16),
            pltpu.VMEM((32, 128), BF16),
            pltpu.SMEM((2,), F32),
            pltpu.SMEM((2, 2), F32),
            pltpu.SMEM((2, 2), F32),
            pltpu.VMEM((4, 256, 256), BF16),
            pltpu.VMEM((4, 256, 256), BF16),
            pltpu.VMEM((2, 32, 640), BF16),
            pltpu.VMEM((4, 4, 2, 32, 256), BF16),
            pltpu.VMEM((4, 4, 2, 32, 128), BF16),
            pltpu.VMEM((4, 4, 2, 32, 128), BF16),
            pltpu.VMEM((4, 4, 4, 2, 32, 128), BF16),
            pltpu.VMEM((384, 128), BF16),
            pltpu.VMEM((2, 64, 128), LINK),
            pltpu.VMEM((4, 4, 64, 128), LINK),
            pltpu.VMEM((4, 64, 128), BF16),
            pltpu.VMEM((4, 64, 128), BF16),
            pltpu.VMEM((4, 2, 32, 256), F32),
            pltpu.VMEM((4, 32, 256), F32),
            pltpu.SemaphoreType.DMA((COPIES,)),
            pltpu.SemaphoreType.DMA((COPIES,)),
            pltpu.SemaphoreType.DMA((18,)),
        ],
        compiler_params=pltpu.CompilerParams(collective_id=0, has_side_effects=True, vmem_limit_bytes=24 * 2**20),
    )(*(pltpu.with_memory_space_constraint(operand, pltpu.HBM) for operand in operands))
    return summed.astype(BF16)


def solution(mesh):
    return jax.shard_map(
        per_device,
        mesh=mesh,
        in_specs=(
            P("sp", "tp"), P(), P("sp", "tp"), P("sp", "tp"), P("sp", "tp"), P("tp"), P("sp", "tp"),
            P("sp", "tp"), P("sp", "tp"), P("sp", "tp"), P("sp", "tp", None), P("sp", "tp", None),
            P(None, "tp"), P(None, "tp"), P(), P("tp", "sp"), P("tp", "sp"),
        ),
        out_specs=P(("sp", "tp"), None),
        check_vma=False,
    )
```

```python
import jax
import jax.numpy as jnp
from jax import lax
from jax.experimental import pallas as pl
from jax.experimental.pallas import tpu as pltpu
from jax.sharding import PartitionSpec as P

HEAD_DIM = 64
WINDOW = 64
ROWS = 256
TOKENS = 4096
EPS = 1e-6
COPIES = 168
MESH = pl.DeviceIdType.MESH
F32 = jnp.float32
BF16 = jnp.bfloat16
LINK = BF16
NN = (((1,), (0,)), ((), ()))
NT = (((1,), (1,)), ((), ()))


def mm(a, b, dims=NN):
    return lax.dot_general(a, b, dims, preferred_element_type=F32)


def split(a):
    hi = a.astype(BF16)
    return hi, (a - hi.astype(F32)).astype(BF16)


def left(a):
    hi, lo = split(a)
    return jnp.concatenate([hi, lo], axis=1)


def right(b):
    hi, lo = split(b)
    return jnp.concatenate(
        [jnp.concatenate([hi, lo], axis=1), jnp.concatenate([hi, jnp.zeros_like(lo)], axis=1)], axis=0
    )


def dot3(a, b):
    both = mm(left(a), right(b))
    return both[:, 0:128] + both[:, 128:256]


def right64(b):
    hi, lo = split(b)
    none = jnp.zeros_like(lo)
    blank = jnp.concatenate([none, none], axis=1)
    return jnp.concatenate(
        [jnp.concatenate([hi, lo], axis=1), blank, jnp.concatenate([hi, none], axis=1), blank], axis=0
    )


def dot64(a, b):
    both = mm(left(a), right64(b))
    return both[:, 0:128] + both[:, 128:256]


def silu(v):
    return v * jax.nn.sigmoid(v)


def layer_kernel(
    tokens_in, gain_in, aq_in, ak_in, av_in, dq_in, dk_in, dv_in, dz_in, bw_in, gw_in, ogain_in, ao_in, do_in,
    sink_in, shift_in, dlog_in,
    out,
    gain, aq, ak, av, dq, dk, dv, dz, bw, gw, ogain, ao, do, sink, shift, dlog,
    tok, normed, stage, w1, wq, wkv, w2, kv, own_map, maps_in, hsend, hall, pbuf, prec, send_sem, recv_sem, own_sem,
):
    sp = lax.axis_index("sp")
    x = lax.axis_index("tp")
    c = lax.rem(sp, 2)
    b = lax.div(sp, 2)
    z = lax.div(b, 4)
    y = lax.rem(b, 4)
    o = 1 - c

    open_scopes = []

    def phase(name):
        while open_scopes:
            open_scopes.pop().__exit__(None, None, None)
        if name:
            open_scopes.append(jax.named_scope(name))
            open_scopes[0].__enter__()

    def m4(v):
        return lax.rem(v + 4, 4)

    def dev(zz, yy, cc, xx):
        return {"sp": (zz * 4 + yy) * 2 + cc, "tp": xx}

    def dev_x(d):
        return dev(z, y, c, m4(x + d))

    def dev_y(d, core=c):
        return dev(z, m4(y + d), core, x)

    def dev_z(d, core=c):
        return dev(m4(z + d), y, core, x)

    def dev_b(d):
        bb = lax.rem(b + d + 16, 16)
        return {"sp": bb * 2 + c, "tp": x}

    partner = dev(z, y, o, x)
    sent = []

    def send(src, dst, device, landed):
        i = len(sent)
        copy = pltpu.make_async_remote_copy(
            src_ref=src, dst_ref=dst, send_sem=send_sem.at[i], recv_sem=recv_sem.at[i],
            device_id=device, device_id_type=MESH,
        )
        copy.start()
        sent.append(copy)
        return pltpu.make_async_remote_copy(
            src_ref=landed, dst_ref=landed, send_sem=send_sem.at[i], recv_sem=recv_sem.at[i],
            device_id=device, device_id_type=MESH,
        )

    phase("load")
    half_rows = pl.ds(128 * c, 128)
    other_rows = pl.ds(128 * o, 128)
    tokens = tok.at[x, half_rows]
    loads = [
        pltpu.make_async_copy(src, dst, own_sem.at[i])
        for i, (src, dst) in enumerate(
            [(aq_in, aq), (ak_in, ak), (av_in, av), (dq_in, dq), (dk_in, dk), (dv_in, dv), (dz_in, dz), (bw_in, bw),
             (gw_in, gw), (ao_in, ao), (do_in, do), (tokens_in, tokens), (gain_in, gain), (ogain_in, ogain),
             (sink_in, sink), (shift_in, shift), (dlog_in, dlog)]
        )
    ]
    for load in loads:
        load.start()
    barrier = pltpu.get_barrier_semaphore()
    peers = [partner]
    for d in (1, 2, 3):
        peers += [dev_x(d), dev_y(d), dev_z(d), dev_y(d, o), dev_z(d, o)]
    for peer in peers:
        pl.semaphore_signal(barrier, inc=1, device_id=peer, device_id_type=MESH)
    for load in loads[:11]:
        load.wait()
    phase("pack")
    attn_t, delta_t = ao[...], do[...]
    blank = jnp.zeros((60, 32), F32)
    for cc in range(2):
        cols = slice(64 * cc, 64 * cc + 64)
        small = jnp.concatenate([bw[cc].astype(F32), gw[cc].astype(F32), blank], axis=0).T.astype(BF16)
        stage[cc] = jnp.concatenate(
            [dk[:, cols], dv[:, cols], dz[:, cols], small, dq[:, cols], aq[:, cols], av[...], ak[...],
             attn_t[:, cols], delta_t[:, cols]],
            axis=1,
        )
    w1[z, y, c] = stage[c, :, 0:256]
    wq[z, y, c] = stage[c, :, 256:384]
    wkv[z, y, c] = stage[c, :, 384:512]
    w2[x, z, y, c] = stage[c, :, 512:640]

    phase("barrier")
    pl.semaphore_wait(barrier, len(peers))

    class Gather:
        def __init__(self, place, y_first, source=None, twin=None):
            self.place, self.y_first, self.source, self.twin = place, y_first, source, twin
            self.waits = {}

        def slot(self, first, second):
            zz, yy = (z + second, y + first) if self.y_first else (z + first, y + second)
            return self.place(m4(zz), m4(yy))

        def own(self, axis, d):
            device = dev_y if axis == self.y_first else dev_z
            if self.source is None:
                return self.slot(0, 0), self.slot(0, 0), device(d)
            return self.source, self.twin, device(d, o)

        def begin(self):
            for d in (1, 3, 2):
                self.waits[d] = send(*self.own(True, d), self.slot(-d, 0))

        def across(self):
            for d in (1, 3, 2):
                self.waits[0, d] = send(*self.own(False, d), self.slot(0, -d))

        def forward(self, d):
            self.waits[d].wait_recv()
            block = self.slot(-d, 0)
            for e in (1, 3, 2):
                device = dev_z(e) if self.y_first else dev_y(e)
                self.waits[-d, e] = send(block, block, device, self.slot(-d, -e))

        def finish(self):
            for e in (1, 3, 2):
                for f in (0, -1, -3, -2):
                    self.waits[f, e].wait_recv()

    in_cols = pl.ds(0, 256)
    query_cols = pl.ds(256, 128)
    out_cols = pl.ds(512, 128)
    phase("start")
    first = Gather(lambda zz, yy: w1.at[zz, yy, c], True)
    second = Gather(lambda zz, yy: w1.at[zz, yy, o], False, stage.at[o, :, in_cols], w1.at[z, y, c])
    out_low = Gather(lambda zz, yy: w2.at[x, zz, yy, c, pl.ds(0, 16)], True)
    out_high = Gather(lambda zz, yy: w2.at[:, zz, yy, c, pl.ds(16, 16)], False)
    out_twin = Gather(
        lambda zz, yy: w2.at[x, zz, yy, o], False, stage.at[o, :, out_cols], w2.at[x, z, y, c]
    )
    query = Gather(lambda zz, yy: wq.at[zz, yy, c], True)
    query_twin = Gather(lambda zz, yy: wq.at[zz, yy, o], False, stage.at[o, :, query_cols], wq.at[z, y, c])
    keys = Gather(lambda zz, yy: wkv.at[zz, yy, c], True)
    later = (query, query_twin, keys, out_twin, out_low)
    first.begin()
    second.begin()
    first.across()
    second.across()
    for ring in later:
        ring.begin()
        ring.across()
    for load in loads[11:]:
        load.wait()
    upper = pl.ds(16, 16)
    w2_own = [
        send(
            stage.at[c, upper, out_cols], w2.at[x, z, y, c, upper], dev_x(d), w2.at[m4(x - d), z, y, c, upper]
        )
        for d in (1, 3, 2)
    ]
    tok_in = [send(tokens, tokens, dev_x(d), tok.at[m4(x - d), half_rows]) for d in (2, 1, 3)]
    w_swap = send(stage.at[o, :, in_cols], w1.at[z, y, c], partner, w1.at[z, y, o])
    tok_swap = [send(tokens, tokens, partner, tok.at[x, other_rows])]
    wq_swap = send(stage.at[o, :, query_cols], wq.at[z, y, c], partner, wq.at[z, y, o])
    w2_swap = send(stage.at[o, :, out_cols], w2.at[x, z, y, c], partner, w2.at[x, z, y, o])
    phase("near")
    for d in (1, 3, 2):
        first.forward(d)
        second.forward(d)
    phase("tokens")
    for d, arrived in zip((1, 3, 2), tok_in[1:] + tok_in[:1]):
        arrived.wait_recv()
        src = m4(x - d)
        tok_swap.append(send(tok.at[src, half_rows], tok.at[src, half_rows], partner, tok.at[src, other_rows]))
    phase("near2")
    for ring in later:
        for d in (1, 3, 2):
            ring.forward(d)
    phase("tokswap")
    for arrived in tok_swap:
        arrived.wait_recv()

    phase("norm")
    squares = jnp.zeros((ROWS, 1), F32)
    for k in range(4):
        wide = tok[k].astype(F32)
        squares = squares + jnp.sum(wide * wide, axis=-1, keepdims=True)
    inv = lax.rsqrt(squares * (1.0 / 1024.0) + EPS)
    for k in range(4):
        normed[k] = (tok[k].astype(F32) * inv * gain[:, 256 * k : 256 * k + 256]).astype(BF16)

    phase("outbegin")
    for arrived in w2_own:
        arrived.wait_recv()
    out_high.begin()
    out_high.across()
    phase("wfinish")
    w_swap.wait_recv()
    first.finish()
    second.finish()

    phase("proj")
    def project(w):
        total = mm(normed[0], w(0))
        for k in range(1, 4):
            total = total + mm(normed[k], w(k))
        return total

    proj = project(lambda k: w1[k].reshape(256, 256))
    phase("gates0")
    t1, t2 = proj[:, 0:128], proj[:, 128:256]
    lane = lax.broadcasted_iota(jnp.int32, (1, 128), 1)
    head = lane < 64
    act = silu(t1.astype(BF16).astype(F32))
    act_k = jnp.where(head, act, 0.0)
    key_val = jnp.where(head, act * lax.rsqrt(jnp.sum(act_k * act_k, axis=-1, keepdims=True) + EPS), act)

    phase("gates")
    bias = jnp.where(lane == 64, shift[0, c], jnp.where(lane == 65, shift[1, c], 0.0))
    rate = jnp.exp(jnp.where(lane == 66, dlog[0, c], jnp.where(lane == 67, dlog[1, c], 0.0)))
    strength = jax.nn.sigmoid(t2 + bias)
    softplus = jnp.maximum(t2, 0.0) + jnp.log1p(jnp.exp(-jnp.abs(t2)))
    decay = jnp.where((lane == 66) | (lane == 67), -rate * softplus * (1.0 / TOKENS), 0.0)

    row = lax.broadcasted_iota(jnp.int32, (128, 128), 0)
    col = lax.broadcasted_iota(jnp.int32, (128, 128), 1)
    masks = (row >= col, row <= col)
    unit = jnp.where(row == col, 1.0, 0.0)
    near16 = lax.shift_right_logical(row, 4) == lax.shift_right_logical(col, 4)

    g_hi = decay.astype(BF16)
    rest = decay - g_hi.astype(F32)
    g_mid = rest.astype(BF16)
    g_lo = (rest - g_mid.astype(F32)).astype(BF16)
    g_parts = jnp.concatenate(
        [jnp.concatenate([part[0:128], part[128:256]], axis=1) for part in (g_hi, g_mid, g_lo)], axis=0
    )
    ones = jnp.concatenate([jnp.where(mask, 1.0, 0.0).astype(BF16) for mask in masks], axis=0)
    sums = mm(jnp.concatenate([ones, ones, ones], axis=1), g_parts)
    g_all = jnp.where(
        lane == 66,
        jnp.concatenate([sums[0:128, 0:128], sums[0:128, 128:256]], axis=0),
        jnp.concatenate([sums[128:256, 0:128], sums[128:256, 128:256]], axis=0),
    )
    turned = jnp.where(head, key_val, g_all).T
    key_t = turned[0:64]
    key_left = left(key_val)

    phase("delta1")
    lane2 = lax.broadcasted_iota(jnp.int32, (64, 128), 1)
    row2 = lax.broadcasted_iota(jnp.int32, (64, 128), 0)
    eye2 = jnp.where(lane2 == row2, 1.0, 0.0)
    chains = [(way, h) for way in range(2) for h in range(2)]
    low, decays, sides, grown, key_end, end = {}, {}, {}, {}, {}, {}
    for h in range(2):
        hs = slice(128 * h, 128 * h + 128)
        pairs = mm(key_left[hs], right64(key_t[:, hs]))
        pairs = pairs[:, 0:128] + pairs[:, 128:256]
        for way in range(2):
            at = way, h
            beta = strength[hs, 64 + way : 65 + way]
            g_col = g_all[hs, 66 + way : 67 + way]
            g_row = turned[66 + way : 67 + way, hs]
            g_end = g_col[127:128] if way == 0 else g_col[0:1]
            decays[at] = jnp.exp(jnp.where(masks[way], g_col - g_row, -jnp.inf))
            low[at] = jnp.where(row == col, 0.0, beta * pairs * decays[at])
            up = jnp.exp(g_col)
            grown[at] = up
            sides[at] = key_val[hs] * jnp.where(head, beta * up, beta)
            key_end[at] = key_t[:, hs] * jnp.exp(g_end - g_row)
            end[at] = jnp.exp(g_end)
    d1 = {at: jnp.where(near16, low[at], 0.0) for at in chains}
    off = {at: jnp.where(near16, 0.0, low[at]) for at in chains}
    d2 = {at: dot3(d1[at], d1[at]) for at in chains}
    inner = {at: unit - d1[at] for at in chains}
    d4 = {at: dot3(d2[at], d2[at]) for at in chains}
    inner = {at: inner[at] + dot3(inner[at], d2[at]) for at in chains}
    d8 = {at: dot3(d4[at], d4[at]) for at in chains}
    inner = {at: inner[at] + dot3(inner[at], d4[at]) for at in chains}
    inner = {at: inner[at] + dot3(inner[at], d8[at]) for at in chains}
    phase("rings")
    keys.finish()
    kv_swap = send(wkv.at[:, :, c], wkv.at[:, :, c], partner, wkv.at[:, :, o])
    w2_swap.wait_recv()
    out_twin.finish()
    out_low.finish()
    w2_in = []
    for d in (1, 3, 2):
        src = m4(x - d)
        lower = pl.ds(0, 16)
        w2_in.append(send(w2.at[x, :, :, o], w2.at[x, :, :, o], dev_x(d), w2.at[src, :, :, o]))
        w2_in.append(
            send(w2.at[x, :, :, c, lower], w2.at[x, :, :, c, lower], dev_x(d), w2.at[src, :, :, c, lower])
        )

    phase("delta2")
    m1 = {at: dot3(inner[at], off[at]) for at in chains}
    wu = {at: dot3(inner[at], sides[at]) for at in chains}
    m2 = {at: dot3(m1[at], m1[at]) for at in chains}
    wu = {at: wu[at] - dot3(m1[at], wu[at]) for at in chains}
    m4_ = {at: dot3(m2[at], m2[at]) for at in chains}
    wu = {at: wu[at] + dot3(m2[at], wu[at]) for at in chains}
    wu = {at: wu[at] + dot3(m4_[at], wu[at]) for at in chains}
    phase("final")

    def after(later, earlier):
        return dot64(later, earlier) + later + earlier

    maps = {}
    for at in chains:
        final = dot3(key_end[at], wu[at])
        maps[at] = jnp.where(lane2 < 64, (end[at] - 1.0) * eye2 - final, final)
    for way in range(2):
        own_map[way] = after(maps[way, 1 - way], maps[way, way]).astype(LINK)
    phase("scan1send")
    scan = []

    def send_map(dz, dy):
        zz, yy = m4(z + dz), m4(y + dy)
        goes = jnp.where(zz * 4 + yy > b, 0, 1)
        scan.append(
            send(own_map.at[goes], maps_in.at[z, y], dev(zz, yy, c, x), maps_in.at[m4(z - dz), m4(y - dy)])
        )

    steps = [(dz, dy) for dz in range(4) for dy in range(4) if (dz, dy) != (0, 0)]
    steps.sort(key=lambda step: -(min(step[0], 4 - step[0]) + min(step[1], 4 - step[1])))
    for dz, dy in steps[:5]:
        send_map(dz, dy)
    phase("kvproj")
    kv_swap.wait_recv()
    kv[64:320, :] = project(lambda k: wkv[k].reshape(256, 128)).astype(BF16)
    halo = [
        send(kv.at[pl.ds(256, 64)], kv.at[pl.ds(0, 64)], dev_b(1), kv.at[pl.ds(0, 64)]),
        send(kv.at[pl.ds(64, 64)], kv.at[pl.ds(320, 64)], dev_b(-1), kv.at[pl.ds(320, 64)]),
    ]
    phase("scan1send2")
    for dz, dy in steps[5:]:
        send_map(dz, dy)
    phase("qproj")
    wq_swap.wait_recv()
    query.finish()
    query_twin.finish()
    t0 = project(lambda k: wq[k].reshape(256, 128))
    act = jnp.where(head, silu(t0.astype(BF16).astype(F32)), 0.0)
    q = act * (lax.rsqrt(jnp.sum(act * act, axis=-1, keepdims=True) + EPS) * HEAD_DIM**-0.5)
    q_left = left(q)

    phase("reads")
    reads = {}
    pairs = []
    for h in range(2):
        hs = slice(128 * h, 128 * h + 128)
        pair = mm(q_left[hs], right64(key_t[:, hs]))
        pairs.append(pair[:, 0:128] + pair[:, 128:256])
    for way, h in chains:
        at = way, h
        read = dot3(pairs[h] * decays[at], wu[at])
        reads[at] = jnp.where(head, grown[at] * q[128 * h : 128 * h + 128] - read, read)
        if h != way:
            reads[at] = reads[at] + dot64(reads[at], maps[way, way])
    reads = [jnp.concatenate([reads[way, 0], reads[way, 1]], axis=0) for way in range(2)]
    reads_left = [left(r) for r in reads]
    local = reads[0] + reads[1]
    gate = silu(t2.astype(BF16).astype(F32))
    gate = jnp.concatenate([gate[:, 64:128], gate[:, 0:64]], axis=1)
    gain_row = jnp.concatenate([ogain[...], ogain[...]], axis=1)

    phase("halo")
    for arrived in halo:
        arrived.wait_recv()
    phase("attn")
    att_q = jnp.where(head, 0.0, t0).astype(BF16)
    scores = mm(att_q, kv[...], NT) * HEAD_DIM**-0.5
    q_pos = lax.broadcasted_iota(jnp.int32, (ROWS, ROWS + 2 * WINDOW), 0)
    k_pos = lax.broadcasted_iota(jnp.int32, (ROWS, ROWS + 2 * WINDOW), 1) - WINDOW
    seen = k_pos + b * ROWS
    allowed = (jnp.abs(q_pos - k_pos) <= WINDOW) & (seen >= 0) & (seen < TOKENS)
    scores = jnp.where(allowed, scores, -jnp.inf)
    top = jnp.maximum(jnp.max(scores, axis=-1, keepdims=True), sink[c])
    weights = jnp.exp(scores - top)
    total = jnp.sum(weights, axis=-1, keepdims=True) + jnp.exp(sink[c] - top)
    weights = (weights / total).astype(BF16)
    attn_heads = mm(weights, kv[...])

    phase("scanwait")
    for arrived in scan:
        arrived.wait_recv()
    phase("outfwd")
    for d in (1, 3, 2):
        out_high.forward(d)
    phase("states")
    states = []
    for way in range(2):
        order = range(16) if way == 0 else range(15, -1, -1)
        chain = []
        for k in order:
            inside = (b > k) if way == 0 else (b < k)
            chain.append(jnp.where(inside, maps_in[k // 4, k % 4], jnp.zeros((64, 128), LINK)))
        level = []
        for k in range(0, 14, 2):
            earlier, later = chain[k], chain[k + 1]
            level.append(
                mm(later, jnp.concatenate([earlier, jnp.zeros_like(earlier)], axis=0))
                + later.astype(F32)
                + earlier.astype(F32)
            )
        level.append(chain[14].astype(F32))
        while len(level) > 1:
            level = [after(level[k + 1], level[k]) for k in range(0, len(level), 2)]
        states.append(jnp.where(lane2 < 64, 0.0, level[0]))

    phase("whole")
    both = mm(reads_left[0], right64(states[0])) + mm(reads_left[1], right64(states[1]))
    whole = jnp.where(head, 0.0, local + both[:, 0:128] + both[:, 128:256])
    scaled = whole * lax.rsqrt(jnp.sum(whole * whole, axis=-1, keepdims=True) * (1.0 / HEAD_DIM) + EPS) * gain_row
    heads = jnp.where(head, attn_heads, scaled * gate).astype(BF16)
    phase("headsend0")
    for k in range(4):
        hsend[k, 0:32] = heads[32 * k : 32 * k + 32]
        hsend[k, 32:64] = heads[128 + 32 * k : 160 + 32 * k]
    phase("headsend")
    head_in = [send(hsend.at[m4(x + d)], hall.at[x], dev_x(d), hall.at[m4(x - d)]) for d in (2, 1, 3)]
    hall[x] = hsend[x]
    phase("w2finish")
    out_high.finish()
    for arrived in w2_in:
        arrived.wait_recv()
    phase("headwait")
    def head_part(k):
        return mm(hall[k], w2[k].reshape(1024, 128), NT)

    part = head_part(x)
    for d, arrived in zip((1, 3, 2), head_in[1:] + head_in[:1]):
        arrived.wait_recv()
        part = part + head_part(m4(x - d))
    phase("outmm")
    last = []
    for k in range(4):
        pbuf[k, 0] = part[0:32, 256 * k : 256 * k + 256]
        pbuf[k, 1] = part[32:64, 256 * k : 256 * k + 256]
        if k % 2:
            pair = pl.ds(k - 1, 2)
            last.append(send(pbuf.at[pair, o], prec.at[pair], partner, prec.at[pair]))
    phase("last")
    for k in range(4):
        if k % 2 == 0:
            last[k // 2].wait_recv()
        out[:, 256 * k : 256 * k + 256] = pbuf[k, c] + prec[k]
    phase("drain")
    for copy in sent:
        copy.wait_send()
    phase(None)


def per_device(
    tokens, norm_gain, attn_query, attn_key, attn_value, sink_logit, delta_query, delta_key, delta_value,
    delta_gate, beta_weight, decay_weight, beta_shift, decay_log, out_gain, attn_out, delta_out,
):
    operands = (
        tokens, norm_gain.reshape(1, -1), attn_query, attn_key, attn_value, delta_query, delta_key, delta_value,
        delta_gate, beta_weight.transpose(1, 2, 0), decay_weight.transpose(1, 2, 0), out_gain.reshape(1, -1),
        attn_out.T, delta_out.T, sink_logit, beta_shift, decay_log,
    )
    hbm = pl.BlockSpec(memory_space=pltpu.HBM)
    vmem = pl.BlockSpec(memory_space=pltpu.VMEM)
    summed = pl.pallas_call(
        layer_kernel,
        out_shape=jax.ShapeDtypeStruct((32, 1024), F32),
        in_specs=[hbm] * 17,
        out_specs=vmem,
        scratch_shapes=[
            pltpu.VMEM((1, 1024), F32),
            pltpu.VMEM((32, 128), BF16),
            pltpu.VMEM((32, 64), BF16),
            pltpu.VMEM((32, 64), BF16),
            pltpu.VMEM((32, 128), BF16),
            pltpu.VMEM((32, 128), BF16),
            pltpu.VMEM((32, 128), BF16),
            pltpu.VMEM((32, 128), BF16),
            pltpu.VMEM((2, 2, 32), BF16),
            pltpu.VMEM((2, 2, 32), BF16),
            pltpu.VMEM((1, 64), F32),
            pltpu.VMEM((32, 128), BF16),
            pltpu.VMEM((32, 128), BF16),
            pltpu.SMEM((2,), F32),
            pltpu.SMEM((2, 2), F32),
            pltpu.SMEM((2, 2), F32),
            pltpu.VMEM((4, 256, 256), BF16),
            pltpu.VMEM((4, 256, 256), BF16),
            pltpu.VMEM((2, 32, 640), BF16),
            pltpu.VMEM((4, 4, 2, 32, 256), BF16),
            pltpu.VMEM((4, 4, 2, 32, 128), BF16),
            pltpu.VMEM((4, 4, 2, 32, 128), BF16),
            pltpu.VMEM((4, 4, 4, 2, 32, 128), BF16),
            pltpu.VMEM((384, 128), BF16),
            pltpu.VMEM((2, 64, 128), LINK),
            pltpu.VMEM((4, 4, 64, 128), LINK),
            pltpu.VMEM((4, 64, 128), BF16),
            pltpu.VMEM((4, 64, 128), BF16),
            pltpu.VMEM((4, 2, 32, 256), F32),
            pltpu.VMEM((4, 32, 256), F32),
            pltpu.SemaphoreType.DMA((COPIES,)),
            pltpu.SemaphoreType.DMA((COPIES,)),
            pltpu.SemaphoreType.DMA((18,)),
        ],
        compiler_params=pltpu.CompilerParams(collective_id=0, has_side_effects=True, vmem_limit_bytes=24 * 2**20),
    )(*(pltpu.with_memory_space_constraint(operand, pltpu.HBM) for operand in operands))
    return summed.astype(BF16)


def solution(mesh):
    return jax.shard_map(
        per_device,
        mesh=mesh,
        in_specs=(
            P("sp", "tp"), P(), P("sp", "tp"), P("sp", "tp"), P("sp", "tp"), P("tp"), P("sp", "tp"),
            P("sp", "tp"), P("sp", "tp"), P("sp", "tp"), P("sp", "tp", None), P("sp", "tp", None),
            P(None, "tp"), P(None, "tp"), P(), P("tp", "sp"), P("tp", "sp"),
        ),
        out_specs=P(("sp", "tp"), None),
        check_vma=False,
    )
```
